128 devices in a mesh: sp: 32 (over z, y, core), tp: 4 (over x).
Axes of the slice: x: 4, y: 4, z: 4, core: 2. Of those that a mesh axis runs over, the one named last changes fastest.
Arguments:
- out_grad: bfloat16 [8192, 4096], P('sp'), may hold values from -6 to 6
- stream: bfloat16 [8192, 4096], P('sp'), may hold values from -6 to 6
- norm_gain: bfloat16 [4096], replicated, may hold values from 0.099609375 to 1.8984375
- routes: int32 [8192, 2], P('sp'), may hold values from 0 to 31, all different within a row; in each aligned block of 256 rows (0 to 255, 256 to 511, ...) at most 20 rows name the same one
- route_weight: float32 [8192, 2], P('sp'), may hold values from 0.3 to 1.5
- gate_weight: bfloat16 [32, 4096, 1024], P('sp', None, 'tp'), may hold values from -0.09375 to 0.09375
- up_weight: bfloat16 [32, 4096, 1024], P('sp', None, 'tp'), may hold values from -0.09375 to 0.09375
- down_weight: bfloat16 [32, 1024, 4096], P('sp', 'tp'), may hold values from -0.1875 to 0.1875
- out_proj: bfloat16 [4096, 1024], P(None, 'tp'), may hold values from -0.1875 to 0.1875
- conv_out: bfloat16 [8192, 1024], P('sp', 'tp'), as said below
- gate_branch: bfloat16 [8192, 1024], P('sp', 'tp'), may hold values from -6 to 6
- decay_map: bfloat16 [2, 4, 256, 256], P(None, 'tp'), as said below
- input_map: bfloat16 [2, 4, 256, 256], P(None, 'tp'), as said below
- decay_param: float32 [2, 1024], P(None, 'tp'), as said below
- decay_shift: float32 [2, 8192, 1024], P(None, 'sp', 'tp'), as said below
- states: float32 [2, 8192, 1024], P(None, 'sp', 'tp'), as said below
Outputs:
- conv_grad: float32 [8192, 1024], P('sp', 'tp')
- gate_branch_grad: float32 [8192, 1024], P('sp', 'tp')
- out_proj_grad: float32 [4096, 1024], P('sp', 'tp')
- gate_weight_grad: bfloat16 [32, 4096, 1024], P('sp', None, 'tp')
- up_weight_grad: bfloat16 [32, 4096, 1024], P('sp', None, 'tp')
- down_weight_grad: bfloat16 [32, 1024, 4096], P('sp', 'tp')
The draws below stay inside these ranges and needn't reach their ends.
Inputs may be any that keep to these rules, and one draw needn't show every extreme that they name: `routes`: each token names 2 different experts. Among the 256 tokens of one index of sp no expert is named more than 20 times, a bound that some expert reaches in some of these blocks. `conv_out`: within -6 to 6. `decay_map`: entries within -4 to 4 times 256 to the power -0.5. `input_map`: entries within -4 to 4 times 256 to the power -0.5. `decay_param`: between 3.7 and 3.5 plus the logarithm of 8192. `decay_shift`: every entry lies between -0.7 and -0.00002. The forward pass's states: they follow the recurrences of the steps from conv_out, decay_map, input_map, decay_param and decay_shift.
All inputs are finite; a program needn't handle non-finite values.
Results may differ from the reference program's by a relative error of at most 0.018.
Values may be sent and summed in bfloat16 or wider, within the bound.
A program may use at most 128 MiB of HBM per device.

```python
import math
import jax
import jax.numpy as jnp
import numpy as np
from jax import lax

D = 4096
RECURRENT_WIDTH = 1024
BLOCKS = 4
BW = 256
FF = 1024
TOP = 2
TOK_DEV = 256
EXPERTS = 32
SEQUENCE_TOKENS = 8192
CAP = 20
N_SP = 32
N_TP = 4


def scan_pairs(coeffs, values, reverse):

    def combine(earlier, later):
        return (earlier[0] * later[0], later[0] * earlier[1] + later[1])
    return lax.associative_scan(combine, (coeffs, values), axis=0, reverse=reverse)[1]


def block_apply(channels, block_maps):
    shaped = channels.reshape(channels.shape[0], block_maps.shape[0], block_maps.shape[1])
    mapped = jnp.einsum('tkc,kcd->tkd', shaped, block_maps.astype(jnp.float32), precision=lax.Precision.HIGHEST)
    return mapped.reshape(channels.shape)


def lru_draw(key):
    random_keys = jax.random.split(jax.random.fold_in(key, 4242), 9)
    conv_field = jax.random.normal(random_keys[1], (SEQUENCE_TOKENS, RECURRENT_WIDTH), jnp.float32)
    fast_share = 0.5
    conv_field = jnp.clip(conv_field, -6.0, 6.0).astype(jnp.bfloat16)
    gate_maps = jnp.clip(jax.random.normal(random_keys[2], (2, 2, BLOCKS, BW, BW), jnp.float32), -4.0, 4.0)
    gate_maps = (gate_maps * BW ** (-0.5)).astype(jnp.bfloat16)
    fast_mask = jax.random.uniform(random_keys[3], (2, RECURRENT_WIDTH), jnp.float32) < fast_share
    slow_values = jnp.log(SEQUENCE_TOKENS * 1.0) + jax.random.uniform(random_keys[4], (2, RECURRENT_WIDTH), jnp.float32, 2.0, 3.5)
    fast_values = jax.random.uniform(random_keys[5], (2, RECURRENT_WIDTH), jnp.float32, 3.7, 4.9)
    decay_values = jnp.where(fast_mask, fast_values, slow_values)
    block_count = SEQUENCE_TOKENS // TOK_DEV
    block_rate = jnp.exp(jax.random.uniform(random_keys[6], (2, block_count), jnp.float32, -10.6, -9.2))
    shift_offset = -jnp.repeat(block_rate, TOK_DEV, axis=1)[:, :, None]
    spike_mask = jax.random.uniform(random_keys[7], (2, SEQUENCE_TOKENS, RECURRENT_WIDTH), jnp.float32) < 1.5 / SEQUENCE_TOKENS
    spike_depth = jnp.log(jax.random.uniform(random_keys[8], (2, SEQUENCE_TOKENS, RECURRENT_WIDTH), jnp.float32, 0.5, 0.8))
    offset_field = shift_offset + jnp.where(spike_mask, spike_depth, 0.0)
    conv_float = conv_field.astype(jnp.float32)
    state_list = []
    for direction in range(2):
        decay_gate = jax.nn.sigmoid(block_apply(conv_float, gate_maps[0, direction]))
        input_gate = jax.nn.sigmoid(block_apply(conv_float, gate_maps[1, direction]))
        log_decay = -8.0 * decay_gate * jax.nn.softplus(-decay_values[direction])[None, :] + offset_field[direction]
        drive_term = jnp.sqrt(-jnp.expm1(2.0 * log_decay)) * input_gate * conv_float
        state_list.append(scan_pairs(jnp.exp(log_decay), drive_term, direction == 1))
    return (conv_field, gate_maps[0], gate_maps[1], decay_values, offset_field, jnp.stack(state_list))


def draw_conv_out(key, part):
    return lru_draw(key)[0]


def draw_decay_map(key, part):
    return lru_draw(key)[1]


def draw_input_map(key, part):
    return lru_draw(key)[2]


def draw_decay_param(key, part):
    return lru_draw(key)[3]


def draw_decay_shift(key, part):
    return lru_draw(key)[4]


def draw_states(key, part):
    return lru_draw(key)[5]


def raised(values, rng, source, target, blocks, factor):
    owner, partner = [(jnp.arange(values.shape[position]) // (values.shape[position] // blocks)).reshape([-1 if axis == position else 1 for axis in range(values.ndim)]) for position in (source, target)]
    chosen = jax.random.permutation(rng, blocks)[partner]
    strong = (owner == chosen) | (owner == (partner + blocks // 2) % blocks)
    return jnp.where(strong, factor * values, values)


def levels(key, dims, pieces, least, largest):
    loudness = 1.0
    for position, parts in pieces:
        heights = jax.random.uniform(jax.random.fold_in(jax.random.fold_in(key, 6), position), (parts,), jnp.float32, least / len(pieces), largest / len(pieces))
        loudness = loudness * jnp.repeat(jnp.exp(heights), dims[position] // parts).reshape((-1,) + (1,) * (len(dims) - 1 - position))
    return loudness


def deal_out(key, own, number, rows, number_of, top, most, lean):
    order = jax.random.permutation(key, number_of)
    crowded, common = load_shares(number_of, rows * top, most, lean, True), load_shares(number_of, rows * top, most, lean, False)
    places = jnp.arange(number_of)

    def named(tallies, offset_by):
        used = int((tallies > 0).sum())
        fixed = max(1, used // 4)
        shifted = fixed + (places - fixed + offset_by * (used - fixed)) % max(1, number_of - fixed)
        return jnp.zeros((number_of,), jnp.int32).at[order[jnp.where(places < fixed, places, shifted)]].set(jnp.asarray(tallies, jnp.int32))

    tallies = jnp.where(number % 4 == 0, named(crowded, number // 4), named(common, number - number // 4 - 1))
    mixed = jax.random.permutation(jax.random.fold_in(own, 3), number_of)
    donor, sink = mixed[0:number_of // 2 * 2:2], mixed[1:number_of // 2 * 2:2]
    room = jnp.minimum(tallies[donor] - 1, most - tallies[sink]) // 2
    room = jnp.where((donor == order[0]) | (sink == order[0]) | (tallies[sink] == 0), 0, jnp.maximum(room, 0))
    shifted = jax.random.randint(jax.random.fold_in(own, 4), (number_of // 2,), 0, 1 << 20) % (room + 1)
    tallies = tallies.at[donor].add(-shifted).at[sink].add(shifted)
    members = jnp.searchsorted(jnp.cumsum(tallies), jnp.arange(rows * top), side="right").astype(jnp.int32)
    grid = members.reshape(top, rows).T
    grid = grid[jax.random.permutation(jax.random.fold_in(own, 1), rows)]
    offset_by = jax.random.randint(jax.random.fold_in(own, 2), (rows, 1), 0, top)
    return jnp.take_along_axis(grid, (jnp.arange(top)[None, :] + offset_by) % top, axis=1)


def load_shares(count, total, limit, skew, full):
    loads = [(1 << 20) // math.isqrt(standing ** skew) + 1 for standing in range(1, count + 1)]
    largest = limit if full else min(limit, max(-(-total // count), total * loads[0] // sum(loads)))
    least = 1 if total - largest >= count - 1 else 0
    counts, rest = [largest] + [least] * (count - 1), total - largest - least * (count - 1)
    while rest > 0:
        movable = [i for i in range(1, count) if counts[i] < largest] or [i for i in range(1, count) if counts[i] < limit]
        whole, remaining = sum([loads[i] for i in movable]), rest
        for i in movable:
            more = min(limit - counts[i], max(1, remaining * loads[i] // whole), rest)
            counts[i] = counts[i] + more
            rest = rest - more
    return np.array(counts)


def bell_draw(stream_key, shape, deviation, reach, shards=(), held_as=jnp.bfloat16):
    drawn = deviation * jax.random.normal(stream_key, shape, jnp.float32)
    if shards:
        drawn = drawn * levels(stream_key, shape, shards, -0.22, 0.18)
    return jnp.clip(drawn, -reach, reach).astype(held_as)


def noise_with(own_key, dims, deviation, most, cuts, heavy, kind=jnp.bfloat16):
    array = deviation * jax.random.normal(own_key, dims, jnp.float32)
    if cuts:
        array = array * levels(own_key, dims, cuts, -0.22, 0.18)
    return jnp.clip(raised(array, jax.random.fold_in(own_key, 3), *heavy), -most, most).astype(kind)


def setup_inputs(seed: int = 0) -> dict:
    key_of = jax.random.split(jax.random.key(seed), 17)
    out_grad = noise_with(key_of[0], (SEQUENCE_TOKENS, D), 1.0, 6.0, ((0, 32),), (0, 1, 32, 2.75))
    stream = bell_draw(key_of[1], (SEQUENCE_TOKENS, D), 1.0, 6.0, ((0, 32),))
    norm_gain = jnp.clip(1.0 + 0.18 * jax.random.normal(key_of[2], (D,), jnp.float32), 0.099609375, 1.8984375).astype(jnp.bfloat16)
    routes_keys = jax.random.split(jax.random.fold_in(key_of[3], 1), SEQUENCE_TOKENS // TOK_DEV)
    routes_turns = jax.random.permutation(jax.random.fold_in(key_of[3], 3), SEQUENCE_TOKENS // TOK_DEV)
    routes = jax.vmap(lambda own, number: deal_out(jax.random.fold_in(key_of[3], 2), own, number, TOK_DEV, EXPERTS, TOP, CAP, 1))(routes_keys, routes_turns).reshape((SEQUENCE_TOKENS, TOP))
    route_weight = jnp.clip(0.3 + 1.2 * jax.random.uniform(key_of[4], (SEQUENCE_TOKENS, TOP), jnp.float32) ** levels(key_of[4], (SEQUENCE_TOKENS, TOP), ((0, 32),), -0.2, 0.2), 0.3, 1.5)
    gate_weight = bell_draw(key_of[5], (EXPERTS, D, FF), D ** -0.5, 0.09375, ((0, 32), (2, 4)))
    up_weight = bell_draw(key_of[6], (EXPERTS, D, FF), D ** -0.5, 0.09375, ((0, 32), (2, 4)))
    down_weight = bell_draw(key_of[7], (EXPERTS, FF, D), FF ** -0.5, 0.1875, ((0, 32), (1, 4)))
    out_proj = bell_draw(key_of[8], (D, RECURRENT_WIDTH), RECURRENT_WIDTH ** -0.5, 0.1875, ((1, 4),))
    conv_out = draw_conv_out(jax.random.fold_in(key_of[16], 71), 0)
    gate_branch = bell_draw(key_of[10], (SEQUENCE_TOKENS, RECURRENT_WIDTH), 1.0, 6.0, ((0, 32), (1, 4)))
    decay_map = draw_decay_map(jax.random.fold_in(key_of[16], 71), 0)
    input_map = draw_input_map(jax.random.fold_in(key_of[16], 71), 0)
    decay_param = draw_decay_param(jax.random.fold_in(key_of[16], 71), 0)
    decay_shift = draw_decay_shift(jax.random.fold_in(key_of[16], 71), 0)
    states = draw_states(jax.random.fold_in(key_of[16], 71), 0)
    return dict(out_grad=out_grad, stream=stream, norm_gain=norm_gain, routes=routes, route_weight=route_weight, gate_weight=gate_weight, up_weight=up_weight, down_weight=down_weight, out_proj=out_proj, conv_out=conv_out, gate_branch=gate_branch, decay_map=decay_map, input_map=input_map, decay_param=decay_param, decay_shift=decay_shift, states=states)


rate_scale = 8.0
norm_eps = 1e-06

def contract(left, right, left_dim, right_dim):
    return lax.dot_general(left, right, (((left_dim,), (right_dim,)), ((), ())), preferred_element_type=jnp.float32)

def linear_scan(coeffs, values, reverse):

    def combine(earlier, later):
        return (earlier[0] * later[0], later[0] * earlier[1] + later[1])
    return lax.associative_scan(combine, (coeffs, values), axis=0, reverse=reverse)

def silu_grad(values):
    logistic = jax.nn.sigmoid(values)
    return logistic * (1.0 + values * (1.0 - logistic))

def expert_pass(slot_inputs, slot_cotan, gate_local, up_local, down_local):
    gate_pre = contract(slot_inputs, gate_local, 1, 0)
    up_pre = contract(slot_inputs, up_local, 1, 0)
    hidden = (jax.nn.silu(gate_pre) * up_pre).astype(jnp.bfloat16)
    down_wgrad = contract(hidden, slot_cotan, 0, 0)
    hidden_grad = contract(slot_cotan, down_local, 1, 1)
    up_grad = (hidden_grad * jax.nn.silu(gate_pre)).astype(jnp.bfloat16)
    gate_grad = (hidden_grad * up_pre * silu_grad(gate_pre)).astype(jnp.bfloat16)
    gate_wgrad = contract(slot_inputs, gate_grad, 0, 0)
    up_wgrad = contract(slot_inputs, up_grad, 0, 0)
    return (gate_wgrad, up_wgrad, down_wgrad, gate_grad, up_grad)

def block_forward(channels, block_maps):
    shaped = channels.reshape(channels.shape[0], block_maps.shape[0], block_maps.shape[1])
    mapped = jnp.einsum('tkc,kcd->tkd', shaped, block_maps.astype(jnp.float32), precision=lax.Precision.HIGHEST)
    return mapped.reshape(channels.shape)

def block_backward(pre_grad, block_maps):
    shaped = pre_grad.reshape(pre_grad.shape[0], block_maps.shape[0], block_maps.shape[2])
    mapped = jnp.einsum('tkd,kcd->tkc', shaped, block_maps.astype(jnp.float32), precision=lax.Precision.HIGHEST)
    return mapped.reshape(pre_grad.shape)

def recurrence_back(adjoint, state_run, conv_float, gate_parts, decay_local, input_local):
    decay_gate, input_gate, decay_base, decay_rate, drive_scale, drive_term = gate_parts
    log_grad = adjoint * (state_run - drive_term) - adjoint * input_gate * conv_float * decay_rate * decay_rate / drive_scale
    decay_pre_grad = log_grad * (-rate_scale * decay_base) * decay_gate * (1.0 - decay_gate)
    input_pre_grad = adjoint * drive_scale * conv_float * input_gate * (1.0 - input_gate)
    return adjoint * drive_scale * input_gate + block_backward(decay_pre_grad, decay_local) + block_backward(input_pre_grad, input_local)

def reference(out_grad, stream, norm_gain, routes, route_weight, gate_weight, up_weight, down_weight, out_proj, conv_out, gate_branch, decay_map, input_map, decay_param, decay_shift, states):
    stream_f = stream.astype(jnp.float32)
    row_scale = lax.rsqrt(lax.optimization_barrier(jnp.mean(stream_f * stream_f, axis=1, keepdims=True)) + norm_eps)
    unit_rows = stream_f * row_scale
    gain_row = norm_gain.astype(jnp.float32)[None, :]
    normed = (unit_rows * gain_row).astype(jnp.bfloat16)
    pair_count = SEQUENCE_TOKENS * TOP
    pair_expert = routes.reshape(N_SP, TOK_DEV * TOP)
    onehot = (pair_expert[:, :, None] == jnp.arange(EXPERTS, dtype=jnp.int32)[None, None, :]).astype(jnp.int32)
    slot_rank = lax.optimization_barrier(jnp.sum((jnp.cumsum(onehot, axis=1) - onehot) * onehot, axis=2))
    source = jnp.arange(N_SP, dtype=jnp.int32)[:, None]
    slot_index = (pair_expert * (N_SP * CAP) + source * CAP + slot_rank).reshape(-1).astype(jnp.int32)
    slot_pair = jnp.full((EXPERTS * N_SP * CAP,), pair_count, jnp.int32).at[slot_index].set(jnp.arange(pair_count, dtype=jnp.int32))
    slot_token = (slot_pair // TOP).astype(jnp.int32)
    zero_row = jnp.zeros((1, D), jnp.bfloat16)
    slot_inputs = jnp.concatenate([normed, zero_row])[slot_token].reshape(EXPERTS, N_SP * CAP, D)
    weight_pad = jnp.concatenate([route_weight.reshape(-1), jnp.zeros((1,), jnp.float32)])
    slot_cotan = (weight_pad[slot_pair][:, None] * jnp.concatenate([out_grad, zero_row])[slot_token].astype(jnp.float32)).astype(jnp.bfloat16)
    slot_cotan = slot_cotan.reshape(EXPERTS, N_SP * CAP, D)

    def one_expert(operands):
        inputs_e, cotan_e, gate_local, up_local, down_local = operands
        gate_wgrad, up_wgrad, down_wgrad, gate_grad, up_grad = expert_pass(inputs_e, cotan_e, gate_local, up_local, down_local)
        run_width = FF // N_TP
        total_sum = jnp.zeros((inputs_e.shape[0], D), jnp.float32)
        for quarter in range(N_TP):
            low_unit = quarter * run_width
            high_unit = low_unit + run_width
            partial_value = contract(gate_grad[:, low_unit:high_unit], gate_local[:, low_unit:high_unit], 1, 1) + contract(up_grad[:, low_unit:high_unit], up_local[:, low_unit:high_unit], 1, 1)
            total_sum = total_sum + lax.optimization_barrier(partial_value.astype(jnp.bfloat16)).astype(jnp.float32)
        return (gate_wgrad.astype(jnp.bfloat16), up_wgrad.astype(jnp.bfloat16), down_wgrad.astype(jnp.bfloat16), total_sum.astype(jnp.bfloat16))
    gate_grads, up_grads, down_grads, pair_grad = lax.map(one_expert, (slot_inputs, slot_cotan, gate_weight, up_weight, down_weight))
    returned = pair_grad.reshape(EXPERTS * N_SP * CAP, D)[slot_index]
    normed_grad = lax.optimization_barrier(jnp.sum(returned.reshape(SEQUENCE_TOKENS, TOP, D).astype(jnp.float32), axis=1))
    scaled_grad = gain_row * normed_grad
    stream_grad = out_grad.astype(jnp.float32) + row_scale * (scaled_grad - unit_rows * lax.optimization_barrier(jnp.mean(unit_rows * scaled_grad, axis=1, keepdims=True)))
    stream_grad_b = stream_grad.astype(jnp.bfloat16)
    total_state = states[0] + states[1]
    gate_float = gate_branch.astype(jnp.float32)
    gelu_gate, gelu_back = jax.vjp(jax.nn.gelu, gate_float)
    lru_out = (total_state * gelu_gate).astype(jnp.bfloat16)
    out_proj_grad = contract(stream_grad_b, lru_out, 0, 0)
    lru_out_grad = contract(stream_grad_b, out_proj, 1, 0)
    gate_branch_grad = gelu_back(lru_out_grad * total_state)[0]
    state_grad = lru_out_grad * gelu_gate
    conv_float = conv_out.astype(jnp.float32)
    ones_row = jnp.ones((1, RECURRENT_WIDTH), jnp.float32)
    conv_grad = jnp.zeros_like(conv_float)
    for direction in range(2):
        decay_gate = jax.nn.sigmoid(block_forward(conv_float, decay_map[direction]))
        input_gate = jax.nn.sigmoid(block_forward(conv_float, input_map[direction]))
        decay_base = jax.nn.softplus(-decay_param[direction])[None, :]
        log_decay = -rate_scale * decay_gate * decay_base + decay_shift[direction]
        decay_rate = jnp.exp(log_decay)
        drive_scale = jnp.sqrt(-jnp.expm1(2.0 * log_decay))
        drive_term = drive_scale * input_gate * conv_float
        if direction == 0:
            adjoint = linear_scan(jnp.concatenate([decay_rate[1:], ones_row]), state_grad, True)[1]
        else:
            adjoint = linear_scan(jnp.concatenate([ones_row, decay_rate[:-1]]), state_grad, False)[1]
        gate_parts = (decay_gate, input_gate, decay_base, decay_rate, drive_scale, drive_term)
        conv_grad = conv_grad + recurrence_back(adjoint, states[direction], conv_float, gate_parts, decay_map[direction], input_map[direction])
    return (conv_grad, gate_branch_grad, out_proj_grad, gate_grads, up_grads, down_grads)
```

```python
import functools

import jax
import jax.numpy as jnp
from jax import lax
from jax.experimental import pallas as pl
from jax.experimental.pallas import tpu as pltpu
from jax.sharding import PartitionSpec as P

BF = jnp.bfloat16
F32 = jnp.float32
I32 = jnp.int32
MESH = pl.DeviceIdType.MESH
ANY = pl.BlockSpec(memory_space=pl.ANY)
VM = pl.BlockSpec(memory_space=pltpu.VMEM)

SPN = 32
TPN = 4
TOK = 256
QW = 1024
FFQ = 256
CHUNKS = 4
SP = "sp"
CW = QW // CHUNKS
HALF = 320
rate_scale = 8.0
norm_eps = 1e-06


def contract(left, right, left_dim, right_dim, precision=None):
    return lax.dot_general(
        left,
        right,
        (((left_dim,), (right_dim,)), ((), ())),
        preferred_element_type=F32,
        precision=precision,
    )


def prep_kernel(stream, out_grad, gain, routes, weight, send, combine, qi, qc0, qc1, scale):
    h = pl.program_id(0)
    low = lax.axis_index("tp") % 2

    @pl.when(h == 0)
    def _():
        wide = stream[...].astype(F32)
        mean = jnp.sum(wide * wide, axis=1, keepdims=True) * (1.0 / (TPN * QW))
        scale[...] = jnp.broadcast_to(lax.rsqrt(mean + norm_eps), (TOK, 128))
        lanes = lax.broadcasted_iota(I32, (TOK, 128), 1)
        r0, r1 = routes[:, 0:1], routes[:, 1:2]
        hot0 = (r0 == lanes).astype(F32)
        hot1 = (r1 == lanes).astype(F32)
        before = (
            lax.broadcasted_iota(I32, (TOK, TOK), 1) < lax.broadcasted_iota(I32, (TOK, TOK), 0)
        ).astype(F32)
        counts = contract(before.astype(BF), (hot0 + hot1).astype(BF), 1, 0)
        upper = lax.axis_index("sp") // 16
        slots = lax.broadcasted_iota(I32, (TOK, 768), 1)

        def places(route, hot):
            rank = jnp.sum(counts * hot, axis=1, keepdims=True).astype(I32)
            pure = (rank // 8) * 256 + route * 8 + rank % 8
            mixed = 512 + route * 8 + (rank - 16)
            of_input = jnp.where(rank < 16, pure, mixed + 4 * upper)
            of_cotan = jnp.where(rank < 16, pure, mixed + 4 * (1 - upper))
            return (slots == of_input).astype(F32), (slots == of_cotan).astype(F32)

        in0, cot0 = places(r0, hot0)
        in1, cot1 = places(r1, hot1)
        both = (in0 + in1).astype(BF)
        qi[...] = both
        combine[...] = both
        qc0[...] = cot0.astype(BF)
        qc1[...] = cot1.astype(BF)

    cols = pl.ds(pl.multiple_of((2 * h + low) * QW, QW), QW)
    normed = (stream[:, cols].astype(F32) * scale[:, 0:1] * gain[:, cols].astype(F32)).astype(BF)
    grad = out_grad[:, cols].astype(F32)
    scaled0 = (weight[:, 0:1] * grad).astype(BF)
    scaled1 = (weight[:, 1:2] * grad).astype(BF)
    for plane in range(3):
        span = slice(plane * 256, plane * 256 + 256)
        rows_in = contract(qi[:, span], normed, 0, 0)
        rows_cot = contract(qc0[:, span], scaled0, 0, 0) + contract(qc1[:, span], scaled1, 0, 0)
        if plane < 2:
            send[0, plane] = rows_in.astype(BF)
            send[0, plane + 2] = rows_cot.astype(BF)
        else:
            send[0, 4] = (rows_in + rows_cot).astype(BF)


def prep(stream, out_grad, gain, routes, weight):
    whole = lambda shape: pl.BlockSpec(shape, lambda h: (0,) * len(shape))
    return pl.pallas_call(
        prep_kernel,
        grid=(2,),
        in_specs=[
            whole((TOK, 4 * QW)),
            whole((TOK, 4 * QW)),
            whole((1, 4 * QW)),
            whole((TOK, 2)),
            whole((TOK, 2)),
        ],
        out_specs=[
            pl.BlockSpec((1, 5, 256, QW), lambda h: (h, 0, 0, 0)),
            whole((TOK, 768)),
        ],
        out_shape=[
            jax.ShapeDtypeStruct((2, 5, 256, QW), BF),
            jax.ShapeDtypeStruct((TOK, 768), BF),
        ],
        scratch_shapes=[
            pltpu.VMEM((TOK, 768), BF),
            pltpu.VMEM((TOK, 768), BF),
            pltpu.VMEM((TOK, 768), BF),
            pltpu.VMEM((TOK, 128), F32),
        ],
        compiler_params=pltpu.CompilerParams(vmem_limit_bytes=48 * 1024 * 1024),
        name="prep",
    )(stream, out_grad, gain, routes, weight)


def greet(s, x):
    barrier = pltpu.get_barrier_semaphore()

    def hello(d, carry):
        pl.semaphore_signal(barrier, inc=1, device_id=(s ^ d, x), device_id_type=MESH)
        return carry

    lax.fori_loop(1, SPN, hello, 0)
    for step in (1, TPN - 1):
        pl.semaphore_signal(
            barrier, inc=1, device_id=(s, lax.rem(x + step, TPN)), device_id_type=MESH
        )
    pl.semaphore_wait(barrier, SPN + 1)


def remote(src, dst, send_sem, recv_sem, target):
    return pltpu.make_async_remote_copy(
        src_ref=src,
        dst_ref=dst,
        send_sem=send_sem,
        recv_sem=recv_sem,
        device_id=target,
        device_id_type=MESH,
    )


def loop(lower, upper, step):
    def run(d, carry):
        step(d)
        return carry

    lax.fori_loop(lower, upper, run, 0)


def dispatch_kernel(send, got, own_sem, send_sem, recv_sem, fwd_send, fwd_recv):
    s = lax.axis_index("sp")
    x = lax.axis_index("tp")
    high, low = x // 2, x % 2
    right, left = lax.rem(x + 1, TPN), lax.rem(x + TPN - 1, TPN)
    greet(s, x)

    def rows(i):
        return pl.ds(pl.multiple_of(i * 8, 8), 8)

    def across(d):
        return remote(
            send.at[:, :, rows(s ^ d), :],
            got.at[:, low, :, rows(s), :],
            send_sem.at[d],
            recv_sem.at[d],
            (s ^ d, x),
        )

    def onward(d, side):
        src = got.at[high, low, :, rows(s ^ d), :]
        return remote(
            src,
            src,
            fwd_send.at[side, d],
            fwd_recv.at[side, d],
            (s, right if side == 0 else left),
        )

    def onward_own(side):
        return remote(
            send.at[high, :, rows(s), :],
            got.at[high, low, :, rows(s), :],
            fwd_send.at[side, 0],
            fwd_recv.at[side, 0],
            (s, right if side == 0 else left),
        )

    def arriving(d, side):
        quarter = left if side == 0 else right
        src = got.at[quarter // 2, quarter % 2, :, rows(s ^ d), :]
        return remote(src, src, fwd_send.at[side, d], fwd_recv.at[side, d], (s, quarter))

    own = pltpu.make_async_copy(
        send.at[:, :, rows(s), :], got.at[:, low, :, rows(s), :], own_sem
    )
    own.start()
    onward_own(0).start()
    onward_own(1).start()
    loop(1, SPN, lambda d: across(d).start())

    def pass_on(d):
        across(d).wait_recv()
        onward(d, 0).start()
        onward(d, 1).start()

    loop(1, SPN, pass_on)
    own.wait()
    onward_own(0).wait_send()
    onward_own(1).wait_send()

    def finish(d):
        across(d).wait_send()
        onward(d, 0).wait_send()
        onward(d, 1).wait_send()

    loop(1, SPN, finish)

    def landed(d):
        arriving(d, 0).wait_recv()
        arriving(d, 1).wait_recv()

    loop(0, SPN, landed)


def dispatch(send):
    return pl.pallas_call(
        dispatch_kernel,
        in_specs=[ANY],
        out_specs=ANY,
        out_shape=jax.ShapeDtypeStruct((2, 2, 5, 256, QW), BF),
        scratch_shapes=[
            pltpu.SemaphoreType.DMA,
            pltpu.SemaphoreType.DMA((SPN,)),
            pltpu.SemaphoreType.DMA((SPN,)),
            pltpu.SemaphoreType.DMA((2, SPN)),
            pltpu.SemaphoreType.DMA((2, SPN)),
        ],
        compiler_params=pltpu.CompilerParams(collective_id=0, has_side_effects=True),
        name="dispatch",
    )(send)


def swap_halves(v):
    tiles = v.reshape(16, 8, v.shape[1])
    return pltpu.roll(tiles, 4, 1).reshape(v.shape)


def expert_kernel(
    got, gate, up, down, part, gate_wg, up_wg, down_wg,
    vin, vcot, vmix, vg, vu, vd, vpart, ogu, od, gp, upre, hg, gu, hid,
    in_sem, w_sem, part_sem, o_sem,
):
    def loads(q):
        hi, lo = q // 2, q % 2
        out = []
        for plane in range(5):
            if plane < 2:
                dst = vin.at[q, pl.ds(plane * 256, 256), :]
            elif plane < 4:
                dst = vcot.at[q, pl.ds((plane - 2) * 256, 256), :]
            else:
                dst = vmix.at[q]
            out.append(pltpu.make_async_copy(got.at[hi, lo, plane], dst, in_sem.at[q, plane]))
        rows = pl.ds(pl.multiple_of(q * QW, QW), QW)
        out.append(pltpu.make_async_copy(gate.at[rows, :], vg.at[q], w_sem.at[0, q]))
        out.append(pltpu.make_async_copy(up.at[rows, :], vu.at[q], w_sem.at[1, q]))
        out.append(pltpu.make_async_copy(down.at[:, rows], vd.at[q], w_sem.at[2, q]))
        return out

    loop(0, TPN, lambda q: [c.start() for c in loads(q)])
    gp[...] = jnp.zeros_like(gp)
    upre[...] = jnp.zeros_like(upre)
    hg[...] = jnp.zeros_like(hg)

    def forward(q):
        for c in loads(q):
            c.wait()
        first = lax.broadcasted_iota(I32, (128, QW), 0) % 8 < 4
        a = vmix[q, 0:128, :].astype(F32)
        b = vmix[q, 128:256, :].astype(F32)
        vin[q, 512:640, :] = jnp.where(first, a, b).astype(BF)
        vcot[q, 512:640, :] = jnp.where(first, b, a).astype(BF)
        rows = vin[q]
        gp[...] += contract(rows, vg[q], 1, 0)
        upre[...] += contract(rows, vu[q], 1, 0)
        hg[...] += contract(vcot[q], vd[q], 1, 1)

    loop(0, TPN, forward)
    hg[512:640, :] = swap_halves(hg[512:640, :])
    gate_pre, up_pre, hidden_grad = gp[...], upre[...], hg[...]
    logistic = jax.nn.sigmoid(gate_pre)
    silu = gate_pre * logistic
    hidden = silu * up_pre
    hid[0:512, :] = hidden[0:512, :].astype(BF)
    hid[512:640, :] = swap_halves(hidden[512:640, :]).astype(BF)
    gu[:, 0:FFQ] = (
        hidden_grad * up_pre * (logistic * (1.0 + gate_pre * (1.0 - logistic)))
    ).astype(BF)
    gu[:, FFQ : 2 * FFQ] = (hidden_grad * silu).astype(BF)

    def part_out(q):
        return pltpu.make_async_copy(vpart.at[q], part.at[q], part_sem.at[q])

    def back(q):
        vpart[q] = (
            contract(gu[:, 0:FFQ], vg[q], 1, 1) + contract(gu[:, FFQ : 2 * FFQ], vu[q], 1, 1)
        ).astype(BF)
        part_out(q).start()

    loop(0, TPN, back)

    def grads_out(q):
        rows = pl.ds(pl.multiple_of(q * QW, QW), QW)
        return (
            pltpu.make_async_copy(ogu.at[0, q], gate_wg.at[rows, :], o_sem.at[0, q]),
            pltpu.make_async_copy(ogu.at[1, q], up_wg.at[rows, :], o_sem.at[1, q]),
            pltpu.make_async_copy(od.at[q], down_wg.at[:, rows], o_sem.at[2, q]),
        )

    def weights(q):
        both = contract(vin[q], gu[...], 0, 0)
        ogu[0, q] = both[:, 0:FFQ].astype(BF)
        ogu[1, q] = both[:, FFQ : 2 * FFQ].astype(BF)
        od[q] = contract(hid[...], vcot[q], 0, 0).astype(BF)
        for c in grads_out(q):
            c.start()

    loop(0, TPN, weights)
    loop(0, TPN, lambda q: part_out(q).wait())
    loop(0, TPN, lambda q: [c.wait() for c in grads_out(q)])


def expert(got, gate, up, down):
    full = TPN * QW
    return pl.pallas_call(
        expert_kernel,
        in_specs=[ANY] * 4,
        out_specs=[ANY] * 4,
        out_shape=[
            jax.ShapeDtypeStruct((TPN, 640, QW), BF),
            jax.ShapeDtypeStruct((full, FFQ), BF),
            jax.ShapeDtypeStruct((full, FFQ), BF),
            jax.ShapeDtypeStruct((FFQ, full), BF),
        ],
        scratch_shapes=[
            pltpu.VMEM((TPN, 640, QW), BF),
            pltpu.VMEM((TPN, 640, QW), BF),
            pltpu.VMEM((TPN, 256, QW), BF),
            pltpu.VMEM((TPN, QW, FFQ), BF),
            pltpu.VMEM((TPN, QW, FFQ), BF),
            pltpu.VMEM((TPN, FFQ, QW), BF),
            pltpu.VMEM((TPN, 640, QW), BF),
            pltpu.VMEM((2, TPN, QW, FFQ), BF),
            pltpu.VMEM((TPN, FFQ, QW), BF),
            pltpu.VMEM((640, FFQ), F32),
            pltpu.VMEM((640, FFQ), F32),
            pltpu.VMEM((640, FFQ), F32),
            pltpu.VMEM((640, 2 * FFQ), BF),
            pltpu.VMEM((640, FFQ), BF),
            pltpu.SemaphoreType.DMA((TPN, 5)),
            pltpu.SemaphoreType.DMA((3, TPN)),
            pltpu.SemaphoreType.DMA((TPN,)),
            pltpu.SemaphoreType.DMA((3, TPN)),
        ],
        compiler_params=pltpu.CompilerParams(vmem_limit_bytes=60 * 1024 * 1024),
        name="expert",
    )(got, gate, up, down)


def back_kernel(
    part, combine, grad, far, near, relay, final, back,
    far_send, far_recv, near_send, near_recv, own_sem, ret_send, ret_recv, all_send, all_recv,
):
    s = lax.axis_index("sp")
    x = lax.axis_index("tp")
    right, left, across = (lax.rem(x + k, TPN) for k in (1, 3, 2))
    greet(s, x)

    def rows(i):
        return pl.ds(pl.multiple_of(i * 8, 8), 8)

    def cols(c):
        return pl.ds(pl.multiple_of(c * CW, CW), CW)

    def half(side):
        return pl.ds(side * HALF, HALF)

    def to_far(c, side):
        return remote(
            part.at[across, half(side), cols(c)],
            far.at[side, c],
            far_send.at[side, c],
            far_recv.at[side, c],
            (s, (right, left)[side]),
        )

    def to_near_plain(c, side):
        return remote(
            part.at[(right, left)[side], half(1 - side), cols(c)],
            near.at[side, c, half(1 - side), :],
            near_send.at[side, 0, c],
            near_recv.at[side, 0, c],
            (s, (right, left)[side]),
        )

    def to_near_sum(c, side):
        return remote(
            relay.at[side, c],
            near.at[side, c, half(side), :],
            near_send.at[side, 1, c],
            near_recv.at[side, 1, c],
            (s, (right, left)[side]),
        )

    def own_back(c):
        return pltpu.make_async_copy(
            final.at[c, :, rows(s), :], back.at[c, :, rows(s), :], own_sem.at[c]
        )

    def home(c, d):
        return remote(
            final.at[c, :, rows(s ^ d), :],
            back.at[c, :, rows(s), :],
            ret_send.at[c, d],
            ret_recv.at[c, d],
            (s ^ d, x),
        )

    def spread(c, side):
        src = grad.at[x, :, cols(c)]
        return remote(
            src, src, all_send.at[side, 0, c], all_recv.at[side, 0, c], (s, (right, left)[side])
        )

    def spread_on(c, side):
        src = grad.at[(left, right)[side], pl.ds(side * 128, 128), cols(c)]
        return remote(
            src, src, all_send.at[side, 1, c], all_recv.at[side, 1, c], (s, (right, left)[side])
        )

    def stage(t):
        @pl.when(t < CHUNKS)
        def _():
            for side in range(2):
                to_far(t, side).start()
                to_near_plain(t, side).start()

        c1 = t - 1

        @pl.when((c1 >= 0) & (c1 < CHUNKS))
        def _():
            for side in range(2):
                to_far(c1, side).wait_recv()
                mine = part[(right, left)[side], pl.ds(side * HALF, HALF), cols(c1)]
                relay[side, c1] = (far[side, c1].astype(F32) + mine.astype(F32)).astype(BF)
                to_near_sum(c1, side).start()

        c2 = t - 2

        @pl.when((c2 >= 0) & (c2 < CHUNKS))
        def _():
            for side in range(2):
                to_near_plain(c2, side).wait_recv()
                to_near_sum(c2, side).wait_recv()
            total = (
                part[x, :, cols(c2)].astype(F32)
                + near[0, c2].astype(F32)
                + near[1, c2].astype(F32)
            ).astype(BF)
            final[c2, 0] = total[0:256]
            final[c2, 1] = total[256:512]
            final[c2, 2, 0:128, :] = total[512:640]
            final[c2, 2, 128:256, :] = total[512:640]
            own_back(c2).start()
            loop(1, SPN, lambda d: home(c2, d).start())

        c3 = t - 3

        @pl.when((c3 >= 0) & (c3 < CHUNKS))
        def _():
            own_back(c3).wait()
            loop(1, SPN, lambda d: home(c3, d).wait_recv())
            summed = contract(combine[...], back[c3].reshape(768, CW), 1, 0)
            grad[x, :, cols(c3)] = summed.astype(BF)
            for side in range(2):
                spread(c3, side).start()

        c4 = t - 4

        @pl.when((c4 >= 0) & (c4 < CHUNKS))
        def _():
            for side in range(2):
                spread(c4, side).wait_recv()
                spread_on(c4, side).start()

    loop(0, CHUNKS + 4, stage)

    def finish(c):
        for side in range(2):
            to_far(c, side).wait_send()
            to_near_plain(c, side).wait_send()
            to_near_sum(c, side).wait_send()
            spread(c, side).wait_send()
            spread_on(c, side).wait_send()
            spread_on(c, side).wait_recv()
        loop(1, SPN, lambda d: home(c, d).wait_send())

    loop(0, CHUNKS, finish)


def send_back(part, combine):
    return pl.pallas_call(
        back_kernel,
        in_specs=[VM, VM],
        out_specs=VM,
        out_shape=jax.ShapeDtypeStruct((TPN, TOK, QW), BF),
        scratch_shapes=[
            pltpu.VMEM((2, CHUNKS, HALF, CW), BF),
            pltpu.VMEM((2, CHUNKS, 2 * HALF, CW), BF),
            pltpu.VMEM((2, CHUNKS, HALF, CW), BF),
            pltpu.VMEM((CHUNKS, 3, 256, CW), BF),
            pltpu.VMEM((CHUNKS, 3, 256, CW), BF),
            pltpu.SemaphoreType.DMA((2, CHUNKS)),
            pltpu.SemaphoreType.DMA((2, CHUNKS)),
            pltpu.SemaphoreType.DMA((2, 2, CHUNKS)),
            pltpu.SemaphoreType.DMA((2, 2, CHUNKS)),
            pltpu.SemaphoreType.DMA((CHUNKS,)),
            pltpu.SemaphoreType.DMA((CHUNKS, SPN)),
            pltpu.SemaphoreType.DMA((CHUNKS, SPN)),
            pltpu.SemaphoreType.DMA((2, 2, CHUNKS)),
            pltpu.SemaphoreType.DMA((2, 2, CHUNKS)),
        ],
        compiler_params=pltpu.CompilerParams(
            collective_id=1, has_side_effects=True, vmem_limit_bytes=48 * 1024 * 1024
        ),
        name="send_back",
    )(part, combine)


def expm1_negative(v):
    series = 1.0 + v * (1.0 / 9.0)
    for k in (8, 7, 6, 5, 4, 3, 2):
        series = 1.0 + v * (1.0 / k) * series
    return jnp.where(v > -0.5, v * series, jnp.exp(v) - 1.0)


def scan_rows(coeff, value, reverse):
    rows = lax.broadcasted_iota(I32, coeff.shape, 0)
    for k in (1, 2, 4, 8, 16, 32, 64, 128):
        if reverse:
            inside = rows < TOK - k
            shift = TOK - k
        else:
            inside = rows >= k
            shift = k
        coeff_far = jnp.where(inside, pltpu.roll(coeff, shift, 0), 1.0)
        value_far = jnp.where(inside, pltpu.roll(value, shift, 0), 0.0)
        value = value + coeff * value_far
        coeff = coeff * coeff_far
    return coeff, value


def mixer_kernel(
    stream, out_grad, gain, grad, states, branch, out_proj, conv, decay_map, input_map, base, shift,
    branch_grad, proj_part, ends, linear, sgb, dot, scale, lru,
):
    def squares(q, carry):
        v = stream[:, pl.ds(pl.multiple_of(q * QW, QW), QW)].astype(F32)
        g = gain[:, pl.ds(pl.multiple_of(q * QW, QW), QW)].astype(F32)
        w = v * (g * grad[q].astype(F32))
        return (
            carry[0] + jnp.sum(v * v, axis=1, keepdims=True),
            carry[1] + jnp.sum(w, axis=1, keepdims=True),
        )

    zero = jnp.zeros((TOK, 1), F32)
    square, along = lax.fori_loop(0, TPN, squares, (zero, zero))
    inverse = 1.0 / (TPN * QW)
    row_scale = lax.rsqrt(square * inverse + norm_eps)
    scale[...] = jnp.broadcast_to(row_scale, (TOK, 128))
    dot[...] = jnp.broadcast_to(along * row_scale * inverse, (TOK, 128))

    def rows_grad(q, carry):
        cols = pl.ds(pl.multiple_of(q * QW, QW), QW)
        r = scale[:, 0:1]
        unit = stream[:, cols].astype(F32) * r
        scaled = gain[:, cols].astype(F32) * grad[q].astype(F32)
        v = (out_grad[:, cols].astype(F32) + r * (scaled - unit * dot[:, 0:1])).astype(BF)
        sgb[:, cols] = v
        return carry + contract(v, out_proj[cols, :], 1, 0)

    lru_grad = lax.fori_loop(0, TPN, rows_grad, jnp.zeros((TOK, FFQ), F32))
    total = states[0] + states[1]
    b = branch[...].astype(F32)
    root = 0.7978845608028654
    tanh = jnp.tanh(root * (b + 0.044715 * b * b * b))
    gelu = 0.5 * b * (1.0 + tanh)
    slope = 0.5 * (1.0 + tanh) + 0.5 * b * (1.0 - tanh * tanh) * root * (
        1.0 + 3.0 * 0.044715 * b * b
    )
    lru[...] = (total * gelu).astype(BF)
    branch_grad[...] = lru_grad * total * slope
    state_grad = lru_grad * gelu

    def proj(q):
        cols = pl.ds(pl.multiple_of(q * QW, QW), QW)
        proj_part[pl.ds(q * 8, 8)] = contract(sgb[:, cols], lru[...], 0, 0).astype(BF).reshape(
            8, 128, FFQ
        )

    loop(0, TPN, proj)
    c = conv[...].astype(F32)
    rows = lax.broadcasted_iota(I32, (TOK, FFQ), 0)
    for d in range(2):
        r = jax.nn.sigmoid(contract(conv[...], decay_map[d], 1, 0))
        i = jax.nn.sigmoid(contract(conv[...], input_map[d], 1, 0))
        rate = (-rate_scale) * base[d : d + 1, :]
        log_decay = r * rate + shift[d]
        decay = jnp.exp(log_decay)
        width = jnp.sqrt(-expm1_negative(2.0 * log_decay))
        drive = width * i * c
        if d == 0:
            coeff = jnp.where(rows == TOK - 1, 1.0, pltpu.roll(decay, TOK - 1, 0))
            edge = slice(0, 1)
        else:
            coeff = jnp.where(rows == 0, 1.0, pltpu.roll(decay, 1, 0))
            edge = slice(TOK - 1, TOK)
        reach, inner = scan_rows(coeff, state_grad, d == 0)
        ends[2 * d : 2 * d + 1, :] = decay[edge] * reach[edge]
        ends[2 * d + 1 : 2 * d + 2, :] = decay[edge] * inner[edge]
        linear[d, 0] = reach
        linear[d, 1] = inner
        linear[d, 2] = width * i
        linear[d, 3] = ((states[d] - drive) - i * c * decay * decay / width) * rate * r * (1.0 - r)
        linear[d, 4] = width * c * i * (1.0 - i)
    ends[4:8, :] = jnp.zeros((4, FFQ), F32)


def mixer(*operands):
    return pl.pallas_call(
        mixer_kernel,
        in_specs=[VM] * 12,
        out_specs=[VM] * 4,
        out_shape=[
            jax.ShapeDtypeStruct((TOK, FFQ), F32),
            jax.ShapeDtypeStruct((SPN, 128, FFQ), BF),
            jax.ShapeDtypeStruct((8, FFQ), F32),
            jax.ShapeDtypeStruct((2, 5, TOK, FFQ), F32),
        ],
        scratch_shapes=[
            pltpu.VMEM((TOK, TPN * QW), BF),
            pltpu.VMEM((TOK, 128), F32),
            pltpu.VMEM((TOK, 128), F32),
            pltpu.VMEM((TOK, FFQ), BF),
        ],
        compiler_params=pltpu.CompilerParams(vmem_limit_bytes=56 * 1024 * 1024),
        name="mixer",
    )(*operands)


def across_kernel(
    ends, proj_part, linear, decay_map, input_map, conv_grad, proj_grad, edges, pieces,
    end_send, end_recv, piece_send, piece_recv, own_sem,
):
    s = lax.axis_index("sp")
    x = lax.axis_index("tp")
    greet(s, x)

    def ends_to(d):
        return remote(ends, edges.at[s], end_send.at[d], end_recv.at[d], (s ^ d, x))

    def piece_to(d):
        return remote(
            proj_part.at[s ^ d], pieces.at[s], piece_send.at[d], piece_recv.at[d], (s ^ d, x)
        )

    loop(1, SPN, lambda d: ends_to(d).start())
    loop(1, SPN, lambda d: piece_to(d).start())
    own = pltpu.make_async_copy(proj_part.at[s], pieces.at[s], own_sem)
    own.start()
    edges[s] = ends[...]
    loop(1, SPN, lambda d: ends_to(d).wait_recv())

    def carry_in(j, carry):
        later = SPN - 1 - j
        e0, e1 = edges[later], edges[j]
        from_right = jnp.where(later > s, e0[1:2] + e0[0:1] * carry[0], carry[0])
        from_left = jnp.where(j < s, e1[3:4] + e1[2:3] * carry[1], carry[1])
        return from_right, from_left

    zero = jnp.zeros((1, FFQ), F32)
    incoming = lax.fori_loop(0, SPN, carry_in, (zero, zero))
    highest = lax.Precision.HIGHEST
    total = jnp.zeros((TOK, FFQ), F32)
    for d in range(2):
        adjoint = linear[d, 1] + linear[d, 0] * incoming[d]
        total = total + (
            adjoint * linear[d, 2]
            + contract(adjoint * linear[d, 3], decay_map[d].astype(F32), 1, 1, highest)
            + contract(adjoint * linear[d, 4], input_map[d].astype(F32), 1, 1, highest)
        )
    conv_grad[...] = total
    own.wait()

    def add(d, acc):
        piece_to(d).wait_recv()
        return acc + pieces[s ^ d].astype(F32)

    proj_grad[...] = lax.fori_loop(1, SPN, add, pieces[s].astype(F32))

    def finish(d):
        ends_to(d).wait_send()
        piece_to(d).wait_send()

    loop(1, SPN, finish)


def across(ends, proj_part, linear, decay_map, input_map):
    return pl.pallas_call(
        across_kernel,
        in_specs=[VM] * 5,
        out_specs=[VM] * 2,
        out_shape=[
            jax.ShapeDtypeStruct((TOK, FFQ), F32),
            jax.ShapeDtypeStruct((128, FFQ), F32),
        ],
        scratch_shapes=[
            pltpu.VMEM((SPN, 8, FFQ), F32),
            pltpu.VMEM((SPN, 128, FFQ), BF),
            pltpu.SemaphoreType.DMA((SPN,)),
            pltpu.SemaphoreType.DMA((SPN,)),
            pltpu.SemaphoreType.DMA((SPN,)),
            pltpu.SemaphoreType.DMA((SPN,)),
            pltpu.SemaphoreType.DMA,
        ],
        compiler_params=pltpu.CompilerParams(
            collective_id=2, has_side_effects=True, vmem_limit_bytes=40 * 1024 * 1024
        ),
        name="across",
    )(ends, proj_part, linear, decay_map, input_map)


def body(
    out_grad,
    stream,
    norm_gain,
    routes,
    route_weight,
    gate_weight,
    up_weight,
    down_weight,
    out_proj,
    conv_out,
    gate_branch,
    decay_map,
    input_map,
    decay_param,
    decay_shift,
    states,
):
    send, combine = prep(stream, out_grad, norm_gain[None, :], routes, route_weight)
    got = dispatch(send)
    part, gate_wgrad, up_wgrad, down_wgrad = expert(
        got, gate_weight[0], up_weight[0], down_weight[0]
    )
    grad = send_back(part, combine)
    base = jax.nn.softplus(-decay_param)
    decay_maps, input_maps = decay_map[:, 0], input_map[:, 0]
    branch_grad, proj_part, ends, linear = mixer(
        stream, out_grad, norm_gain[None, :], grad, states, gate_branch, out_proj, conv_out,
        decay_maps, input_maps, base, decay_shift,
    )
    conv_grad, proj_grad = across(ends, proj_part, linear, decay_maps, input_maps)
    return (
        conv_grad, branch_grad, proj_grad, gate_wgrad[None], up_wgrad[None], down_wgrad[None]
    )


def solution(mesh):
    in_specs = (
        P(SP, None),
        P(SP, None),
        P(),
        P(SP, None),
        P(SP, None),
        P(SP, None, "tp"),
        P(SP, None, "tp"),
        P(SP, "tp", None),
        P(None, "tp"),
        P(SP, "tp"),
        P(SP, "tp"),
        P(None, "tp", None, None),
        P(None, "tp", None, None),
        P(None, "tp"),
        P(None, SP, "tp"),
        P(None, SP, "tp"),
    )
    out_specs = (
        P(SP, "tp"),
        P(SP, "tp"),
        P(SP, "tp"),
        P(SP, None, "tp"),
        P(SP, None, "tp"),
        P(SP, "tp", None),
    )
    return jax.shard_map(body, mesh=mesh, in_specs=in_specs, out_specs=out_specs, check_vma=False)
```

```python
import functools

import jax
import jax.numpy as jnp
from jax import lax
from jax.experimental import pallas as pl
from jax.experimental.pallas import tpu as pltpu
from jax.sharding import PartitionSpec as P

BF = jnp.bfloat16
F32 = jnp.float32
I32 = jnp.int32
MESH = pl.DeviceIdType.MESH
ANY = pl.BlockSpec(memory_space=pl.ANY)
VM = pl.BlockSpec(memory_space=pltpu.VMEM)

SPN = 32
TPN = 4
TOK = 256
QW = 1024
FFQ = 256
CHUNKS = 4
SP = "sp"
CW = QW // CHUNKS
HALF = 320
rate_scale = 8.0
norm_eps = 1e-06


def contract(left, right, left_dim, right_dim, precision=None):
    return lax.dot_general(
        left,
        right,
        (((left_dim,), (right_dim,)), ((), ())),
        preferred_element_type=F32,
        precision=precision,
    )


def prep_kernel(stream, out_grad, gain, routes, weight, send, combine, qi, qc0, qc1, scale):
    h = pl.program_id(0)
    low = lax.axis_index("tp") % 2

    @pl.when(h == 0)
    def _():
        wide = stream[...].astype(F32)
        mean = jnp.sum(wide * wide, axis=1, keepdims=True) * (1.0 / (TPN * QW))
        scale[...] = jnp.broadcast_to(lax.rsqrt(mean + norm_eps), (TOK, 128))
        lanes = lax.broadcasted_iota(I32, (TOK, 128), 1)
        r0, r1 = routes[:, 0:1], routes[:, 1:2]
        hot0 = (r0 == lanes).astype(F32)
        hot1 = (r1 == lanes).astype(F32)
        before = (
            lax.broadcasted_iota(I32, (TOK, TOK), 1) < lax.broadcasted_iota(I32, (TOK, TOK), 0)
        ).astype(F32)
        counts = contract(before.astype(BF), (hot0 + hot1).astype(BF), 1, 0)
        upper = lax.axis_index("sp") // 16
        slots = lax.broadcasted_iota(I32, (TOK, 768), 1)

        def places(route, hot):
            rank = jnp.sum(counts * hot, axis=1, keepdims=True).astype(I32)
            pure = (rank // 8) * 256 + route * 8 + rank % 8
            mixed = 512 + route * 8 + (rank - 16)
            of_input = jnp.where(rank < 16, pure, mixed + 4 * upper)
            of_cotan = jnp.where(rank < 16, pure, mixed + 4 * (1 - upper))
            return (slots == of_input).astype(F32), (slots == of_cotan).astype(F32)

        in0, cot0 = places(r0, hot0)
        in1, cot1 = places(r1, hot1)
        both = (in0 + in1).astype(BF)
        qi[...] = both
        combine[...] = both
        qc0[...] = cot0.astype(BF)
        qc1[...] = cot1.astype(BF)

    cols = pl.ds(pl.multiple_of((2 * h + low) * QW, QW), QW)
    normed = (stream[:, cols].astype(F32) * scale[:, 0:1] * gain[:, cols].astype(F32)).astype(BF)
    grad = out_grad[:, cols].astype(F32)
    scaled0 = (weight[:, 0:1] * grad).astype(BF)
    scaled1 = (weight[:, 1:2] * grad).astype(BF)
    for plane in range(3):
        span = slice(plane * 256, plane * 256 + 256)
        rows_in = contract(qi[:, span], normed, 0, 0)
        rows_cot = contract(qc0[:, span], scaled0, 0, 0) + contract(qc1[:, span], scaled1, 0, 0)
        if plane < 2:
            send[0, plane] = rows_in.astype(BF)
            send[0, plane + 2] = rows_cot.astype(BF)
        else:
            send[0, 4] = (rows_in + rows_cot).astype(BF)


def prep(stream, out_grad, gain, routes, weight):
    whole = lambda shape: pl.BlockSpec(shape, lambda h: (0,) * len(shape))
    return pl.pallas_call(
        prep_kernel,
        grid=(2,),
        in_specs=[
            whole((TOK, 4 * QW)),
            whole((TOK, 4 * QW)),
            whole((1, 4 * QW)),
            whole((TOK, 2)),
            whole((TOK, 2)),
        ],
        out_specs=[
            pl.BlockSpec((1, 5, 256, QW), lambda h: (h, 0, 0, 0)),
            whole((TOK, 768)),
        ],
        out_shape=[
            jax.ShapeDtypeStruct((2, 5, 256, QW), BF),
            jax.ShapeDtypeStruct((TOK, 768), BF),
        ],
        scratch_shapes=[
            pltpu.VMEM((TOK, 768), BF),
            pltpu.VMEM((TOK, 768), BF),
            pltpu.VMEM((TOK, 768), BF),
            pltpu.VMEM((TOK, 128), F32),
        ],
        compiler_params=pltpu.CompilerParams(vmem_limit_bytes=48 * 1024 * 1024),
        name="prep",
    )(stream, out_grad, gain, routes, weight)


NEAR = (
    (0, 1), (1, 0), (0, 3), (3, 0), (1, 1), (3, 3), (1, 3), (3, 1),
    (0, 2), (2, 0), (1, 2), (2, 1), (3, 2), (2, 3), (2, 2),
)
STEPS = ((0, 0, 1),) + tuple((z, y, c) for c in (0, 1) for z, y in NEAR)


def peer(s, k, sign=1):
    z, y, c = STEPS[k - 1]
    return (
        lax.rem(s // 8 + (z if sign > 0 else 4 - z), 4) * 8
        + lax.rem((s // 2) % 4 + (y if sign > 0 else 4 - y), 4) * 2
        + lax.rem(s % 2 + c, 2)
    )


def greet(s, x):
    barrier = pltpu.get_barrier_semaphore()

    def hello(d, carry):
        pl.semaphore_signal(barrier, inc=1, device_id=(s ^ d, x), device_id_type=MESH)
        return carry

    lax.fori_loop(1, SPN, hello, 0)
    for step in (1, TPN - 1):
        pl.semaphore_signal(
            barrier, inc=1, device_id=(s, lax.rem(x + step, TPN)), device_id_type=MESH
        )
    pl.semaphore_wait(barrier, SPN + 1)


def remote(src, dst, send_sem, recv_sem, target):
    return pltpu.make_async_remote_copy(
        src_ref=src,
        dst_ref=dst,
        send_sem=send_sem,
        recv_sem=recv_sem,
        device_id=target,
        device_id_type=MESH,
    )


def loop(lower, upper, step):
    def run(d, carry):
        step(d)
        return carry

    lax.fori_loop(lower, upper, run, 0)


def dispatch_kernel(send, got, own_sem, send_sem, recv_sem, fwd_send, fwd_recv):
    s = lax.axis_index("sp")
    x = lax.axis_index("tp")
    high, low = x // 2, x % 2
    right, left = lax.rem(x + 1, TPN), lax.rem(x + TPN - 1, TPN)
    greet(s, x)

    def rows(i):
        return pl.ds(pl.multiple_of(i * 8, 8), 8)

    def over(turn, k, target):
        hi = high if turn == 0 else 1 - high
        return remote(
            send.at[hi, :, rows(target), :],
            got.at[hi, low, :, rows(s), :],
            send_sem.at[turn, k],
            recv_sem.at[turn, k],
            (target, x),
        )

    def onward(src, dst, k, side):
        return remote(
            src, dst, fwd_send.at[side, k], fwd_recv.at[side, k], (s, (right, left)[side])
        )

    def block(i):
        return got.at[high, low, :, rows(i), :]

    own = pltpu.make_async_copy(
        send.at[:, :, rows(s), :], got.at[:, low, :, rows(s), :], own_sem
    )
    own.start()
    for side in range(2):
        onward(send.at[high, :, rows(s), :], block(s), 0, side).start()
    for turn in range(2):
        for k in range(1, SPN):
            over(turn, k, peer(s, k)).start()
    for k in range(1, SPN):
        source = peer(s, k, -1)
        over(0, k, source).wait_recv()
        for side in range(2):
            onward(block(source), block(source), k, side).start()
    own.wait()

    def finish(k):
        for turn in range(2):
            over(turn, k, s ^ 1).wait_send()
        over(1, k, s ^ 1).wait_recv()

    def finish_onward(k):
        for side in range(2):
            copy = onward(block(s), block(s), k, side)
            copy.wait_send()
            copy.wait_recv()

    loop(1, SPN, finish)
    loop(0, SPN, finish_onward)


def dispatch(send):
    return pl.pallas_call(
        dispatch_kernel,
        in_specs=[ANY],
        out_specs=ANY,
        out_shape=jax.ShapeDtypeStruct((2, 2, 5, 256, QW), BF),
        scratch_shapes=[
            pltpu.SemaphoreType.DMA,
            pltpu.SemaphoreType.DMA((2, SPN)),
            pltpu.SemaphoreType.DMA((2, SPN)),
            pltpu.SemaphoreType.DMA((2, SPN)),
            pltpu.SemaphoreType.DMA((2, SPN)),
        ],
        compiler_params=pltpu.CompilerParams(collective_id=0, has_side_effects=True),
        name="dispatch",
    )(send)


def swap_halves(v):
    tiles = v.reshape(16, 8, v.shape[1])
    return pltpu.roll(tiles, 4, 1).reshape(v.shape)


def expert_kernel(
    got, gate, up, down, part, gate_wg, up_wg, down_wg,
    vin, vcot, vmix, vg, vu, vd, vpart, ogu, od, gp, upre, hg, gu, hid,
    in_sem, w_sem, part_sem, o_sem,
):
    def loads(q):
        hi, lo = q // 2, q % 2
        out = []
        for plane in range(5):
            if plane < 2:
                dst = vin.at[q, pl.ds(plane * 256, 256), :]
            elif plane < 4:
                dst = vcot.at[q, pl.ds((plane - 2) * 256, 256), :]
            else:
                dst = vmix.at[q]
            out.append(pltpu.make_async_copy(got.at[hi, lo, plane], dst, in_sem.at[q, plane]))
        rows = pl.ds(pl.multiple_of(q * QW, QW), QW)
        out.append(pltpu.make_async_copy(gate.at[rows, :], vg.at[q], w_sem.at[0, q]))
        out.append(pltpu.make_async_copy(up.at[rows, :], vu.at[q], w_sem.at[1, q]))
        out.append(pltpu.make_async_copy(down.at[:, rows], vd.at[q], w_sem.at[2, q]))
        return out

    loop(0, TPN, lambda q: [c.start() for c in loads(q)])
    gp[...] = jnp.zeros_like(gp)
    upre[...] = jnp.zeros_like(upre)
    hg[...] = jnp.zeros_like(hg)

    def forward(q):
        for c in loads(q):
            c.wait()
        first = lax.broadcasted_iota(I32, (128, QW), 0) % 8 < 4
        a = vmix[q, 0:128, :].astype(F32)
        b = vmix[q, 128:256, :].astype(F32)
        vin[q, 512:640, :] = jnp.where(first, a, b).astype(BF)
        vcot[q, 512:640, :] = jnp.where(first, b, a).astype(BF)
        rows = vin[q]
        gp[...] += contract(rows, vg[q], 1, 0)
        upre[...] += contract(rows, vu[q], 1, 0)
        hg[...] += contract(vcot[q], vd[q], 1, 1)

    loop(0, TPN, forward)
    hg[512:640, :] = swap_halves(hg[512:640, :])
    gate_pre, up_pre, hidden_grad = gp[...], upre[...], hg[...]
    logistic = jax.nn.sigmoid(gate_pre)
    silu = gate_pre * logistic
    hidden = silu * up_pre
    hid[0:512, :] = hidden[0:512, :].astype(BF)
    hid[512:640, :] = swap_halves(hidden[512:640, :]).astype(BF)
    gu[:, 0:FFQ] = (
        hidden_grad * up_pre * (logistic * (1.0 + gate_pre * (1.0 - logistic)))
    ).astype(BF)
    gu[:, FFQ : 2 * FFQ] = (hidden_grad * silu).astype(BF)

    def part_out(q):
        return pltpu.make_async_copy(vpart.at[q], part.at[q], part_sem.at[q])

    def back(q):
        vpart[q] = (
            contract(gu[:, 0:FFQ], vg[q], 1, 1) + contract(gu[:, FFQ : 2 * FFQ], vu[q], 1, 1)
        ).astype(BF)
        part_out(q).start()

    loop(0, TPN, back)

    def grads_out(q):
        rows = pl.ds(pl.multiple_of(q * QW, QW), QW)
        return (
            pltpu.make_async_copy(ogu.at[0, q], gate_wg.at[rows, :], o_sem.at[0, q]),
            pltpu.make_async_copy(ogu.at[1, q], up_wg.at[rows, :], o_sem.at[1, q]),
            pltpu.make_async_copy(od.at[q], down_wg.at[:, rows], o_sem.at[2, q]),
        )

    def weights(q):
        both = contract(vin[q], gu[...], 0, 0)
        ogu[0, q] = both[:, 0:FFQ].astype(BF)
        ogu[1, q] = both[:, FFQ : 2 * FFQ].astype(BF)
        od[q] = contract(hid[...], vcot[q], 0, 0).astype(BF)
        for c in grads_out(q):
            c.start()

    loop(0, TPN, weights)
    loop(0, TPN, lambda q: part_out(q).wait())
    loop(0, TPN, lambda q: [c.wait() for c in grads_out(q)])


def expert(got, gate, up, down):
    full = TPN * QW
    return pl.pallas_call(
        expert_kernel,
        in_specs=[ANY] * 4,
        out_specs=[ANY] * 4,
        out_shape=[
            jax.ShapeDtypeStruct((TPN, 640, QW), BF),
            jax.ShapeDtypeStruct((full, FFQ), BF),
            jax.ShapeDtypeStruct((full, FFQ), BF),
            jax.ShapeDtypeStruct((FFQ, full), BF),
        ],
        scratch_shapes=[
            pltpu.VMEM((TPN, 640, QW), BF),
            pltpu.VMEM((TPN, 640, QW), BF),
            pltpu.VMEM((TPN, 256, QW), BF),
            pltpu.VMEM((TPN, QW, FFQ), BF),
            pltpu.VMEM((TPN, QW, FFQ), BF),
            pltpu.VMEM((TPN, FFQ, QW), BF),
            pltpu.VMEM((TPN, 640, QW), BF),
            pltpu.VMEM((2, TPN, QW, FFQ), BF),
            pltpu.VMEM((TPN, FFQ, QW), BF),
            pltpu.VMEM((640, FFQ), F32),
            pltpu.VMEM((640, FFQ), F32),
            pltpu.VMEM((640, FFQ), F32),
            pltpu.VMEM((640, 2 * FFQ), BF),
            pltpu.VMEM((640, FFQ), BF),
            pltpu.SemaphoreType.DMA((TPN, 5)),
            pltpu.SemaphoreType.DMA((3, TPN)),
            pltpu.SemaphoreType.DMA((TPN,)),
            pltpu.SemaphoreType.DMA((3, TPN)),
        ],
        compiler_params=pltpu.CompilerParams(vmem_limit_bytes=60 * 1024 * 1024),
        name="expert",
    )(got, gate, up, down)


def back_kernel(
    part, combine, grad, far, near, relay, final, back,
    far_send, far_recv, near_send, near_recv, own_sem, ret_send, ret_recv, all_send, all_recv,
):
    s = lax.axis_index("sp")
    x = lax.axis_index("tp")
    right, left, across = (lax.rem(x + k, TPN) for k in (1, 3, 2))
    greet(s, x)

    def rows(i):
        return pl.ds(pl.multiple_of(i * 8, 8), 8)

    def cols(c):
        return pl.ds(pl.multiple_of(c * CW, CW), CW)

    def half(side):
        return pl.ds(side * HALF, HALF)

    def to_far(c, side):
        return remote(
            part.at[across, half(side), cols(c)],
            far.at[side, c],
            far_send.at[side, c],
            far_recv.at[side, c],
            (s, (right, left)[side]),
        )

    def to_near_plain(c, side):
        return remote(
            part.at[(right, left)[side], half(1 - side), cols(c)],
            near.at[side, c, half(1 - side), :],
            near_send.at[side, 0, c],
            near_recv.at[side, 0, c],
            (s, (right, left)[side]),
        )

    def to_near_sum(c, side):
        return remote(
            relay.at[side, c],
            near.at[side, c, half(side), :],
            near_send.at[side, 1, c],
            near_recv.at[side, 1, c],
            (s, (right, left)[side]),
        )

    def own_back(c):
        return pltpu.make_async_copy(
            final.at[c, :, rows(s), :], back.at[c, :, rows(s), :], own_sem.at[c]
        )

    def home(c, k, target):
        return remote(
            final.at[c, :, rows(target), :],
            back.at[c, :, rows(s), :],
            ret_send.at[c, k],
            ret_recv.at[c, k],
            (target, x),
        )

    def spread(c, side):
        src = grad.at[x, :, cols(c)]
        return remote(
            src, src, all_send.at[side, 0, c], all_recv.at[side, 0, c], (s, (right, left)[side])
        )

    def spread_on(c, side):
        src = grad.at[(left, right)[side], pl.ds(side * 128, 128), cols(c)]
        return remote(
            src, src, all_send.at[side, 1, c], all_recv.at[side, 1, c], (s, (right, left)[side])
        )

    def stage(t):
        @pl.when(t < CHUNKS)
        def _():
            for side in range(2):
                to_far(t, side).start()
                to_near_plain(t, side).start()

        c1 = t - 1

        @pl.when((c1 >= 0) & (c1 < CHUNKS))
        def _():
            for side in range(2):
                to_far(c1, side).wait_recv()
                mine = part[(right, left)[side], pl.ds(side * HALF, HALF), cols(c1)]
                relay[side, c1] = (far[side, c1].astype(F32) + mine.astype(F32)).astype(BF)
                to_near_sum(c1, side).start()

        c2 = t - 2

        @pl.when((c2 >= 0) & (c2 < CHUNKS))
        def _():
            for side in range(2):
                to_near_plain(c2, side).wait_recv()
                to_near_sum(c2, side).wait_recv()
            total = (
                part[x, :, cols(c2)].astype(F32)
                + near[0, c2].astype(F32)
                + near[1, c2].astype(F32)
            ).astype(BF)
            final[c2, 0] = total[0:256]
            final[c2, 1] = total[256:512]
            final[c2, 2, 0:128, :] = total[512:640]
            final[c2, 2, 128:256, :] = total[512:640]
            own_back(c2).start()
            for k in range(1, SPN):
                home(c2, k, peer(s, k)).start()

        c3 = t - 3

        @pl.when((c3 >= 0) & (c3 < CHUNKS))
        def _():
            own_back(c3).wait()
            loop(1, SPN, lambda k: home(c3, k, s ^ 1).wait_recv())
            summed = contract(combine[...], back[c3].reshape(768, CW), 1, 0)
            grad[x, :, cols(c3)] = summed.astype(BF)
            for side in range(2):
                spread(c3, side).start()

        c4 = t - 4

        @pl.when((c4 >= 0) & (c4 < CHUNKS))
        def _():
            for side in range(2):
                spread(c4, side).wait_recv()
                spread_on(c4, side).start()

    loop(0, CHUNKS + 4, stage)

    def finish(c):
        for side in range(2):
            to_far(c, side).wait_send()
            to_near_plain(c, side).wait_send()
            to_near_sum(c, side).wait_send()
            spread(c, side).wait_send()
            spread_on(c, side).wait_send()
            spread_on(c, side).wait_recv()
        loop(1, SPN, lambda k: home(c, k, s ^ 1).wait_send())

    loop(0, CHUNKS, finish)


def send_back(part, combine):
    return pl.pallas_call(
        back_kernel,
        in_specs=[VM, VM],
        out_specs=VM,
        out_shape=jax.ShapeDtypeStruct((TPN, TOK, QW), BF),
        scratch_shapes=[
            pltpu.VMEM((2, CHUNKS, HALF, CW), BF),
            pltpu.VMEM((2, CHUNKS, 2 * HALF, CW), BF),
            pltpu.VMEM((2, CHUNKS, HALF, CW), BF),
            pltpu.VMEM((CHUNKS, 3, 256, CW), BF),
            pltpu.VMEM((CHUNKS, 3, 256, CW), BF),
            pltpu.SemaphoreType.DMA((2, CHUNKS)),
            pltpu.SemaphoreType.DMA((2, CHUNKS)),
            pltpu.SemaphoreType.DMA((2, 2, CHUNKS)),
            pltpu.SemaphoreType.DMA((2, 2, CHUNKS)),
            pltpu.SemaphoreType.DMA((CHUNKS,)),
            pltpu.SemaphoreType.DMA((CHUNKS, SPN)),
            pltpu.SemaphoreType.DMA((CHUNKS, SPN)),
            pltpu.SemaphoreType.DMA((2, 2, CHUNKS)),
            pltpu.SemaphoreType.DMA((2, 2, CHUNKS)),
        ],
        compiler_params=pltpu.CompilerParams(
            collective_id=1, has_side_effects=True, vmem_limit_bytes=48 * 1024 * 1024
        ),
        name="send_back",
    )(part, combine)


def expm1_negative(v):
    series = 1.0 + v * (1.0 / 9.0)
    for k in (8, 7, 6, 5, 4, 3, 2):
        series = 1.0 + v * (1.0 / k) * series
    return jnp.where(v > -0.5, v * series, jnp.exp(v) - 1.0)


def scan_rows(coeff, value, reverse):
    rows = lax.broadcasted_iota(I32, coeff.shape, 0)
    for k in (1, 2, 4, 8, 16, 32, 64, 128):
        if reverse:
            inside = rows < TOK - k
            shift = TOK - k
        else:
            inside = rows >= k
            shift = k
        coeff_far = jnp.where(inside, pltpu.roll(coeff, shift, 0), 1.0)
        value_far = jnp.where(inside, pltpu.roll(value, shift, 0), 0.0)
        value = value + coeff * value_far
        coeff = coeff * coeff_far
    return coeff, value


def mixer_kernel(
    stream, out_grad, gain, grad, states, branch, out_proj, conv, decay_map, input_map, base, shift,
    branch_grad, proj_part, ends, linear, sgb, dot, scale, lru,
):
    def squares(q, carry):
        v = stream[:, pl.ds(pl.multiple_of(q * QW, QW), QW)].astype(F32)
        g = gain[:, pl.ds(pl.multiple_of(q * QW, QW), QW)].astype(F32)
        w = v * (g * grad[q].astype(F32))
        return (
            carry[0] + jnp.sum(v * v, axis=1, keepdims=True),
            carry[1] + jnp.sum(w, axis=1, keepdims=True),
        )

    zero = jnp.zeros((TOK, 1), F32)
    square, along = lax.fori_loop(0, TPN, squares, (zero, zero))
    inverse = 1.0 / (TPN * QW)
    row_scale = lax.rsqrt(square * inverse + norm_eps)
    scale[...] = jnp.broadcast_to(row_scale, (TOK, 128))
    dot[...] = jnp.broadcast_to(along * row_scale * inverse, (TOK, 128))

    def rows_grad(q, carry):
        cols = pl.ds(pl.multiple_of(q * QW, QW), QW)
        r = scale[:, 0:1]
        unit = stream[:, cols].astype(F32) * r
        scaled = gain[:, cols].astype(F32) * grad[q].astype(F32)
        v = (out_grad[:, cols].astype(F32) + r * (scaled - unit * dot[:, 0:1])).astype(BF)
        sgb[:, cols] = v
        return carry + contract(v, out_proj[cols, :], 1, 0)

    lru_grad = lax.fori_loop(0, TPN, rows_grad, jnp.zeros((TOK, FFQ), F32))
    total = states[0] + states[1]
    b = branch[...].astype(F32)
    root = 0.7978845608028654
    tanh = jnp.tanh(root * (b + 0.044715 * b * b * b))
    gelu = 0.5 * b * (1.0 + tanh)
    slope = 0.5 * (1.0 + tanh) + 0.5 * b * (1.0 - tanh * tanh) * root * (
        1.0 + 3.0 * 0.044715 * b * b
    )
    lru[...] = (total * gelu).astype(BF)
    branch_grad[...] = lru_grad * total * slope
    state_grad = lru_grad * gelu

    def proj(q):
        cols = pl.ds(pl.multiple_of(q * QW, QW), QW)
        proj_part[pl.ds(q * 8, 8)] = contract(sgb[:, cols], lru[...], 0, 0).astype(BF).reshape(
            8, 128, FFQ
        )

    loop(0, TPN, proj)
    c = conv[...].astype(F32)
    rows = lax.broadcasted_iota(I32, (TOK, FFQ), 0)
    for d in range(2):
        r = jax.nn.sigmoid(contract(conv[...], decay_map[d], 1, 0))
        i = jax.nn.sigmoid(contract(conv[...], input_map[d], 1, 0))
        rate = (-rate_scale) * base[d : d + 1, :]
        log_decay = r * rate + shift[d]
        decay = jnp.exp(log_decay)
        width = jnp.sqrt(-expm1_negative(2.0 * log_decay))
        drive = width * i * c
        if d == 0:
            coeff = jnp.where(rows == TOK - 1, 1.0, pltpu.roll(decay, TOK - 1, 0))
            edge = slice(0, 1)
        else:
            coeff = jnp.where(rows == 0, 1.0, pltpu.roll(decay, 1, 0))
            edge = slice(TOK - 1, TOK)
        reach, inner = scan_rows(coeff, state_grad, d == 0)
        ends[2 * d : 2 * d + 1, :] = decay[edge] * reach[edge]
        ends[2 * d + 1 : 2 * d + 2, :] = decay[edge] * inner[edge]
        linear[d, 0] = reach
        linear[d, 1] = inner
        linear[d, 2] = width * i
        linear[d, 3] = ((states[d] - drive) - i * c * decay * decay / width) * rate * r * (1.0 - r)
        linear[d, 4] = width * c * i * (1.0 - i)
    ends[4:8, :] = jnp.zeros((4, FFQ), F32)


def mixer(*operands):
    return pl.pallas_call(
        mixer_kernel,
        in_specs=[VM] * 12,
        out_specs=[VM] * 4,
        out_shape=[
            jax.ShapeDtypeStruct((TOK, FFQ), F32),
            jax.ShapeDtypeStruct((SPN, 128, FFQ), BF),
            jax.ShapeDtypeStruct((8, FFQ), F32),
            jax.ShapeDtypeStruct((2, 5, TOK, FFQ), F32),
        ],
        scratch_shapes=[
            pltpu.VMEM((TOK, TPN * QW), BF),
            pltpu.VMEM((TOK, 128), F32),
            pltpu.VMEM((TOK, 128), F32),
            pltpu.VMEM((TOK, FFQ), BF),
        ],
        compiler_params=pltpu.CompilerParams(vmem_limit_bytes=56 * 1024 * 1024),
        name="mixer",
    )(*operands)


def across_kernel(
    ends, proj_part, linear, decay_map, input_map, conv_grad, proj_grad, edges, pieces,
    end_send, end_recv, piece_send, piece_recv, own_sem,
):
    s = lax.axis_index("sp")
    x = lax.axis_index("tp")
    greet(s, x)

    def ends_to(d):
        return remote(ends, edges.at[s], end_send.at[d], end_recv.at[d], (s ^ d, x))

    def piece_to(turn, k, target):
        half = pl.ds(turn * 64, 64)
        return remote(
            proj_part.at[target, half, :],
            pieces.at[s, half, :],
            piece_send.at[turn, k],
            piece_recv.at[turn, k],
            (target, x),
        )

    loop(1, SPN, lambda d: ends_to(d).start())
    for turn in range(2):
        for k in range(1, SPN):
            piece_to(turn, k, peer(s, k)).start()
    own = pltpu.make_async_copy(proj_part.at[s], pieces.at[s], own_sem)
    own.start()
    edges[s] = ends[...]
    loop(1, SPN, lambda d: ends_to(d).wait_recv())

    def carry_in(j, carry):
        later = SPN - 1 - j
        e0, e1 = edges[later], edges[j]
        from_right = jnp.where(later > s, e0[1:2] + e0[0:1] * carry[0], carry[0])
        from_left = jnp.where(j < s, e1[3:4] + e1[2:3] * carry[1], carry[1])
        return from_right, from_left

    zero = jnp.zeros((1, FFQ), F32)
    incoming = lax.fori_loop(0, SPN, carry_in, (zero, zero))
    highest = lax.Precision.HIGHEST
    total = jnp.zeros((TOK, FFQ), F32)
    for d in range(2):
        adjoint = linear[d, 1] + linear[d, 0] * incoming[d]
        total = total + (
            adjoint * linear[d, 2]
            + contract(adjoint * linear[d, 3], decay_map[d].astype(F32), 1, 1, highest)
            + contract(adjoint * linear[d, 4], input_map[d].astype(F32), 1, 1, highest)
        )
    conv_grad[...] = total
    own.wait()

    def landed(k):
        for turn in range(2):
            piece_to(turn, k, s ^ 1).wait_recv()

    loop(1, SPN, landed)
    proj_grad[...] = lax.fori_loop(
        1, SPN, lambda i, acc: acc + pieces[i].astype(F32), pieces[0].astype(F32)
    )

    def finish(k):
        ends_to(k).wait_send()
        for turn in range(2):
            piece_to(turn, k, s ^ 1).wait_send()

    loop(1, SPN, finish)


def across(ends, proj_part, linear, decay_map, input_map):
    return pl.pallas_call(
        across_kernel,
        in_specs=[VM] * 5,
        out_specs=[VM] * 2,
        out_shape=[
            jax.ShapeDtypeStruct((TOK, FFQ), F32),
            jax.ShapeDtypeStruct((128, FFQ), F32),
        ],
        scratch_shapes=[
            pltpu.VMEM((SPN, 8, FFQ), F32),
            pltpu.VMEM((SPN, 128, FFQ), BF),
            pltpu.SemaphoreType.DMA((SPN,)),
            pltpu.SemaphoreType.DMA((SPN,)),
            pltpu.SemaphoreType.DMA((2, SPN)),
            pltpu.SemaphoreType.DMA((2, SPN)),
            pltpu.SemaphoreType.DMA,
        ],
        compiler_params=pltpu.CompilerParams(
            collective_id=2, has_side_effects=True, vmem_limit_bytes=40 * 1024 * 1024
        ),
        name="across",
    )(ends, proj_part, linear, decay_map, input_map)


def body(
    out_grad,
    stream,
    norm_gain,
    routes,
    route_weight,
    gate_weight,
    up_weight,
    down_weight,
    out_proj,
    conv_out,
    gate_branch,
    decay_map,
    input_map,
    decay_param,
    decay_shift,
    states,
):
    send, combine = prep(stream, out_grad, norm_gain[None, :], routes, route_weight)
    got = dispatch(send)
    part, gate_wgrad, up_wgrad, down_wgrad = expert(
        got, gate_weight[0], up_weight[0], down_weight[0]
    )
    grad = send_back(part, combine)
    base = jax.nn.softplus(-decay_param)
    decay_maps, input_maps = decay_map[:, 0], input_map[:, 0]
    branch_grad, proj_part, ends, linear = mixer(
        stream, out_grad, norm_gain[None, :], grad, states, gate_branch, out_proj, conv_out,
        decay_maps, input_maps, base, decay_shift,
    )
    conv_grad, proj_grad = across(ends, proj_part, linear, decay_maps, input_maps)
    return (
        conv_grad, branch_grad, proj_grad, gate_wgrad[None], up_wgrad[None], down_wgrad[None]
    )


def solution(mesh):
    in_specs = (
        P(SP, None),
        P(SP, None),
        P(),
        P(SP, None),
        P(SP, None),
        P(SP, None, "tp"),
        P(SP, None, "tp"),
        P(SP, "tp", None),
        P(None, "tp"),
        P(SP, "tp"),
        P(SP, "tp"),
        P(None, "tp", None, None),
        P(None, "tp", None, None),
        P(None, "tp"),
        P(None, SP, "tp"),
        P(None, SP, "tp"),
    )
    out_specs = (
        P(SP, "tp"),
        P(SP, "tp"),
        P(SP, "tp"),
        P(SP, None, "tp"),
        P(SP, None, "tp"),
        P(SP, "tp", None),
    )
    return jax.shard_map(body, mesh=mesh, in_specs=in_specs, out_specs=out_specs, check_vma=False)
```

```python
import functools

import jax
import jax.numpy as jnp
from jax import lax
from jax.experimental import pallas as pl
from jax.experimental.pallas import tpu as pltpu
from jax.sharding import PartitionSpec as P

BF = jnp.bfloat16
F32 = jnp.float32
I32 = jnp.int32
MESH = pl.DeviceIdType.MESH
ANY = pl.BlockSpec(memory_space=pl.ANY)
VM = pl.BlockSpec(memory_space=pltpu.VMEM)

SPN = 32
TPN = 4
TOK = 256
QW = 1024
FFQ = 256
CHUNKS = 4
SP = "sp"
CW = QW // CHUNKS
HALF = 320
rate_scale = 8.0
norm_eps = 1e-06


def contract(left, right, left_dim, right_dim, precision=None):
    return lax.dot_general(
        left,
        right,
        (((left_dim,), (right_dim,)), ((), ())),
        preferred_element_type=F32,
        precision=precision,
    )


def prep_kernel(stream, out_grad, gain, routes, weight, send, combine, qi, qc0, qc1, scale):
    h = pl.program_id(0)
    low = lax.axis_index("tp") % 2

    @pl.when(h == 0)
    def _():
        wide = stream[...].astype(F32)
        mean = jnp.sum(wide * wide, axis=1, keepdims=True) * (1.0 / (TPN * QW))
        scale[...] = jnp.broadcast_to(lax.rsqrt(mean + norm_eps), (TOK, 128))
        lanes = lax.broadcasted_iota(I32, (TOK, 128), 1)
        r0, r1 = routes[:, 0:1], routes[:, 1:2]
        hot0 = (r0 == lanes).astype(F32)
        hot1 = (r1 == lanes).astype(F32)
        before = (
            lax.broadcasted_iota(I32, (TOK, TOK), 1) < lax.broadcasted_iota(I32, (TOK, TOK), 0)
        ).astype(F32)
        counts = contract(before.astype(BF), (hot0 + hot1).astype(BF), 1, 0)
        upper = lax.axis_index("sp") // 16
        slots = lax.broadcasted_iota(I32, (TOK, 768), 1)

        def places(route, hot):
            rank = jnp.sum(counts * hot, axis=1, keepdims=True).astype(I32)
            pure = (rank // 8) * 256 + route * 8 + rank % 8
            mixed = 512 + route * 8 + (rank - 16)
            of_input = jnp.where(rank < 16, pure, mixed + 4 * upper)
            of_cotan = jnp.where(rank < 16, pure, mixed + 4 * (1 - upper))
            return (slots == of_input).astype(F32), (slots == of_cotan).astype(F32)

        in0, cot0 = places(r0, hot0)
        in1, cot1 = places(r1, hot1)
        both = (in0 + in1).astype(BF)
        qi[...] = both
        combine[...] = both
        qc0[...] = cot0.astype(BF)
        qc1[...] = cot1.astype(BF)

    cols = pl.ds(pl.multiple_of((2 * h + low) * QW, QW), QW)
    normed = (stream[:, cols].astype(F32) * scale[:, 0:1] * gain[:, cols].astype(F32)).astype(BF)
    grad = out_grad[:, cols].astype(F32)
    scaled0 = (weight[:, 0:1] * grad).astype(BF)
    scaled1 = (weight[:, 1:2] * grad).astype(BF)
    for plane in range(3):
        span = slice(plane * 256, plane * 256 + 256)
        rows_in = contract(qi[:, span], normed, 0, 0)
        rows_cot = contract(qc0[:, span], scaled0, 0, 0) + contract(qc1[:, span], scaled1, 0, 0)
        if plane < 2:
            send[0, plane] = rows_in.astype(BF)
            send[0, plane + 2] = rows_cot.astype(BF)
        else:
            send[0, 4] = (rows_in + rows_cot).astype(BF)


def prep(stream, out_grad, gain, routes, weight):
    whole = lambda shape: pl.BlockSpec(shape, lambda h: (0,) * len(shape))
    return pl.pallas_call(
        prep_kernel,
        grid=(2,),
        in_specs=[
            whole((TOK, 4 * QW)),
            whole((TOK, 4 * QW)),
            whole((1, 4 * QW)),
            whole((TOK, 2)),
            whole((TOK, 2)),
        ],
        out_specs=[
            pl.BlockSpec((1, 5, 256, QW), lambda h: (h, 0, 0, 0)),
            whole((TOK, 768)),
        ],
        out_shape=[
            jax.ShapeDtypeStruct((2, 5, 256, QW), BF),
            jax.ShapeDtypeStruct((TOK, 768), BF),
        ],
        scratch_shapes=[
            pltpu.VMEM((TOK, 768), BF),
            pltpu.VMEM((TOK, 768), BF),
            pltpu.VMEM((TOK, 768), BF),
            pltpu.VMEM((TOK, 128), F32),
        ],
        compiler_params=pltpu.CompilerParams(vmem_limit_bytes=48 * 1024 * 1024),
        name="prep",
    )(stream, out_grad, gain, routes, weight)


NEAR = (
    (0, 1), (1, 0), (0, 3), (3, 0), (1, 1), (3, 3), (1, 3), (3, 1),
    (0, 2), (2, 0), (1, 2), (2, 1), (3, 2), (2, 3), (2, 2),
)
STEPS = ((0, 0, 1),) + tuple((z, y, c) for c in (0, 1) for z, y in NEAR)


def peer(s, k, sign=1):
    z, y, c = STEPS[k - 1]
    return (
        lax.rem(s // 8 + (z if sign > 0 else 4 - z), 4) * 8
        + lax.rem((s // 2) % 4 + (y if sign > 0 else 4 - y), 4) * 2
        + lax.rem(s % 2 + c, 2)
    )


def greet(s, x):
    hello_all(s, x)
    met()


def met():
    pl.semaphore_wait(pltpu.get_barrier_semaphore(), SPN + 1)


def hello_all(s, x):
    barrier = pltpu.get_barrier_semaphore()

    def hello(d, carry):
        pl.semaphore_signal(barrier, inc=1, device_id=(s ^ d, x), device_id_type=MESH)
        return carry

    lax.fori_loop(1, SPN, hello, 0)
    for step in (1, TPN - 1):
        pl.semaphore_signal(
            barrier, inc=1, device_id=(s, lax.rem(x + step, TPN)), device_id_type=MESH
        )


def remote(src, dst, send_sem, recv_sem, target):
    return pltpu.make_async_remote_copy(
        src_ref=src,
        dst_ref=dst,
        send_sem=send_sem,
        recv_sem=recv_sem,
        device_id=target,
        device_id_type=MESH,
    )


def loop(lower, upper, step):
    def run(d, carry):
        step(d)
        return carry

    lax.fori_loop(lower, upper, run, 0)


def dispatch_kernel(send, got, own_sem, send_sem, recv_sem, fwd_send, fwd_recv):
    s = lax.axis_index("sp")
    x = lax.axis_index("tp")
    high, low = x // 2, x % 2
    right, left = lax.rem(x + 1, TPN), lax.rem(x + TPN - 1, TPN)
    greet(s, x)

    def rows(i):
        return pl.ds(pl.multiple_of(i * 8, 8), 8)

    def over(turn, k, target):
        hi = high if turn == 0 else 1 - high
        return remote(
            send.at[hi, :, rows(target), :],
            got.at[hi, low, :, rows(s), :],
            send_sem.at[turn, k],
            recv_sem.at[turn, k],
            (target, x),
        )

    def onward(src, dst, k, side):
        return remote(
            src, dst, fwd_send.at[side, k], fwd_recv.at[side, k], (s, (right, left)[side])
        )

    def block(i):
        return got.at[high, low, :, rows(i), :]

    own = pltpu.make_async_copy(
        send.at[:, :, rows(s), :], got.at[:, low, :, rows(s), :], own_sem
    )
    own.start()
    for side in range(2):
        onward(send.at[high, :, rows(s), :], block(s), 0, side).start()
    for turn in range(2):
        for k in range(1, SPN):
            over(turn, k, peer(s, k)).start()
    for k in range(1, SPN):
        source = peer(s, k, -1)
        over(0, k, source).wait_recv()
        for side in range(2):
            onward(block(source), block(source), k, side).start()
    own.wait()

    def finish(k):
        for turn in range(2):
            over(turn, k, s ^ 1).wait_send()
        over(1, k, s ^ 1).wait_recv()

    def finish_onward(k):
        for side in range(2):
            copy = onward(block(s), block(s), k, side)
            copy.wait_send()
            copy.wait_recv()

    loop(1, SPN, finish)
    loop(0, SPN, finish_onward)


def dispatch(send):
    return pl.pallas_call(
        dispatch_kernel,
        in_specs=[ANY],
        out_specs=ANY,
        out_shape=jax.ShapeDtypeStruct((2, 2, 5, 256, QW), BF),
        scratch_shapes=[
            pltpu.SemaphoreType.DMA,
            pltpu.SemaphoreType.DMA((2, SPN)),
            pltpu.SemaphoreType.DMA((2, SPN)),
            pltpu.SemaphoreType.DMA((2, SPN)),
            pltpu.SemaphoreType.DMA((2, SPN)),
        ],
        compiler_params=pltpu.CompilerParams(collective_id=0, has_side_effects=True),
        name="dispatch",
    )(send)


def swap_halves(v):
    tiles = v.reshape(16, 8, v.shape[1])
    return pltpu.roll(tiles, 4, 1).reshape(v.shape)


def expert_kernel(
    got, gate, up, down, part, gate_wg, up_wg, down_wg,
    vin, vcot, vmix, vg, vu, vd, vpart, ogu, od, gp, upre, hg, gu, hid,
    in_sem, w_sem, part_sem, o_sem,
):
    def loads(q):
        hi, lo = q // 2, q % 2
        out = []
        for plane in range(5):
            if plane < 2:
                dst = vin.at[q, pl.ds(plane * 256, 256), :]
            elif plane < 4:
                dst = vcot.at[q, pl.ds((plane - 2) * 256, 256), :]
            else:
                dst = vmix.at[q]
            out.append(pltpu.make_async_copy(got.at[hi, lo, plane], dst, in_sem.at[q, plane]))
        rows = pl.ds(pl.multiple_of(q * QW, QW), QW)
        out.append(pltpu.make_async_copy(gate.at[rows, :], vg.at[q], w_sem.at[0, q]))
        out.append(pltpu.make_async_copy(up.at[rows, :], vu.at[q], w_sem.at[1, q]))
        out.append(pltpu.make_async_copy(down.at[:, rows], vd.at[q], w_sem.at[2, q]))
        return out

    loop(0, TPN, lambda q: [c.start() for c in loads(q)])
    gp[...] = jnp.zeros_like(gp)
    upre[...] = jnp.zeros_like(upre)
    hg[...] = jnp.zeros_like(hg)

    def forward(q):
        for c in loads(q):
            c.wait()
        first = lax.broadcasted_iota(I32, (128, QW), 0) % 8 < 4
        a = vmix[q, 0:128, :].astype(F32)
        b = vmix[q, 128:256, :].astype(F32)
        vin[q, 512:640, :] = jnp.where(first, a, b).astype(BF)
        vcot[q, 512:640, :] = jnp.where(first, b, a).astype(BF)
        rows = vin[q]
        gp[...] += contract(rows, vg[q], 1, 0)
        upre[...] += contract(rows, vu[q], 1, 0)
        hg[...] += contract(vcot[q], vd[q], 1, 1)

    loop(0, TPN, forward)
    hg[512:640, :] = swap_halves(hg[512:640, :])
    gate_pre, up_pre, hidden_grad = gp[...], upre[...], hg[...]
    logistic = jax.nn.sigmoid(gate_pre)
    silu = gate_pre * logistic
    hidden = silu * up_pre
    hid[0:512, :] = hidden[0:512, :].astype(BF)
    hid[512:640, :] = swap_halves(hidden[512:640, :]).astype(BF)
    gu[:, 0:FFQ] = (
        hidden_grad * up_pre * (logistic * (1.0 + gate_pre * (1.0 - logistic)))
    ).astype(BF)
    gu[:, FFQ : 2 * FFQ] = (hidden_grad * silu).astype(BF)

    def part_out(q):
        return pltpu.make_async_copy(vpart.at[q], part.at[q], part_sem.at[q])

    def back(q):
        vpart[q] = (
            contract(gu[:, 0:FFQ], vg[q], 1, 1) + contract(gu[:, FFQ : 2 * FFQ], vu[q], 1, 1)
        ).astype(BF)
        part_out(q).start()

    loop(0, TPN, back)

    def grads_out(q):
        rows = pl.ds(pl.multiple_of(q * QW, QW), QW)
        return (
            pltpu.make_async_copy(ogu.at[0, q], gate_wg.at[rows, :], o_sem.at[0, q]),
            pltpu.make_async_copy(ogu.at[1, q], up_wg.at[rows, :], o_sem.at[1, q]),
            pltpu.make_async_copy(od.at[q], down_wg.at[:, rows], o_sem.at[2, q]),
        )

    def weights(q):
        both = contract(vin[q], gu[...], 0, 0)
        ogu[0, q] = both[:, 0:FFQ].astype(BF)
        ogu[1, q] = both[:, FFQ : 2 * FFQ].astype(BF)
        od[q] = contract(hid[...], vcot[q], 0, 0).astype(BF)
        for c in grads_out(q):
            c.start()

    loop(0, TPN, weights)
    loop(0, TPN, lambda q: part_out(q).wait())
    loop(0, TPN, lambda q: [c.wait() for c in grads_out(q)])


def expert(got, gate, up, down):
    full = TPN * QW
    return pl.pallas_call(
        expert_kernel,
        in_specs=[ANY] * 4,
        out_specs=[ANY] * 4,
        out_shape=[
            jax.ShapeDtypeStruct((TPN, 640, QW), BF),
            jax.ShapeDtypeStruct((full, FFQ), BF),
            jax.ShapeDtypeStruct((full, FFQ), BF),
            jax.ShapeDtypeStruct((FFQ, full), BF),
        ],
        scratch_shapes=[
            pltpu.VMEM((TPN, 640, QW), BF),
            pltpu.VMEM((TPN, 640, QW), BF),
            pltpu.VMEM((TPN, 256, QW), BF),
            pltpu.VMEM((TPN, QW, FFQ), BF),
            pltpu.VMEM((TPN, QW, FFQ), BF),
            pltpu.VMEM((TPN, FFQ, QW), BF),
            pltpu.VMEM((TPN, 640, QW), BF),
            pltpu.VMEM((2, TPN, QW, FFQ), BF),
            pltpu.VMEM((TPN, FFQ, QW), BF),
            pltpu.VMEM((640, FFQ), F32),
            pltpu.VMEM((640, FFQ), F32),
            pltpu.VMEM((640, FFQ), F32),
            pltpu.VMEM((640, 2 * FFQ), BF),
            pltpu.VMEM((640, FFQ), BF),
            pltpu.SemaphoreType.DMA((TPN, 5)),
            pltpu.SemaphoreType.DMA((3, TPN)),
            pltpu.SemaphoreType.DMA((TPN,)),
            pltpu.SemaphoreType.DMA((3, TPN)),
        ],
        compiler_params=pltpu.CompilerParams(vmem_limit_bytes=60 * 1024 * 1024),
        name="expert",
    )(got, gate, up, down)


def back_kernel(
    part, combine, grad, far, near, relay, final, back,
    far_send, far_recv, near_send, near_recv, own_sem, ret_send, ret_recv, all_send, all_recv,
):
    s = lax.axis_index("sp")
    x = lax.axis_index("tp")
    right, left, across = (lax.rem(x + k, TPN) for k in (1, 3, 2))
    greet(s, x)

    def rows(i):
        return pl.ds(pl.multiple_of(i * 8, 8), 8)

    def cols(c):
        return pl.ds(pl.multiple_of(c * CW, CW), CW)

    def half(side):
        return pl.ds(side * HALF, HALF)

    def to_far(c, side):
        return remote(
            part.at[across, half(side), cols(c)],
            far.at[side, c],
            far_send.at[side, c],
            far_recv.at[side, c],
            (s, (right, left)[side]),
        )

    def to_near_plain(c, side):
        return remote(
            part.at[(right, left)[side], half(1 - side), cols(c)],
            near.at[side, c, half(1 - side), :],
            near_send.at[side, 0, c],
            near_recv.at[side, 0, c],
            (s, (right, left)[side]),
        )

    def to_near_sum(c, side):
        return remote(
            relay.at[side, c],
            near.at[side, c, half(side), :],
            near_send.at[side, 1, c],
            near_recv.at[side, 1, c],
            (s, (right, left)[side]),
        )

    def own_back(c):
        return pltpu.make_async_copy(
            final.at[c, :, rows(s), :], back.at[c, :, rows(s), :], own_sem.at[c]
        )

    def home(c, k, target):
        return remote(
            final.at[c, :, rows(target), :],
            back.at[c, :, rows(s), :],
            ret_send.at[c, k],
            ret_recv.at[c, k],
            (target, x),
        )

    def spread(c, side):
        src = grad.at[x, :, cols(c)]
        return remote(
            src, src, all_send.at[side, 0, c], all_recv.at[side, 0, c], (s, (right, left)[side])
        )

    def spread_on(c, side):
        src = grad.at[(left, right)[side], pl.ds(side * 128, 128), cols(c)]
        return remote(
            src, src, all_send.at[side, 1, c], all_recv.at[side, 1, c], (s, (right, left)[side])
        )

    def stage(t):
        @pl.when(t < CHUNKS)
        def _():
            for side in range(2):
                to_far(t, side).start()
                to_near_plain(t, side).start()

        c1 = t - 1

        @pl.when((c1 >= 0) & (c1 < CHUNKS))
        def _():
            for side in range(2):
                to_far(c1, side).wait_recv()
                mine = part[(right, left)[side], pl.ds(side * HALF, HALF), cols(c1)]
                relay[side, c1] = (far[side, c1].astype(F32) + mine.astype(F32)).astype(BF)
                to_near_sum(c1, side).start()

        c2 = t - 2

        @pl.when((c2 >= 0) & (c2 < CHUNKS))
        def _():
            for side in range(2):
                to_near_plain(c2, side).wait_recv()
                to_near_sum(c2, side).wait_recv()
            total = (
                part[x, :, cols(c2)].astype(F32)
                + near[0, c2].astype(F32)
                + near[1, c2].astype(F32)
            ).astype(BF)
            final[c2, 0] = total[0:256]
            final[c2, 1] = total[256:512]
            final[c2, 2, 0:128, :] = total[512:640]
            final[c2, 2, 128:256, :] = total[512:640]
            own_back(c2).start()
            for k in range(1, SPN):
                home(c2, k, peer(s, k)).start()

        c3 = t - 3

        @pl.when((c3 >= 0) & (c3 < CHUNKS))
        def _():
            own_back(c3).wait()
            loop(1, SPN, lambda k: home(c3, k, s ^ 1).wait_recv())
            summed = contract(combine[...], back[c3].reshape(768, CW), 1, 0)
            grad[x, :, cols(c3)] = summed.astype(BF)
            for side in range(2):
                spread(c3, side).start()

        c4 = t - 4

        @pl.when((c4 >= 0) & (c4 < CHUNKS))
        def _():
            for side in range(2):
                spread(c4, side).wait_recv()
                spread_on(c4, side).start()

    loop(0, CHUNKS + 4, stage)

    def finish(c):
        for side in range(2):
            to_far(c, side).wait_send()
            to_near_plain(c, side).wait_send()
            to_near_sum(c, side).wait_send()
            spread(c, side).wait_send()
            spread_on(c, side).wait_send()
            spread_on(c, side).wait_recv()
        loop(1, SPN, lambda k: home(c, k, s ^ 1).wait_send())

    loop(0, CHUNKS, finish)


def send_back(part, combine):
    return pl.pallas_call(
        back_kernel,
        in_specs=[VM, VM],
        out_specs=VM,
        out_shape=jax.ShapeDtypeStruct((TPN, TOK, QW), BF),
        scratch_shapes=[
            pltpu.VMEM((2, CHUNKS, HALF, CW), BF),
            pltpu.VMEM((2, CHUNKS, 2 * HALF, CW), BF),
            pltpu.VMEM((2, CHUNKS, HALF, CW), BF),
            pltpu.VMEM((CHUNKS, 3, 256, CW), BF),
            pltpu.VMEM((CHUNKS, 3, 256, CW), BF),
            pltpu.SemaphoreType.DMA((2, CHUNKS)),
            pltpu.SemaphoreType.DMA((2, CHUNKS)),
            pltpu.SemaphoreType.DMA((2, 2, CHUNKS)),
            pltpu.SemaphoreType.DMA((2, 2, CHUNKS)),
            pltpu.SemaphoreType.DMA((CHUNKS,)),
            pltpu.SemaphoreType.DMA((CHUNKS, SPN)),
            pltpu.SemaphoreType.DMA((CHUNKS, SPN)),
            pltpu.SemaphoreType.DMA((2, 2, CHUNKS)),
            pltpu.SemaphoreType.DMA((2, 2, CHUNKS)),
        ],
        compiler_params=pltpu.CompilerParams(
            collective_id=1, has_side_effects=True, vmem_limit_bytes=48 * 1024 * 1024
        ),
        name="send_back",
    )(part, combine)


def expm1_negative(v):
    series = 1.0 + v * (1.0 / 9.0)
    for k in (8, 7, 6, 5, 4, 3, 2):
        series = 1.0 + v * (1.0 / k) * series
    return jnp.where(v > -0.5, v * series, jnp.exp(v) - 1.0)


def scan_rows(coeff, value, reverse):
    rows = lax.broadcasted_iota(I32, coeff.shape, 0)
    for k in (1, 2, 4, 8, 16, 32, 64, 128):
        if reverse:
            inside = rows < TOK - k
            shift = TOK - k
        else:
            inside = rows >= k
            shift = k
        coeff_far = jnp.where(inside, pltpu.roll(coeff, shift, 0), 1.0)
        value_far = jnp.where(inside, pltpu.roll(value, shift, 0), 0.0)
        value = value + coeff * value_far
        coeff = coeff * coeff_far
    return coeff, value


def mixer_kernel(
    stream, out_grad, gain, grad, states, branch, out_proj, conv, decay_map, input_map, base, shift,
    branch_grad, conv_grad, proj_grad,
    v_stream, v_out, v_grad, v_proj, v_states, v_shift, v_branch, v_conv, v_decay, v_input,
    sgb, dot, scale, lru, pulled, linear, coeffs,
    ends, edges, pieces, pair, paired, far_y, far_z, sum_y, sum_z, last_y, last_z,
    big_sem, small_sem, end_send, end_recv, pair_send, pair_recv, one_send, one_recv,
    two_send, two_recv,
):
    s = lax.axis_index("sp")
    x = lax.axis_index("tp")
    z, y, core = s // 8, (s // 2) % 4, s % 2
    hello_all(s, x)

    def big(which, q):
        cols = pl.ds(pl.multiple_of(q * QW, QW), QW)
        src, dst = (
            (stream.at[:, cols], v_stream.at[q]),
            (grad.at[q], v_grad.at[q]),
            (out_grad.at[:, cols], v_out.at[q]),
            (out_proj.at[cols, :], v_proj.at[q]),
        )[which]
        return pltpu.make_async_copy(src, dst, big_sem.at[which, q])

    small = [
        pltpu.make_async_copy(src, dst, small_sem.at[k])
        for k, (src, dst) in enumerate(
            (
                (conv, v_conv),
                (decay_map, v_decay),
                (input_map, v_input),
                (shift, v_shift),
                (states, v_states),
                (branch, v_branch),
            )
        )
    ]
    for copy in small:
        copy.start()

    def begin(q):
        for which in range(4):
            big(which, q).start()

    loop(0, TPN, begin)
    for copy in small:
        copy.wait()

    c = v_conv[...].astype(F32)
    rows = lax.broadcasted_iota(I32, (TOK, FFQ), 0)
    for d in range(2):
        r = jax.nn.sigmoid(contract(v_conv[...], v_decay[d], 1, 0))
        i = jax.nn.sigmoid(contract(v_conv[...], v_input[d], 1, 0))
        rate = (-rate_scale) * base[d : d + 1, :]
        log_decay = r * rate + v_shift[d]
        decay = jnp.exp(log_decay)
        width = jnp.sqrt(-expm1_negative(2.0 * log_decay))
        drive = width * i * c
        if d == 0:
            coeffs[d] = jnp.where(rows == TOK - 1, 1.0, pltpu.roll(decay, TOK - 1, 0))
            ends[0:1, :] = decay[0:1]
        else:
            coeffs[d] = jnp.where(rows == 0, 1.0, pltpu.roll(decay, 1, 0))
            ends[2:3, :] = decay[TOK - 1 : TOK]
        linear[d, 0] = width * i
        linear[d, 1] = (
            ((v_states[d] - drive) - i * c * decay * decay / width) * rate * r * (1.0 - r)
        )
        linear[d, 2] = width * c * i * (1.0 - i)

    def squares(q, carry):
        big(0, q).wait()
        big(1, q).wait()
        v = v_stream[q].astype(F32)
        g = gain[:, pl.ds(pl.multiple_of(q * QW, QW), QW)].astype(F32)
        w = v * (g * v_grad[q].astype(F32))
        return (
            carry[0] + jnp.sum(v * v, axis=1, keepdims=True),
            carry[1] + jnp.sum(w, axis=1, keepdims=True),
        )

    zero = jnp.zeros((TOK, 1), F32)
    square, along = lax.fori_loop(0, TPN, squares, (zero, zero))
    inverse = 1.0 / (TPN * QW)
    row_scale = lax.rsqrt(square * inverse + norm_eps)
    scale[...] = jnp.broadcast_to(row_scale, (TOK, 128))
    dot[...] = jnp.broadcast_to(along * row_scale * inverse, (TOK, 128))
    pulled[...] = jnp.zeros_like(pulled)

    def rows_grad(q):
        big(2, q).wait()
        big(3, q).wait()
        r = scale[:, 0:1]
        unit = v_stream[q].astype(F32) * r
        scaled = gain[:, pl.ds(pl.multiple_of(q * QW, QW), QW)].astype(F32) * v_grad[q].astype(F32)
        v = (v_out[q].astype(F32) + r * (scaled - unit * dot[:, 0:1])).astype(BF)
        sgb[q] = v
        pulled[...] += contract(v, v_proj[q], 1, 0)

    loop(0, TPN, rows_grad)
    lru_grad = pulled[...]
    total = v_states[0] + v_states[1]
    b = v_branch[...].astype(F32)
    root = 0.7978845608028654
    tanh = jnp.tanh(root * (b + 0.044715 * b * b * b))
    gelu = 0.5 * b * (1.0 + tanh)
    slope = 0.5 * (1.0 + tanh) + 0.5 * b * (1.0 - tanh * tanh) * root * (
        1.0 + 3.0 * 0.044715 * b * b
    )
    lru[...] = (total * gelu).astype(BF)
    branch_grad[...] = lru_grad * total * slope
    state_grad = lru_grad * gelu
    for d in range(2):
        reach, inner = scan_rows(coeffs[d], state_grad, d == 0)
        edge = slice(0, 1) if d == 0 else slice(TOK - 1, TOK)
        decay = ends[2 * d : 2 * d + 1, :]
        ends[2 * d : 2 * d + 1, :] = decay * reach[edge]
        ends[2 * d + 1 : 2 * d + 2, :] = decay * inner[edge]
        linear[d, 3] = reach
        linear[d, 4] = inner

    def ends_to(k, target):
        return remote(ends, edges.at[s], end_send.at[k], end_recv.at[k], (target, x))

    met()
    for k in range(1, SPN):
        ends_to(k, peer(s, k)).start()
    edges[s] = ends[...]

    def pair_to(q):
        return remote(
            pieces.at[q, :, 1 - core],
            pair.at[q],
            pair_send.at[q],
            pair_recv.at[q],
            (s + 1 - 2 * core, x),
        )

    def proj(q):
        pieces[q] = (
            contract(sgb[q], lru[...], 0, 0).astype(BF).reshape(TPN, 2, 128, FFQ)
        )
        pair_to(q).start()

    loop(0, TPN, proj)

    def meet(q):
        pair_to(q).wait_recv()
        paired[q] = (pieces[q, :, core].astype(F32) + pair[q].astype(F32)).astype(BF)

    loop(0, TPN, meet)
    first, second = pl.ds(0, 64), pl.ds(64, 64)

    def along_y(k):
        return lax.rem(y + k, 4), (z * 8 + lax.rem(y + k, 4) * 2 + core, x)

    def along_z(k):
        return lax.rem(z + k, 4), (lax.rem(z + k, 4) * 8 + y * 2 + core, x)

    def one(side, k):
        place, target = (along_y, along_z)[side](k)
        if side == 0:
            src, dst = paired.at[:, place, first, :], far_y.at[k - 1]
        else:
            src, dst = paired.at[place, :, second, :], far_z.at[k - 1]
        return remote(src, dst, one_send.at[side, k], one_recv.at[side, k], target)

    def two(side, k):
        place, target = (along_z, along_y)[side](k)
        if side == 0:
            src, dst = sum_y.at[place], last_y.at[k - 1]
        else:
            src, dst = sum_z.at[place], last_z.at[k - 1]
        return remote(src, dst, two_send.at[side, k], two_recv.at[side, k], target)

    for k in (1, 3, 2):
        for side in range(2):
            one(side, k).start()

    for k in range(1, SPN):
        ends_to(k, s ^ 1).wait_recv()

    def carry_in(j, carry):
        later = SPN - 1 - j
        e0, e1 = edges[later], edges[j]
        from_right = jnp.where(later > s, e0[1:2] + e0[0:1] * carry[0], carry[0])
        from_left = jnp.where(j < s, e1[3:4] + e1[2:3] * carry[1], carry[1])
        return from_right, from_left

    none = jnp.zeros((1, FFQ), F32)
    incoming = lax.fori_loop(0, SPN, carry_in, (none, none))

    def back_maps(d):
        adjoint = linear[d, 4] + linear[d, 3] * incoming[d]
        highest = lax.Precision.HIGHEST
        return (
            adjoint * linear[d, 0]
            + contract(adjoint * linear[d, 1], v_decay[d].astype(F32), 1, 1, highest)
            + contract(adjoint * linear[d, 2], v_input[d].astype(F32), 1, 1, highest)
        )

    conv_grad[...] = back_maps(0) + back_maps(1)

    for side in range(2):
        for k in (1, 3, 2):
            one(side, k).wait_recv()
        if side == 0:
            acc = paired[:, y, first, :].astype(F32)
        else:
            acc = paired[z, :, second, :].astype(F32)
        came = (far_y, far_z)[side]
        acc = acc + came[0].astype(F32) + came[1].astype(F32) + came[2].astype(F32)
        (sum_y, sum_z)[side][...] = acc.astype(BF)
        for k in (1, 3, 2):
            two(side, k).start()

    for side in range(2):
        for k in (1, 3, 2):
            two(side, k).wait_recv()
        came = (last_y, last_z)[side]
        acc = (sum_y[z] if side == 0 else sum_z[y]).astype(F32)
        acc = acc + came[0].astype(F32) + came[1].astype(F32) + came[2].astype(F32)
        proj_grad[pl.ds(side * 64, 64), :] = acc

    for side in range(2):
        for k in (1, 3, 2):
            one(side, k).wait_send()
            two(side, k).wait_send()
    loop(1, SPN, lambda k: ends_to(k, s ^ 1).wait_send())
    loop(0, TPN, lambda q: pair_to(q).wait_send())


def mixer(*operands):
    whole = (TPN, TOK, QW)
    square = (TOK, FFQ)
    dma = pltpu.SemaphoreType.DMA
    return pl.pallas_call(
        mixer_kernel,
        in_specs=[ANY, ANY, VM, ANY, ANY, ANY, ANY, ANY, ANY, ANY, VM, ANY],
        out_specs=[VM] * 3,
        out_shape=[
            jax.ShapeDtypeStruct(square, F32),
            jax.ShapeDtypeStruct(square, F32),
            jax.ShapeDtypeStruct((128, FFQ), F32),
        ],
        scratch_shapes=[
            pltpu.VMEM(whole, BF),
            pltpu.VMEM(whole, BF),
            pltpu.VMEM(whole, BF),
            pltpu.VMEM((TPN, QW, FFQ), BF),
            pltpu.VMEM((2,) + square, F32),
            pltpu.VMEM((2,) + square, F32),
            pltpu.VMEM(square, BF),
            pltpu.VMEM(square, BF),
            pltpu.VMEM((2, FFQ, FFQ), BF),
            pltpu.VMEM((2, FFQ, FFQ), BF),
            pltpu.VMEM(whole, BF),
            pltpu.VMEM((TOK, 128), F32),
            pltpu.VMEM((TOK, 128), F32),
            pltpu.VMEM(square, BF),
            pltpu.VMEM(square, F32),
            pltpu.VMEM((2, 5) + square, F32),
            pltpu.VMEM((2,) + square, F32),
            pltpu.VMEM((4, FFQ), F32),
            pltpu.VMEM((SPN, 4, FFQ), F32),
            pltpu.VMEM((4, 4, 2, 128, FFQ), BF),
            pltpu.VMEM((4, 4, 128, FFQ), BF),
            pltpu.VMEM((4, 4, 128, FFQ), BF),
            pltpu.VMEM((3, 4, 64, FFQ), BF),
            pltpu.VMEM((3, 4, 64, FFQ), BF),
            pltpu.VMEM((4, 64, FFQ), BF),
            pltpu.VMEM((4, 64, FFQ), BF),
            pltpu.VMEM((3, 64, FFQ), BF),
            pltpu.VMEM((3, 64, FFQ), BF),
            dma((4, TPN)),
            dma((6,)),
            dma((SPN,)),
            dma((SPN,)),
            dma((TPN,)),
            dma((TPN,)),
            dma((2, 4)),
            dma((2, 4)),
            dma((2, 4)),
            dma((2, 4)),
        ],
        compiler_params=pltpu.CompilerParams(
            collective_id=2, has_side_effects=True, vmem_limit_bytes=48 * 1024 * 1024
        ),
        name="mixer",
    )(*operands)


def body(
    out_grad,
    stream,
    norm_gain,
    routes,
    route_weight,
    gate_weight,
    up_weight,
    down_weight,
    out_proj,
    conv_out,
    gate_branch,
    decay_map,
    input_map,
    decay_param,
    decay_shift,
    states,
):
    send, combine = prep(stream, out_grad, norm_gain[None, :], routes, route_weight)
    got = dispatch(send)
    part, gate_wgrad, up_wgrad, down_wgrad = expert(
        got, gate_weight[0], up_weight[0], down_weight[0]
    )
    grad = send_back(part, combine)
    base = jax.nn.softplus(-decay_param)
    branch_grad, conv_grad, proj_grad = mixer(
        stream, out_grad, norm_gain[None, :], grad, states, gate_branch, out_proj, conv_out,
        decay_map[:, 0], input_map[:, 0], base, decay_shift,
    )
    return (
        conv_grad, branch_grad, proj_grad, gate_wgrad[None], up_wgrad[None], down_wgrad[None]
    )


def solution(mesh):
    in_specs = (
        P(SP, None),
        P(SP, None),
        P(),
        P(SP, None),
        P(SP, None),
        P(SP, None, "tp"),
        P(SP, None, "tp"),
        P(SP, "tp", None),
        P(None, "tp"),
        P(SP, "tp"),
        P(SP, "tp"),
        P(None, "tp", None, None),
        P(None, "tp", None, None),
        P(None, "tp"),
        P(None, SP, "tp"),
        P(None, SP, "tp"),
    )
    out_specs = (
        P(SP, "tp"),
        P(SP, "tp"),
        P(SP, "tp"),
        P(SP, None, "tp"),
        P(SP, None, "tp"),
        P(SP, "tp", None),
    )
    return jax.shard_map(body, mesh=mesh, in_specs=in_specs, out_specs=out_specs, check_vma=False)
```

```python
import functools

import jax
import jax.numpy as jnp
from jax import lax
from jax.experimental import pallas as pl
from jax.experimental.pallas import tpu as pltpu
from jax.sharding import PartitionSpec as P

BF = jnp.bfloat16
F32 = jnp.float32
I32 = jnp.int32
MESH = pl.DeviceIdType.MESH
ANY = pl.BlockSpec(memory_space=pl.ANY)
VM = pl.BlockSpec(memory_space=pltpu.VMEM)

SPN = 32
TPN = 4
TOK = 256
QW = 1024
FFQ = 256
CHUNKS = 8
SP = "sp"
CW = QW // CHUNKS
rate_scale = 8.0
norm_eps = 1e-06


def contract(left, right, left_dim, right_dim, precision=None):
    return lax.dot_general(
        left,
        right,
        (((left_dim,), (right_dim,)), ((), ())),
        preferred_element_type=F32,
        precision=precision,
    )


def prep_kernel(
    stream, out_grad, gain, routes, weight, send, combine,
    v_stream, v_out, qi, qc0, qc1, scale, load_sem,
):
    h = pl.program_id(0)
    low = lax.axis_index("tp") % 2
    cols = pl.ds(pl.multiple_of((2 * h + low) * QW, QW), QW)

    def load_stream():
        return pltpu.make_async_copy(stream, v_stream, load_sem.at[0])

    def load_out(half):
        part = pl.ds(pl.multiple_of((2 * half + low) * QW, QW), QW)
        return pltpu.make_async_copy(out_grad.at[:, part], v_out.at[half], load_sem.at[1 + half])

    diagonal = lax.broadcasted_iota(I32, (TOK, TOK), 0) == lax.broadcasted_iota(
        I32, (TOK, TOK), 1
    )

    def column(row):
        return jnp.sum(jnp.where(diagonal, row.astype(F32), 0.0), axis=1, keepdims=True)

    @pl.when(h == 0)
    def _():
        load_stream().start()
        load_out(0).start()
        load_out(1).start()
        lanes = lax.broadcasted_iota(I32, (TOK, 128), 1)
        r0 = column(routes[0:1, :]).astype(I32)
        r1 = column(routes[1:2, :]).astype(I32)
        hot0 = (r0 == lanes).astype(F32)
        hot1 = (r1 == lanes).astype(F32)
        before = (
            lax.broadcasted_iota(I32, (TOK, TOK), 1) < lax.broadcasted_iota(I32, (TOK, TOK), 0)
        ).astype(F32)
        counts = contract(before.astype(BF), (hot0 + hot1).astype(BF), 1, 0)
        upper = lax.axis_index("sp") // 16
        slots = lax.broadcasted_iota(I32, (TOK, 768), 1)

        def places(route, hot):
            rank = jnp.sum(counts * hot, axis=1, keepdims=True).astype(I32)
            pure = (rank // 8) * 256 + route * 8 + rank % 8
            mixed = 512 + route * 8 + (rank - 16)
            of_input = jnp.where(rank < 16, pure, mixed + 4 * upper)
            of_cotan = jnp.where(rank < 16, pure, mixed + 4 * (1 - upper))
            of_return = route * 24 + rank + jnp.where(rank < 16, 0, 4 * upper)
            return tuple(
                (slots == place).astype(F32) for place in (of_input, of_cotan, of_return)
            )

        in0, cot0, ret0 = places(r0, hot0)
        in1, cot1, ret1 = places(r1, hot1)
        qi[...] = (in0 + in1).astype(BF)
        combine[...] = (ret0 + ret1).astype(BF)
        qc0[...] = cot0.astype(BF)
        qc1[...] = cot1.astype(BF)
        load_stream().wait()
        wide = v_stream[...].astype(F32)
        mean = jnp.sum(wide * wide, axis=1, keepdims=True) * (1.0 / (TPN * QW))
        scale[...] = jnp.broadcast_to(lax.rsqrt(mean + norm_eps), (TOK, 128))

    load_out(h).wait()
    normed = (
        v_stream[:, cols].astype(F32) * scale[:, 0:1] * gain[:, cols].astype(F32)
    ).astype(BF)
    grad = v_out[h].astype(F32)
    scaled0 = (column(weight[0:1, :]) * grad).astype(BF)
    scaled1 = (column(weight[1:2, :]) * grad).astype(BF)
    for plane in range(3):
        span = slice(plane * 256, plane * 256 + 256)
        rows_in = contract(qi[:, span], normed, 0, 0)
        rows_cot = contract(qc0[:, span], scaled0, 0, 0) + contract(qc1[:, span], scaled1, 0, 0)
        if plane < 2:
            send[0, plane] = rows_in.astype(BF)
            send[0, plane + 2] = rows_cot.astype(BF)
        else:
            send[0, 4] = (rows_in + rows_cot).astype(BF)


def prep(stream, out_grad, gain, routes, weight):
    whole = lambda shape: pl.BlockSpec(shape, lambda h: (0,) * len(shape))
    return pl.pallas_call(
        prep_kernel,
        grid=(2,),
        in_specs=[ANY, ANY, whole((1, 4 * QW)), whole((2, TOK)), whole((2, TOK))],
        out_specs=[
            pl.BlockSpec((1, 5, 256, QW), lambda h: (h, 0, 0, 0)),
            whole((TOK, 768)),
        ],
        out_shape=[
            jax.ShapeDtypeStruct((2, 5, 256, QW), BF),
            jax.ShapeDtypeStruct((TOK, 768), BF),
        ],
        scratch_shapes=[
            pltpu.VMEM((TOK, 4 * QW), BF),
            pltpu.VMEM((2, TOK, QW), BF),
            pltpu.VMEM((TOK, 768), BF),
            pltpu.VMEM((TOK, 768), BF),
            pltpu.VMEM((TOK, 768), BF),
            pltpu.VMEM((TOK, 128), F32),
            pltpu.SemaphoreType.DMA((3,)),
        ],
        compiler_params=pltpu.CompilerParams(vmem_limit_bytes=48 * 1024 * 1024),
        name="prep",
    )(stream, out_grad, gain, routes, weight)


NEAR = (
    (0, 1), (1, 0), (0, 3), (3, 0), (1, 1), (3, 3), (1, 3), (3, 1),
    (0, 2), (2, 0), (1, 2), (2, 1), (3, 2), (2, 3), (2, 2),
)
STEPS = ((0, 0, 1),) + tuple((z, y, c) for c in (0, 1) for z, y in NEAR)


def peer(s, k, sign=1):
    z, y, c = STEPS[k - 1]
    return (
        lax.rem(s // 8 + (z if sign > 0 else 4 - z), 4) * 8
        + lax.rem((s // 2) % 4 + (y if sign > 0 else 4 - y), 4) * 2
        + lax.rem(s % 2 + c, 2)
    )


def greet(s, x):
    hello_all(s, x)
    met()


def met():
    pl.semaphore_wait(pltpu.get_barrier_semaphore(), SPN + 1)


def hello_all(s, x):
    barrier = pltpu.get_barrier_semaphore()

    def hello(d, carry):
        pl.semaphore_signal(barrier, inc=1, device_id=(s ^ d, x), device_id_type=MESH)
        return carry

    lax.fori_loop(1, SPN, hello, 0)
    for step in (1, TPN - 1):
        pl.semaphore_signal(
            barrier, inc=1, device_id=(s, lax.rem(x + step, TPN)), device_id_type=MESH
        )


def remote(src, dst, send_sem, recv_sem, target):
    return pltpu.make_async_remote_copy(
        src_ref=src,
        dst_ref=dst,
        send_sem=send_sem,
        recv_sem=recv_sem,
        device_id=target,
        device_id_type=MESH,
    )


def loop(lower, upper, step):
    def run(d, carry):
        step(d)
        return carry

    lax.fori_loop(lower, upper, run, 0)


def dispatch_kernel(send, got, own_sem, send_sem, recv_sem, fwd_send, fwd_recv):
    s = lax.axis_index("sp")
    x = lax.axis_index("tp")
    high, low = x // 2, x % 2
    right, left = lax.rem(x + 1, TPN), lax.rem(x + TPN - 1, TPN)
    greet(s, x)

    def rows(i):
        return pl.ds(pl.multiple_of(i * 8, 8), 8)

    def over(turn, k, target):
        hi = high if turn == 0 else 1 - high
        return remote(
            send.at[hi, :, rows(target), :],
            got.at[hi, low, :, rows(s), :],
            send_sem.at[turn, k],
            recv_sem.at[turn, k],
            (target, x),
        )

    def onward(src, dst, k, side):
        return remote(
            src, dst, fwd_send.at[side, k], fwd_recv.at[side, k], (s, (right, left)[side])
        )

    def block(i):
        return got.at[high, low, :, rows(i), :]

    own = pltpu.make_async_copy(
        send.at[:, :, rows(s), :], got.at[:, low, :, rows(s), :], own_sem
    )
    own.start()
    for side in range(2):
        onward(send.at[high, :, rows(s), :], block(s), 0, side).start()
    for turn in range(2):
        for k in range(1, SPN):
            over(turn, k, peer(s, k)).start()
    for k in range(1, SPN):
        source = peer(s, k, -1)
        over(0, k, source).wait_recv()
        for side in range(2):
            onward(block(source), block(source), k, side).start()
    own.wait()

    def finish(k):
        for turn in range(2):
            over(turn, k, s ^ 1).wait_send()
        over(1, k, s ^ 1).wait_recv()

    def finish_onward(k):
        for side in range(2):
            copy = onward(block(s), block(s), k, side)
            copy.wait_send()
            copy.wait_recv()

    loop(1, SPN, finish)
    loop(0, SPN, finish_onward)


def dispatch(send):
    return pl.pallas_call(
        dispatch_kernel,
        in_specs=[ANY],
        out_specs=ANY,
        out_shape=jax.ShapeDtypeStruct((2, 2, 5, 256, QW), BF),
        scratch_shapes=[
            pltpu.SemaphoreType.DMA,
            pltpu.SemaphoreType.DMA((2, SPN)),
            pltpu.SemaphoreType.DMA((2, SPN)),
            pltpu.SemaphoreType.DMA((2, SPN)),
            pltpu.SemaphoreType.DMA((2, SPN)),
        ],
        compiler_params=pltpu.CompilerParams(collective_id=0, has_side_effects=True),
        name="dispatch",
    )(send)


def swap_halves(v):
    tiles = v.reshape(16, 8, v.shape[1])
    return pltpu.roll(tiles, 4, 1).reshape(v.shape)


def expert_kernel(
    got, gate, up, down, part, gate_wg, up_wg, down_wg,
    vin, vcot, vmix, vg, vu, vd, vpart, ogu, od, gp, upre, hg, gu, hid,
    in_sem, w_sem, part_sem, o_sem,
):
    def loads(q):
        hi, lo = q // 2, q % 2
        out = []
        for plane in range(5):
            if plane < 2:
                dst = vin.at[q, pl.ds(plane * 256, 256), :]
            elif plane < 4:
                dst = vcot.at[q, pl.ds((plane - 2) * 256, 256), :]
            else:
                dst = vmix.at[q]
            out.append(pltpu.make_async_copy(got.at[hi, lo, plane], dst, in_sem.at[q, plane]))
        rows = pl.ds(pl.multiple_of(q * QW, QW), QW)
        out.append(pltpu.make_async_copy(gate.at[rows, :], vg.at[q], w_sem.at[0, q]))
        out.append(pltpu.make_async_copy(up.at[rows, :], vu.at[q], w_sem.at[1, q]))
        out.append(pltpu.make_async_copy(down.at[:, rows], vd.at[q], w_sem.at[2, q]))
        return out

    loop(0, TPN, lambda q: [c.start() for c in loads(q)])
    gp[...] = jnp.zeros_like(gp)
    upre[...] = jnp.zeros_like(upre)
    hg[...] = jnp.zeros_like(hg)

    def forward(q):
        for c in loads(q):
            c.wait()
        first = lax.broadcasted_iota(I32, (128, QW), 0) % 8 < 4
        a = vmix[q, 0:128, :].astype(F32)
        b = vmix[q, 128:256, :].astype(F32)
        vin[q, 512:640, :] = jnp.where(first, a, b).astype(BF)
        vcot[q, 512:640, :] = jnp.where(first, b, a).astype(BF)
        rows = vin[q]
        gp[...] += contract(rows, vg[q], 1, 0)
        upre[...] += contract(rows, vu[q], 1, 0)
        hg[...] += contract(vcot[q], vd[q], 1, 1)

    loop(0, TPN, forward)
    hg[512:640, :] = swap_halves(hg[512:640, :])
    gate_pre, up_pre, hidden_grad = gp[...], upre[...], hg[...]
    logistic = jax.nn.sigmoid(gate_pre)
    silu = gate_pre * logistic
    hidden = silu * up_pre
    hid[0:512, :] = hidden[0:512, :].astype(BF)
    hid[512:640, :] = swap_halves(hidden[512:640, :]).astype(BF)
    gu[:, 0:FFQ] = (
        hidden_grad * up_pre * (logistic * (1.0 + gate_pre * (1.0 - logistic)))
    ).astype(BF)
    gu[:, FFQ : 2 * FFQ] = (hidden_grad * silu).astype(BF)

    def part_out(q):
        return pltpu.make_async_copy(vpart.at[q], part.at[q], part_sem.at[q])

    def back(q):
        rows = (
            contract(gu[:, 0:FFQ], vg[q], 1, 1) + contract(gu[:, FFQ : 2 * FFQ], vu[q], 1, 1)
        ).astype(BF)
        for c in range(CHUNKS):
            vpart[q, c] = rows[:, c * CW : (c + 1) * CW]
        part_out(q).start()

    loop(0, TPN, back)

    def grads_out(q):
        rows = pl.ds(pl.multiple_of(q * QW, QW), QW)
        return (
            pltpu.make_async_copy(ogu.at[0, q], gate_wg.at[rows, :], o_sem.at[0, q]),
            pltpu.make_async_copy(ogu.at[1, q], up_wg.at[rows, :], o_sem.at[1, q]),
            pltpu.make_async_copy(od.at[q], down_wg.at[:, rows], o_sem.at[2, q]),
        )

    def weights(q):
        both = contract(vin[q], gu[...], 0, 0)
        ogu[0, q] = both[:, 0:FFQ].astype(BF)
        ogu[1, q] = both[:, FFQ : 2 * FFQ].astype(BF)
        od[q] = contract(hid[...], vcot[q], 0, 0).astype(BF)
        for c in grads_out(q):
            c.start()

    loop(0, TPN, weights)
    loop(0, TPN, lambda q: part_out(q).wait())
    loop(0, TPN, lambda q: [c.wait() for c in grads_out(q)])


def expert(got, gate, up, down):
    full = TPN * QW
    return pl.pallas_call(
        expert_kernel,
        in_specs=[ANY] * 4,
        out_specs=[ANY] * 4,
        out_shape=[
            jax.ShapeDtypeStruct((TPN, CHUNKS, 640, CW), BF),
            jax.ShapeDtypeStruct((full, FFQ), BF),
            jax.ShapeDtypeStruct((full, FFQ), BF),
            jax.ShapeDtypeStruct((FFQ, full), BF),
        ],
        scratch_shapes=[
            pltpu.VMEM((TPN, 640, QW), BF),
            pltpu.VMEM((TPN, 640, QW), BF),
            pltpu.VMEM((TPN, 256, QW), BF),
            pltpu.VMEM((TPN, QW, FFQ), BF),
            pltpu.VMEM((TPN, QW, FFQ), BF),
            pltpu.VMEM((TPN, FFQ, QW), BF),
            pltpu.VMEM((TPN, CHUNKS, 640, CW), BF),
            pltpu.VMEM((2, TPN, QW, FFQ), BF),
            pltpu.VMEM((TPN, FFQ, QW), BF),
            pltpu.VMEM((640, FFQ), F32),
            pltpu.VMEM((640, FFQ), F32),
            pltpu.VMEM((640, FFQ), F32),
            pltpu.VMEM((640, 2 * FFQ), BF),
            pltpu.VMEM((640, FFQ), BF),
            pltpu.SemaphoreType.DMA((TPN, 5)),
            pltpu.SemaphoreType.DMA((3, TPN)),
            pltpu.SemaphoreType.DMA((TPN,)),
            pltpu.SemaphoreType.DMA((3, TPN)),
        ],
        compiler_params=pltpu.CompilerParams(vmem_limit_bytes=60 * 1024 * 1024),
        name="expert",
    )(got, gate, up, down)


def back_kernel(
    part, combine, grad, near, final, back, held, give, second,
    near_send, near_recv, own_sem, ret_send, ret_recv, two_send, two_recv, all_send, all_recv,
):
    s = lax.axis_index("sp")
    x = lax.axis_index("tp")
    right, left = lax.rem(x + 1, TPN), lax.rem(x + 3, TPN)
    greet(s, x)

    def partners(c):
        odd = lax.rem(c, 2)
        one = x + 1 - 2 * lax.rem(x, 2)
        other = TPN - 1 - x
        return one + odd * (other - one), other + odd * (one - other)

    def to_pair(c, j):
        pair, _ = partners(c)
        quarter = pair if j == 0 else lax.rem(x + 2, TPN)
        return remote(
            part.at[quarter, c],
            near.at[c, j],
            near_send.at[c, j],
            near_recv.at[c, j],
            (s, pair),
        )

    def own_back(c):
        return pltpu.make_async_copy(final.at[c, s], back.at[c, s], own_sem.at[c])

    def home(c, k, target):
        return remote(
            final.at[c, target], back.at[c, s], ret_send.at[c, k], ret_recv.at[c, k], (target, x)
        )

    def to_other(c):
        _, other = partners(c)
        return remote(give.at[c], second.at[c], two_send.at[c], two_recv.at[c], (s, other))

    def spread(c, side):
        src = grad.at[x, c]
        return remote(
            src, src, all_send.at[side, 0, c], all_recv.at[side, 0, c], (s, (right, left)[side])
        )

    def spread_on(c, side):
        src = grad.at[(left, right)[side], c, pl.ds(side * 128, 128), :]
        return remote(
            src, src, all_send.at[side, 1, c], all_recv.at[side, 1, c], (s, (right, left)[side])
        )

    def begin(c):
        for j in range(2):
            to_pair(c, j).start()

    loop(0, CHUNKS, begin)

    def stage(t):
        @pl.when(t < CHUNKS)
        def _():
            _, other = partners(t)
            for j in range(2):
                to_pair(t, j).wait_recv()
                mine = part[x if j == 0 else other, t]
                total = (mine.astype(F32) + near[t, j].astype(F32)).astype(BF)
                lanes = slice(j * CW, (j + 1) * CW)
                final[t, :, 0:8, lanes] = total[0:256].reshape(32, 8, CW)
                final[t, :, 8:16, lanes] = total[256:512].reshape(32, 8, CW)
                mixed = total[512:640].reshape(16, 8, CW)
                final[t, 0:16, 16:24, lanes] = mixed
                final[t, 16:32, 16:24, lanes] = mixed
            own_back(t).start()
            for k in range(1, SPN):
                home(t, k, peer(s, k)).start()

        c2 = t - 2

        @pl.when((c2 >= 0) & (c2 < CHUNKS))
        def _():
            own_back(c2).wait()
            loop(1, SPN, lambda k: home(c2, k, s ^ 1).wait_recv())
            summed = contract(combine[...], back[c2].reshape(768, 2 * CW), 1, 0)
            held[c2] = summed[:, 0:CW]
            give[c2] = summed[:, CW : 2 * CW].astype(BF)
            to_other(c2).start()

        c3 = t - 3

        @pl.when((c3 >= 0) & (c3 < CHUNKS))
        def _():
            to_other(c3).wait_recv()
            grad[x, c3] = (held[c3] + second[c3].astype(F32)).astype(BF)
            for side in range(2):
                spread(c3, side).start()

        c4 = t - 4

        @pl.when((c4 >= 0) & (c4 < CHUNKS))
        def _():
            for side in range(2):
                spread(c4, side).wait_recv()
                spread_on(c4, side).start()

    loop(0, CHUNKS + 4, stage)

    def finish(c):
        for j in range(2):
            to_pair(c, j).wait_send()
        to_other(c).wait_send()
        for side in range(2):
            spread(c, side).wait_send()
            spread_on(c, side).wait_send()
            spread_on(c, side).wait_recv()
        loop(1, SPN, lambda k: home(c, k, s ^ 1).wait_send())

    loop(0, CHUNKS, finish)


def send_back(part, combine):
    dma = pltpu.SemaphoreType.DMA
    return pl.pallas_call(
        back_kernel,
        in_specs=[VM, VM],
        out_specs=VM,
        out_shape=jax.ShapeDtypeStruct((TPN, CHUNKS, TOK, CW), BF),
        scratch_shapes=[
            pltpu.VMEM((CHUNKS, 2, 640, CW), BF),
            pltpu.VMEM((CHUNKS, SPN, 24, 2 * CW), BF),
            pltpu.VMEM((CHUNKS, SPN, 24, 2 * CW), BF),
            pltpu.VMEM((CHUNKS, TOK, CW), F32),
            pltpu.VMEM((CHUNKS, TOK, CW), BF),
            pltpu.VMEM((CHUNKS, TOK, CW), BF),
            dma((CHUNKS, 2)),
            dma((CHUNKS, 2)),
            dma((CHUNKS,)),
            dma((CHUNKS, SPN)),
            dma((CHUNKS, SPN)),
            dma((CHUNKS,)),
            dma((CHUNKS,)),
            dma((2, 2, CHUNKS)),
            dma((2, 2, CHUNKS)),
        ],
        compiler_params=pltpu.CompilerParams(
            collective_id=1, has_side_effects=True, vmem_limit_bytes=48 * 1024 * 1024
        ),
        name="send_back",
    )(part, combine)


def expm1_negative(v):
    series = 1.0 + v * (1.0 / 9.0)
    for k in (8, 7, 6, 5, 4, 3, 2):
        series = 1.0 + v * (1.0 / k) * series
    return jnp.where(v > -0.5, v * series, jnp.exp(v) - 1.0)


def scan_rows(coeff, value, reverse):
    rows = lax.broadcasted_iota(I32, coeff.shape, 0)
    for k in (1, 2, 4, 8, 16, 32, 64, 128):
        if reverse:
            inside = rows < TOK - k
            shift = TOK - k
        else:
            inside = rows >= k
            shift = k
        coeff_far = jnp.where(inside, pltpu.roll(coeff, shift, 0), 1.0)
        value_far = jnp.where(inside, pltpu.roll(value, shift, 0), 0.0)
        value = value + coeff * value_far
        coeff = coeff * coeff_far
    return coeff, value


def mixer_kernel(
    stream, out_grad, gain, grad, states, branch, out_proj, conv, decay_map, input_map, base, shift,
    branch_grad, conv_grad, proj_grad,
    v_stream, v_out, v_proj, v_states, v_shift, v_branch, v_conv, v_decay, v_input,
    sgb, dot, scale, lru, pulled, linear, coeffs,
    ends, edges, pieces, pair, paired, far_y, far_z, sum_y, sum_z, last_y, last_z,
    big_sem, small_sem, end_send, end_recv, pair_send, pair_recv, one_send, one_recv,
    two_send, two_recv,
):
    s = lax.axis_index("sp")
    x = lax.axis_index("tp")
    z, y, core = s // 8, (s // 2) % 4, s % 2
    hello_all(s, x)

    def big(which, q):
        cols = pl.ds(pl.multiple_of(q * QW, QW), QW)
        src, dst = (
            (stream.at[:, cols], v_stream.at[q]),
            (out_grad.at[:, cols], v_out.at[q]),
            (out_proj.at[cols, :], v_proj.at[q]),
        )[which]
        return pltpu.make_async_copy(src, dst, big_sem.at[which, q])

    small = [
        pltpu.make_async_copy(src, dst, small_sem.at[k])
        for k, (src, dst) in enumerate(
            (
                (conv, v_conv),
                (decay_map, v_decay),
                (input_map, v_input),
                (shift, v_shift),
                (states, v_states),
                (branch, v_branch),
            )
        )
    ]
    for copy in small:
        copy.start()

    def begin(q):
        for which in range(3):
            big(which, q).start()

    loop(0, TPN, begin)
    for copy in small:
        copy.wait()

    c = v_conv[...].astype(F32)
    rows = lax.broadcasted_iota(I32, (TOK, FFQ), 0)
    for d in range(2):
        r = jax.nn.sigmoid(contract(v_conv[...], v_decay[d], 1, 0))
        i = jax.nn.sigmoid(contract(v_conv[...], v_input[d], 1, 0))
        rate = (-rate_scale) * base[d : d + 1, :]
        log_decay = r * rate + v_shift[d]
        decay = jnp.exp(log_decay)
        width = jnp.sqrt(-expm1_negative(2.0 * log_decay))
        drive = width * i * c
        if d == 0:
            coeffs[d] = jnp.where(rows == TOK - 1, 1.0, pltpu.roll(decay, TOK - 1, 0))
            ends[0:1, :] = decay[0:1]
        else:
            coeffs[d] = jnp.where(rows == 0, 1.0, pltpu.roll(decay, 1, 0))
            ends[2:3, :] = decay[TOK - 1 : TOK]
        linear[d, 0] = width * i
        linear[d, 1] = (
            ((v_states[d] - drive) - i * c * decay * decay / width) * rate * r * (1.0 - r)
        )
        linear[d, 2] = width * c * i * (1.0 - i)

    def grad_of(q):
        return jnp.concatenate([grad[q, c] for c in range(CHUNKS)], axis=1).astype(F32)

    def squares(q, carry):
        big(0, q).wait()
        v = v_stream[q].astype(F32)
        g = gain[:, pl.ds(pl.multiple_of(q * QW, QW), QW)].astype(F32)
        w = v * (g * grad_of(q))
        return (
            carry[0] + jnp.sum(v * v, axis=1, keepdims=True),
            carry[1] + jnp.sum(w, axis=1, keepdims=True),
        )

    zero = jnp.zeros((TOK, 1), F32)
    square, along = lax.fori_loop(0, TPN, squares, (zero, zero))
    inverse = 1.0 / (TPN * QW)
    row_scale = lax.rsqrt(square * inverse + norm_eps)
    scale[...] = jnp.broadcast_to(row_scale, (TOK, 128))
    dot[...] = jnp.broadcast_to(along * row_scale * inverse, (TOK, 128))
    pulled[...] = jnp.zeros_like(pulled)

    def rows_grad(q):
        big(1, q).wait()
        big(2, q).wait()
        r = scale[:, 0:1]
        unit = v_stream[q].astype(F32) * r
        scaled = gain[:, pl.ds(pl.multiple_of(q * QW, QW), QW)].astype(F32) * grad_of(q)
        v = (v_out[q].astype(F32) + r * (scaled - unit * dot[:, 0:1])).astype(BF)
        sgb[q] = v
        pulled[...] += contract(v, v_proj[q], 1, 0)

    loop(0, TPN, rows_grad)
    lru_grad = pulled[...]
    total = v_states[0] + v_states[1]
    b = v_branch[...].astype(F32)
    root = 0.7978845608028654
    tanh = jnp.tanh(root * (b + 0.044715 * b * b * b))
    gelu = 0.5 * b * (1.0 + tanh)
    slope = 0.5 * (1.0 + tanh) + 0.5 * b * (1.0 - tanh * tanh) * root * (
        1.0 + 3.0 * 0.044715 * b * b
    )
    lru[...] = (total * gelu).astype(BF)
    branch_grad[...] = lru_grad * total * slope
    state_grad = lru_grad * gelu
    def pair_to(q):
        return remote(
            pieces.at[q, :, 1 - core],
            pair.at[q],
            pair_send.at[q],
            pair_recv.at[q],
            (s + 1 - 2 * core, x),
        )

    def proj(q):
        pieces[q] = (
            contract(sgb[q], lru[...], 0, 0).astype(BF).reshape(TPN, 2, 128, FFQ)
        )
        pair_to(q).start()

    met()
    loop(0, TPN, proj)
    for d in range(2):
        reach, inner = scan_rows(coeffs[d], state_grad, d == 0)
        edge = slice(0, 1) if d == 0 else slice(TOK - 1, TOK)
        decay = ends[2 * d : 2 * d + 1, :]
        ends[2 * d : 2 * d + 1, :] = decay * reach[edge]
        ends[2 * d + 1 : 2 * d + 2, :] = decay * inner[edge]
        linear[d, 3] = reach
        linear[d, 4] = inner

    def ends_to(k, target):
        return remote(ends, edges.at[s], end_send.at[k], end_recv.at[k], (target, x))

    for k in range(1, SPN):
        ends_to(k, peer(s, k)).start()
    edges[s] = ends[...]


    def meet(q):
        pair_to(q).wait_recv()
        paired[q] = (pieces[q, :, core].astype(F32) + pair[q].astype(F32)).astype(BF)

    loop(0, TPN, meet)
    first, second = pl.ds(0, 64), pl.ds(64, 64)

    def along_y(k):
        return lax.rem(y + k, 4), (z * 8 + lax.rem(y + k, 4) * 2 + core, x)

    def along_z(k):
        return lax.rem(z + k, 4), (lax.rem(z + k, 4) * 8 + y * 2 + core, x)

    def one(side, k):
        place, target = (along_y, along_z)[side](k)
        if side == 0:
            src, dst = paired.at[:, place, first, :], far_y.at[k - 1]
        else:
            src, dst = paired.at[place, :, second, :], far_z.at[k - 1]
        return remote(src, dst, one_send.at[side, k], one_recv.at[side, k], target)

    def two(side, k):
        place, target = (along_z, along_y)[side](k)
        if side == 0:
            src, dst = sum_y.at[place], last_y.at[k - 1]
        else:
            src, dst = sum_z.at[place], last_z.at[k - 1]
        return remote(src, dst, two_send.at[side, k], two_recv.at[side, k], target)

    for k in (1, 3, 2):
        for side in range(2):
            one(side, k).start()

    for k in range(1, SPN):
        ends_to(k, s ^ 1).wait_recv()

    def carry_in(j, carry):
        later = SPN - 1 - j
        e0, e1 = edges[later], edges[j]
        from_right = jnp.where(later > s, e0[1:2] + e0[0:1] * carry[0], carry[0])
        from_left = jnp.where(j < s, e1[3:4] + e1[2:3] * carry[1], carry[1])
        return from_right, from_left

    none = jnp.zeros((1, FFQ), F32)
    incoming = lax.fori_loop(0, SPN, carry_in, (none, none))

    def back_maps(d):
        adjoint = linear[d, 4] + linear[d, 3] * incoming[d]
        highest = lax.Precision.HIGHEST
        return (
            adjoint * linear[d, 0]
            + contract(adjoint * linear[d, 1], v_decay[d].astype(F32), 1, 1, highest)
            + contract(adjoint * linear[d, 2], v_input[d].astype(F32), 1, 1, highest)
        )

    conv_grad[...] = back_maps(0) + back_maps(1)

    for side in range(2):
        for k in (1, 3, 2):
            one(side, k).wait_recv()
        if side == 0:
            acc = paired[:, y, first, :].astype(F32)
        else:
            acc = paired[z, :, second, :].astype(F32)
        came = (far_y, far_z)[side]
        acc = acc + came[0].astype(F32) + came[1].astype(F32) + came[2].astype(F32)
        (sum_y, sum_z)[side][...] = acc.astype(BF)
        for k in (1, 3, 2):
            two(side, k).start()

    for side in range(2):
        for k in (1, 3, 2):
            two(side, k).wait_recv()
        came = (last_y, last_z)[side]
        acc = (sum_y[z] if side == 0 else sum_z[y]).astype(F32)
        acc = acc + came[0].astype(F32) + came[1].astype(F32) + came[2].astype(F32)
        proj_grad[pl.ds(side * 64, 64), :] = acc

    for side in range(2):
        for k in (1, 3, 2):
            one(side, k).wait_send()
            two(side, k).wait_send()
    loop(1, SPN, lambda k: ends_to(k, s ^ 1).wait_send())
    loop(0, TPN, lambda q: pair_to(q).wait_send())


def mixer(*operands):
    whole = (TPN, TOK, QW)
    square = (TOK, FFQ)
    dma = pltpu.SemaphoreType.DMA
    return pl.pallas_call(
        mixer_kernel,
        in_specs=[ANY, ANY, VM, VM, ANY, ANY, ANY, ANY, ANY, ANY, VM, ANY],
        out_specs=[VM] * 3,
        out_shape=[
            jax.ShapeDtypeStruct(square, F32),
            jax.ShapeDtypeStruct(square, F32),
            jax.ShapeDtypeStruct((128, FFQ), F32),
        ],
        scratch_shapes=[
            pltpu.VMEM(whole, BF),
            pltpu.VMEM(whole, BF),
            pltpu.VMEM((TPN, QW, FFQ), BF),
            pltpu.VMEM((2,) + square, F32),
            pltpu.VMEM((2,) + square, F32),
            pltpu.VMEM(square, BF),
            pltpu.VMEM(square, BF),
            pltpu.VMEM((2, FFQ, FFQ), BF),
            pltpu.VMEM((2, FFQ, FFQ), BF),
            pltpu.VMEM(whole, BF),
            pltpu.VMEM((TOK, 128), F32),
            pltpu.VMEM((TOK, 128), F32),
            pltpu.VMEM(square, BF),
            pltpu.VMEM(square, F32),
            pltpu.VMEM((2, 5) + square, F32),
            pltpu.VMEM((2,) + square, F32),
            pltpu.VMEM((4, FFQ), F32),
            pltpu.VMEM((SPN, 4, FFQ), F32),
            pltpu.VMEM((4, 4, 2, 128, FFQ), BF),
            pltpu.VMEM((4, 4, 128, FFQ), BF),
            pltpu.VMEM((4, 4, 128, FFQ), BF),
            pltpu.VMEM((3, 4, 64, FFQ), BF),
            pltpu.VMEM((3, 4, 64, FFQ), BF),
            pltpu.VMEM((4, 64, FFQ), BF),
            pltpu.VMEM((4, 64, FFQ), BF),
            pltpu.VMEM((3, 64, FFQ), BF),
            pltpu.VMEM((3, 64, FFQ), BF),
            dma((3, TPN)),
            dma((6,)),
            dma((SPN,)),
            dma((SPN,)),
            dma((TPN,)),
            dma((TPN,)),
            dma((2, 4)),
            dma((2, 4)),
            dma((2, 4)),
            dma((2, 4)),
        ],
        compiler_params=pltpu.CompilerParams(
            collective_id=2, has_side_effects=True, vmem_limit_bytes=48 * 1024 * 1024
        ),
        name="mixer",
    )(*operands)


def body(
    out_grad,
    stream,
    norm_gain,
    routes,
    route_weight,
    gate_weight,
    up_weight,
    down_weight,
    out_proj,
    conv_out,
    gate_branch,
    decay_map,
    input_map,
    decay_param,
    decay_shift,
    states,
):
    send, combine = prep(stream, out_grad, norm_gain[None, :], routes.T, route_weight.T)
    got = dispatch(send)
    part, gate_wgrad, up_wgrad, down_wgrad = expert(
        got, gate_weight[0], up_weight[0], down_weight[0]
    )
    grad = send_back(part, combine)
    base = jax.nn.softplus(-decay_param)
    branch_grad, conv_grad, proj_grad = mixer(
        stream, out_grad, norm_gain[None, :], grad, states, gate_branch, out_proj, conv_out,
        decay_map[:, 0], input_map[:, 0], base, decay_shift,
    )
    return (
        conv_grad, branch_grad, proj_grad, gate_wgrad[None], up_wgrad[None], down_wgrad[None]
    )


def solution(mesh):
    in_specs = (
        P(SP, None),
        P(SP, None),
        P(),
        P(SP, None),
        P(SP, None),
        P(SP, None, "tp"),
        P(SP, None, "tp"),
        P(SP, "tp", None),
        P(None, "tp"),
        P(SP, "tp"),
        P(SP, "tp"),
        P(None, "tp", None, None),
        P(None, "tp", None, None),
        P(None, "tp"),
        P(None, SP, "tp"),
        P(None, SP, "tp"),
    )
    out_specs = (
        P(SP, "tp"),
        P(SP, "tp"),
        P(SP, "tp"),
        P(SP, None, "tp"),
        P(SP, None, "tp"),
        P(SP, "tp", None),
    )
    return jax.shard_map(body, mesh=mesh, in_specs=in_specs, out_specs=out_specs, check_vma=False)
```

```python
import functools

import jax
import jax.numpy as jnp
from jax import lax
from jax.experimental import pallas as pl
from jax.experimental.pallas import tpu as pltpu
from jax.sharding import PartitionSpec as P

BF = jnp.bfloat16
F32 = jnp.float32
I32 = jnp.int32
MESH = pl.DeviceIdType.MESH
ANY = pl.BlockSpec(memory_space=pl.ANY)
VM = pl.BlockSpec(memory_space=pltpu.VMEM)

SPN = 32
TPN = 4
TOK = 256
QW = 1024
FFQ = 256
CHUNKS = 8
SP = "sp"
CW = QW // CHUNKS
rate_scale = 8.0
norm_eps = 1e-06


def contract(left, right, left_dim, right_dim, precision=None):
    return lax.dot_general(
        left,
        right,
        (((left_dim,), (right_dim,)), ((), ())),
        preferred_element_type=F32,
        precision=precision,
    )


NEAR = (
    (0, 1), (1, 0), (0, 3), (3, 0), (1, 1), (3, 3), (1, 3), (3, 1),
    (0, 2), (2, 0), (1, 2), (2, 1), (3, 2), (2, 3), (2, 2),
)
STEPS = ((0, 0, 1),) + tuple((z, y, c) for c in (0, 1) for z, y in NEAR)


def peer(s, k, sign=1):
    z, y, c = STEPS[k - 1]
    return (
        lax.rem(s // 8 + (z if sign > 0 else 4 - z), 4) * 8
        + lax.rem((s // 2) % 4 + (y if sign > 0 else 4 - y), 4) * 2
        + lax.rem(s % 2 + c, 2)
    )


def greet(s, x):
    hello_all(s, x)
    met()


def met():
    pl.semaphore_wait(pltpu.get_barrier_semaphore(), SPN + 1)


def hello_all(s, x):
    barrier = pltpu.get_barrier_semaphore()

    def hello(d, carry):
        pl.semaphore_signal(barrier, inc=1, device_id=(s ^ d, x), device_id_type=MESH)
        return carry

    lax.fori_loop(1, SPN, hello, 0)
    for step in (1, TPN - 1):
        pl.semaphore_signal(
            barrier, inc=1, device_id=(s, lax.rem(x + step, TPN)), device_id_type=MESH
        )


def remote(src, dst, send_sem, recv_sem, target):
    return pltpu.make_async_remote_copy(
        src_ref=src,
        dst_ref=dst,
        send_sem=send_sem,
        recv_sem=recv_sem,
        device_id=target,
        device_id_type=MESH,
    )


def loop(lower, upper, step):
    def run(d, carry):
        step(d)
        return carry

    lax.fori_loop(lower, upper, run, 0)


def dispatch_kernel(
    stream, out_grad, gain, routes, weight, got, combine,
    send, v_stream, v_out, qi, qc0, qc1, scale,
    load_sem, own_sem, send_sem, recv_sem, fwd_send, fwd_recv,
):
    s = lax.axis_index("sp")
    x = lax.axis_index("tp")
    high, low = x // 2, x % 2
    right, left = lax.rem(x + 1, TPN), lax.rem(x + TPN - 1, TPN)
    hello_all(s, x)

    def columns(h):
        return pl.ds(pl.multiple_of((2 * h + low) * QW, QW), QW)

    def load(h):
        return pltpu.make_async_copy(out_grad.at[:, columns(h)], v_out.at[h], load_sem.at[1 + h])

    whole = pltpu.make_async_copy(stream, v_stream, load_sem.at[0])
    whole.start()
    load(high).start()
    load(1 - high).start()
    diagonal = lax.broadcasted_iota(I32, (TOK, TOK), 0) == lax.broadcasted_iota(
        I32, (TOK, TOK), 1
    )

    def column(row):
        return jnp.sum(jnp.where(diagonal, row.astype(F32), 0.0), axis=1, keepdims=True)

    lanes = lax.broadcasted_iota(I32, (TOK, 128), 1)
    r0 = column(routes[0:1, :]).astype(I32)
    r1 = column(routes[1:2, :]).astype(I32)
    w0, w1 = column(weight[0:1, :]), column(weight[1:2, :])
    hot0 = (r0 == lanes).astype(F32)
    hot1 = (r1 == lanes).astype(F32)
    before = (
        lax.broadcasted_iota(I32, (TOK, TOK), 1) < lax.broadcasted_iota(I32, (TOK, TOK), 0)
    ).astype(F32)
    counts = contract(before.astype(BF), (hot0 + hot1).astype(BF), 1, 0)
    upper = s // 16
    slots = lax.broadcasted_iota(I32, (TOK, 768), 1)

    def places(route, hot):
        rank = jnp.sum(counts * hot, axis=1, keepdims=True).astype(I32)
        pure = (rank // 8) * 256 + route * 8 + rank % 8
        mixed = 512 + route * 8 + (rank - 16)
        of_input = jnp.where(rank < 16, pure, mixed + 4 * upper)
        of_cotan = jnp.where(rank < 16, pure, mixed + 4 * (1 - upper))
        of_return = route * 24 + rank + jnp.where(rank < 16, 0, 4 * upper)
        return tuple((slots == place).astype(F32) for place in (of_input, of_cotan, of_return))

    in0, cot0, ret0 = places(r0, hot0)
    in1, cot1, ret1 = places(r1, hot1)
    qi[...] = (in0 + in1).astype(BF)
    combine[...] = (ret0 + ret1).astype(BF)
    qc0[...] = cot0.astype(BF)
    qc1[...] = cot1.astype(BF)
    whole.wait()
    wide = v_stream[...].astype(F32)
    mean = jnp.sum(wide * wide, axis=1, keepdims=True) * (1.0 / (TPN * QW))
    scale[...] = jnp.broadcast_to(lax.rsqrt(mean + norm_eps), (TOK, 128))

    def gather_rows(h):
        load(h).wait()
        cols = columns(h)
        normed = (
            v_stream[:, cols].astype(F32) * scale[:, 0:1] * gain[:, cols].astype(F32)
        ).astype(BF)
        grad = v_out[h].astype(F32)
        scaled0 = (w0 * grad).astype(BF)
        scaled1 = (w1 * grad).astype(BF)
        for plane in range(3):
            span = slice(plane * 256, plane * 256 + 256)
            rows_in = contract(qi[:, span], normed, 0, 0)
            rows_cot = contract(qc0[:, span], scaled0, 0, 0) + contract(
                qc1[:, span], scaled1, 0, 0
            )
            if plane < 2:
                send[h, plane] = rows_in.astype(BF)
                send[h, plane + 2] = rows_cot.astype(BF)
            else:
                send[h, 4] = (rows_in + rows_cot).astype(BF)

    def rows(i):
        return pl.ds(pl.multiple_of(i * 8, 8), 8)

    def half(turn):
        return high if turn == 0 else 1 - high

    def over(turn, k, target):
        return remote(
            send.at[half(turn), :, rows(target), :],
            got.at[half(turn), low, :, rows(s), :],
            send_sem.at[turn, k],
            recv_sem.at[turn, k],
            (target, x),
        )

    def own(turn):
        return pltpu.make_async_copy(
            send.at[half(turn), :, rows(s), :],
            got.at[half(turn), low, :, rows(s), :],
            own_sem.at[turn],
        )

    def onward(src, dst, k, side):
        return remote(
            src, dst, fwd_send.at[side, k], fwd_recv.at[side, k], (s, (right, left)[side])
        )

    def block(i):
        return got.at[high, low, :, rows(i), :]

    gather_rows(high)
    met()
    for side in range(2):
        onward(send.at[high, :, rows(s), :], block(s), 0, side).start()
    for turn in range(2):
        if turn == 1:
            gather_rows(1 - high)
        own(turn).start()
        for k in range(1, SPN):
            over(turn, k, peer(s, k)).start()
    for k in range(1, SPN):
        source = peer(s, k, -1)
        over(0, k, source).wait_recv()
        for side in range(2):
            onward(block(source), block(source), k, side).start()
    own(0).wait()
    own(1).wait()

    def finish(k):
        for turn in range(2):
            over(turn, k, s ^ 1).wait_send()
        over(1, k, s ^ 1).wait_recv()

    def finish_onward(k):
        for side in range(2):
            copy = onward(block(s), block(s), k, side)
            copy.wait_send()
            copy.wait_recv()

    loop(1, SPN, finish)
    loop(0, SPN, finish_onward)


def dispatch(stream, out_grad, gain, routes, weight):
    dma = pltpu.SemaphoreType.DMA
    return pl.pallas_call(
        dispatch_kernel,
        in_specs=[ANY, ANY, VM, VM, VM],
        out_specs=[ANY, VM],
        out_shape=[
            jax.ShapeDtypeStruct((2, 2, 5, 256, QW), BF),
            jax.ShapeDtypeStruct((TOK, 768), BF),
        ],
        scratch_shapes=[
            pltpu.VMEM((2, 5, 256, QW), BF),
            pltpu.VMEM((TOK, 4 * QW), BF),
            pltpu.VMEM((2, TOK, QW), BF),
            pltpu.VMEM((TOK, 768), BF),
            pltpu.VMEM((TOK, 768), BF),
            pltpu.VMEM((TOK, 768), BF),
            pltpu.VMEM((TOK, 128), F32),
            dma((3,)),
            dma((2,)),
            dma((2, SPN)),
            dma((2, SPN)),
            dma((2, SPN)),
            dma((2, SPN)),
        ],
        compiler_params=pltpu.CompilerParams(
            collective_id=0, has_side_effects=True, vmem_limit_bytes=62 * 1024 * 1024
        ),
        name="dispatch",
    )(stream, out_grad, gain, routes, weight)


def swap_halves(v):
    tiles = v.reshape(16, 8, v.shape[1])
    return pltpu.roll(tiles, 4, 1).reshape(v.shape)


def expert_kernel(
    got, gate, up, down, part, gate_wg, up_wg, down_wg,
    vin, vcot, vmix, vg, vu, vd, vpart, ogu, od, gp, upre, hg, gu, hid,
    in_sem, w_sem, part_sem, o_sem,
):
    def loads(q):
        hi, lo = q // 2, q % 2
        out = []
        for plane in range(5):
            if plane < 2:
                dst = vin.at[q, pl.ds(plane * 256, 256), :]
            elif plane < 4:
                dst = vcot.at[q, pl.ds((plane - 2) * 256, 256), :]
            else:
                dst = vmix.at[q]
            out.append(pltpu.make_async_copy(got.at[hi, lo, plane], dst, in_sem.at[q, plane]))
        rows = pl.ds(pl.multiple_of(q * QW, QW), QW)
        out.append(pltpu.make_async_copy(gate.at[rows, :], vg.at[q], w_sem.at[0, q]))
        out.append(pltpu.make_async_copy(up.at[rows, :], vu.at[q], w_sem.at[1, q]))
        out.append(pltpu.make_async_copy(down.at[:, rows], vd.at[q], w_sem.at[2, q]))
        return out

    loop(0, TPN, lambda q: [c.start() for c in loads(q)])
    gp[...] = jnp.zeros_like(gp)
    upre[...] = jnp.zeros_like(upre)
    hg[...] = jnp.zeros_like(hg)

    def forward(q):
        for c in loads(q):
            c.wait()
        first = lax.broadcasted_iota(I32, (128, QW), 0) % 8 < 4
        a = vmix[q, 0:128, :].astype(F32)
        b = vmix[q, 128:256, :].astype(F32)
        vin[q, 512:640, :] = jnp.where(first, a, b).astype(BF)
        vcot[q, 512:640, :] = jnp.where(first, b, a).astype(BF)
        rows = vin[q]
        gp[...] += contract(rows, vg[q], 1, 0)
        upre[...] += contract(rows, vu[q], 1, 0)
        hg[...] += contract(vcot[q], vd[q], 1, 1)

    loop(0, TPN, forward)
    hg[512:640, :] = swap_halves(hg[512:640, :])
    gate_pre, up_pre, hidden_grad = gp[...], upre[...], hg[...]
    logistic = jax.nn.sigmoid(gate_pre)
    silu = gate_pre * logistic
    hidden = silu * up_pre
    hid[0:512, :] = hidden[0:512, :].astype(BF)
    hid[512:640, :] = swap_halves(hidden[512:640, :]).astype(BF)
    gu[:, 0:FFQ] = (
        hidden_grad * up_pre * (logistic * (1.0 + gate_pre * (1.0 - logistic)))
    ).astype(BF)
    gu[:, FFQ : 2 * FFQ] = (hidden_grad * silu).astype(BF)

    def part_out(q):
        return pltpu.make_async_copy(vpart.at[q], part.at[q], part_sem.at[q])

    def back(q):
        rows = (
            contract(gu[:, 0:FFQ], vg[q], 1, 1) + contract(gu[:, FFQ : 2 * FFQ], vu[q], 1, 1)
        ).astype(BF)
        for c in range(CHUNKS):
            vpart[q, c] = rows[:, c * CW : (c + 1) * CW]
        part_out(q).start()

    loop(0, TPN, back)

    def grads_out(q):
        rows = pl.ds(pl.multiple_of(q * QW, QW), QW)
        return (
            pltpu.make_async_copy(ogu.at[0, q], gate_wg.at[rows, :], o_sem.at[0, q]),
            pltpu.make_async_copy(ogu.at[1, q], up_wg.at[rows, :], o_sem.at[1, q]),
            pltpu.make_async_copy(od.at[q], down_wg.at[:, rows], o_sem.at[2, q]),
        )

    def weights(q):
        both = contract(vin[q], gu[...], 0, 0)
        ogu[0, q] = both[:, 0:FFQ].astype(BF)
        ogu[1, q] = both[:, FFQ : 2 * FFQ].astype(BF)
        od[q] = contract(hid[...], vcot[q], 0, 0).astype(BF)
        for c in grads_out(q):
            c.start()

    loop(0, TPN, weights)
    loop(0, TPN, lambda q: part_out(q).wait())
    loop(0, TPN, lambda q: [c.wait() for c in grads_out(q)])


def expert(got, gate, up, down):
    full = TPN * QW
    return pl.pallas_call(
        expert_kernel,
        in_specs=[ANY] * 4,
        out_specs=[ANY] * 4,
        out_shape=[
            jax.ShapeDtypeStruct((TPN, CHUNKS, 640, CW), BF),
            jax.ShapeDtypeStruct((full, FFQ), BF),
            jax.ShapeDtypeStruct((full, FFQ), BF),
            jax.ShapeDtypeStruct((FFQ, full), BF),
        ],
        scratch_shapes=[
            pltpu.VMEM((TPN, 640, QW), BF),
            pltpu.VMEM((TPN, 640, QW), BF),
            pltpu.VMEM((TPN, 256, QW), BF),
            pltpu.VMEM((TPN, QW, FFQ), BF),
            pltpu.VMEM((TPN, QW, FFQ), BF),
            pltpu.VMEM((TPN, FFQ, QW), BF),
            pltpu.VMEM((TPN, CHUNKS, 640, CW), BF),
            pltpu.VMEM((2, TPN, QW, FFQ), BF),
            pltpu.VMEM((TPN, FFQ, QW), BF),
            pltpu.VMEM((640, FFQ), F32),
            pltpu.VMEM((640, FFQ), F32),
            pltpu.VMEM((640, FFQ), F32),
            pltpu.VMEM((640, 2 * FFQ), BF),
            pltpu.VMEM((640, FFQ), BF),
            pltpu.SemaphoreType.DMA((TPN, 5)),
            pltpu.SemaphoreType.DMA((3, TPN)),
            pltpu.SemaphoreType.DMA((TPN,)),
            pltpu.SemaphoreType.DMA((3, TPN)),
        ],
        compiler_params=pltpu.CompilerParams(vmem_limit_bytes=60 * 1024 * 1024),
        name="expert",
    )(got, gate, up, down)


def back_steps(
    fill, part, combine, grad, mine, near, final, back, held, give, second,
    near_send, near_recv, own_sem, ret_send, ret_recv, two_send, two_recv, all_send, all_recv, mine_sem,
):
    s = lax.axis_index("sp")
    x = lax.axis_index("tp")
    right, left = lax.rem(x + 1, TPN), lax.rem(x + 3, TPN)

    def partners(c):
        odd = lax.rem(c, 2)
        one = x + 1 - 2 * lax.rem(x, 2)
        other = TPN - 1 - x
        return one + odd * (other - one), other + odd * (one - other)

    def to_pair(c, j):
        pair, _ = partners(c)
        quarter = pair if j == 0 else lax.rem(x + 2, TPN)
        return remote(
            part.at[quarter, c],
            near.at[c, j],
            near_send.at[c, j],
            near_recv.at[c, j],
            (s, pair),
        )

    def load_mine(c, j):
        _, other = partners(c)
        return pltpu.make_async_copy(
            part.at[x if j == 0 else other, c], mine.at[c, j], mine_sem.at[c, j]
        )

    def own_back(c):
        return pltpu.make_async_copy(final.at[c, s], back.at[c, s], own_sem.at[c])

    def home(c, k, target):
        return remote(
            final.at[c, target], back.at[c, s], ret_send.at[c, k], ret_recv.at[c, k], (target, x)
        )

    def to_other(c):
        _, other = partners(c)
        return remote(give.at[c], second.at[c], two_send.at[c], two_recv.at[c], (s, other))

    def spread(c, side):
        src = grad.at[x, c]
        return remote(
            src, src, all_send.at[side, 0, c], all_recv.at[side, 0, c], (s, (right, left)[side])
        )

    def spread_on(c, side):
        src = grad.at[(left, right)[side], c, pl.ds(side * 128, 128), :]
        return remote(
            src, src, all_send.at[side, 1, c], all_recv.at[side, 1, c], (s, (right, left)[side])
        )

    def begin(c):
        for j in range(2):
            to_pair(c, j).start()

    def begin_load(c):
        for j in range(2):
            load_mine(c, j).start()

    met()
    loop(0, CHUNKS, begin)
    loop(0, CHUNKS, begin_load)

    fill()

    def open_chunk(t):
        for j in range(2):
            load_mine(t, j).wait()
            to_pair(t, j).wait_recv()
            total = (mine[t, j].astype(F32) + near[t, j].astype(F32)).astype(BF)
            lanes = slice(j * CW, (j + 1) * CW)
            final[t, :, 0:8, lanes] = total[0:256].reshape(32, 8, CW)
            final[t, :, 8:16, lanes] = total[256:512].reshape(32, 8, CW)
            mixed = total[512:640].reshape(16, 8, CW)
            final[t, 0:16, 16:24, lanes] = mixed
            final[t, 16:32, 16:24, lanes] = mixed
        own_back(t).start()
        for k in range(1, SPN):
            home(t, k, peer(s, k)).start()

    def close_chunk(c):
        own_back(c).wait()
        loop(1, SPN, lambda k: home(c, k, s ^ 1).wait_recv())
        summed = contract(combine[...], back[c].reshape(768, 2 * CW), 1, 0)
        held[c] = summed[:, 0:CW]
        give[c] = summed[:, CW : 2 * CW].astype(BF)
        to_other(c).start()

    def share(c):
        to_other(c).wait_recv()
        grad[x, c] = (held[c] + second[c].astype(F32)).astype(BF)
        for side in range(2):
            spread(c, side).start()

    def share_on(c):
        for side in range(2):
            spread(c, side).wait_recv()
            spread_on(c, side).start()

    lag = 3

    def stage(t):
        open_chunk(t)

        @pl.when(t >= lag)
        def _():
            close_chunk(t - lag)

    loop(0, CHUNKS, stage)
    loop(0, CHUNKS - lag, share)
    loop(CHUNKS - lag, CHUNKS, close_chunk)
    loop(0, CHUNKS - lag, share_on)
    loop(CHUNKS - lag, CHUNKS, share)
    loop(CHUNKS - lag, CHUNKS, share_on)

    def finish(c):
        for j in range(2):
            to_pair(c, j).wait_send()
        to_other(c).wait_send()
        for side in range(2):
            spread(c, side).wait_send()
            spread_on(c, side).wait_send()
            spread_on(c, side).wait_recv()
        loop(1, SPN, lambda k: home(c, k, s ^ 1).wait_send())

    loop(0, CHUNKS, finish)


def expm1_negative(v):
    series = 1.0 + v * (1.0 / 9.0)
    for k in (8, 7, 6, 5, 4, 3, 2):
        series = 1.0 + v * (1.0 / k) * series
    return jnp.where(v > -0.5, v * series, jnp.exp(v) - 1.0)


def scan_rows(coeff, value, reverse):
    rows = lax.broadcasted_iota(I32, coeff.shape, 0)
    for k in (1, 2, 4, 8, 16, 32, 64, 128):
        if reverse:
            inside = rows < TOK - k
            shift = TOK - k
        else:
            inside = rows >= k
            shift = k
        coeff_far = jnp.where(inside, pltpu.roll(coeff, shift, 0), 1.0)
        value_far = jnp.where(inside, pltpu.roll(value, shift, 0), 0.0)
        value = value + coeff * value_far
        coeff = coeff * coeff_far
    return coeff, value


def mixer_steps(
    stream, out_grad, gain, grad, states, branch, out_proj, conv, decay_map, input_map, base, shift,
    branch_grad, conv_grad, proj_grad,
    v_stream, v_out, v_proj, v_states, v_shift, v_branch, v_conv, v_decay, v_input,
    sgb, dot, scale, lru, pulled, linear, coeffs,
    ends, edges, pieces, pair, paired, far_y, far_z, sum_y, sum_z, last_y, last_z,
    big_sem, small_sem, end_send, end_recv, pair_send, pair_recv, one_send, one_recv,
    two_send, two_recv,
):
    s = lax.axis_index("sp")
    x = lax.axis_index("tp")
    z, y, core = s // 8, (s // 2) % 4, s % 2

    def big(which, q):
        cols = pl.ds(pl.multiple_of(q * QW, QW), QW)
        src, dst = (
            (stream.at[:, cols], v_stream.at[q]),
            (out_grad.at[:, cols], v_out.at[q]),
            (out_proj.at[cols, :], v_proj.at[q]),
        )[which]
        return pltpu.make_async_copy(src, dst, big_sem.at[which, q])

    small = [
        pltpu.make_async_copy(src, dst, small_sem.at[k])
        for k, (src, dst) in enumerate(
            (
                (conv, v_conv),
                (decay_map, v_decay),
                (input_map, v_input),
                (shift, v_shift),
                (states, v_states),
                (branch, v_branch),
            )
        )
    ]
    for copy in small:
        copy.start()

    def begin(q):
        for which in range(3):
            big(which, q).start()

    loop(0, TPN, begin)
    def gates():
        for copy in small:
            copy.wait()

        c = v_conv[...].astype(F32)
        rows = lax.broadcasted_iota(I32, (TOK, FFQ), 0)
        for d in range(2):
            r = jax.nn.sigmoid(contract(v_conv[...], v_decay[d], 1, 0))
            i = jax.nn.sigmoid(contract(v_conv[...], v_input[d], 1, 0))
            rate = (-rate_scale) * base[d : d + 1, :]
            log_decay = r * rate + v_shift[d]
            decay = jnp.exp(log_decay)
            width = jnp.sqrt(-expm1_negative(2.0 * log_decay))
            drive = width * i * c
            if d == 0:
                coeffs[d] = jnp.where(rows == TOK - 1, 1.0, pltpu.roll(decay, TOK - 1, 0))
                ends[0:1, :] = decay[0:1]
            else:
                coeffs[d] = jnp.where(rows == 0, 1.0, pltpu.roll(decay, 1, 0))
                ends[2:3, :] = decay[TOK - 1 : TOK]
            linear[d, 0] = width * i
            linear[d, 1] = (
                ((v_states[d] - drive) - i * c * decay * decay / width) * rate * r * (1.0 - r)
            )
            linear[d, 2] = width * c * i * (1.0 - i)

    def rest():
        def grad_of(q):
            return jnp.concatenate([grad[q, c] for c in range(CHUNKS)], axis=1).astype(F32)

        def squares(q, carry):
            big(0, q).wait()
            v = v_stream[q].astype(F32)
            g = gain[:, pl.ds(pl.multiple_of(q * QW, QW), QW)].astype(F32)
            w = v * (g * grad_of(q))
            return (
                carry[0] + jnp.sum(v * v, axis=1, keepdims=True),
                carry[1] + jnp.sum(w, axis=1, keepdims=True),
            )

        zero = jnp.zeros((TOK, 1), F32)
        square, along = lax.fori_loop(0, TPN, squares, (zero, zero))
        inverse = 1.0 / (TPN * QW)
        row_scale = lax.rsqrt(square * inverse + norm_eps)
        scale[...] = jnp.broadcast_to(row_scale, (TOK, 128))
        dot[...] = jnp.broadcast_to(along * row_scale * inverse, (TOK, 128))
        pulled[...] = jnp.zeros_like(pulled)

        def rows_grad(q):
            big(1, q).wait()
            big(2, q).wait()
            r = scale[:, 0:1]
            unit = v_stream[q].astype(F32) * r
            scaled = gain[:, pl.ds(pl.multiple_of(q * QW, QW), QW)].astype(F32) * grad_of(q)
            v = (v_out[q].astype(F32) + r * (scaled - unit * dot[:, 0:1])).astype(BF)
            sgb[q] = v
            pulled[...] += contract(v, v_proj[q], 1, 0)

        loop(0, TPN, rows_grad)
        lru_grad = pulled[...]
        total = v_states[0] + v_states[1]
        b = v_branch[...].astype(F32)
        root = 0.7978845608028654
        tanh = jnp.tanh(root * (b + 0.044715 * b * b * b))
        gelu = 0.5 * b * (1.0 + tanh)
        slope = 0.5 * (1.0 + tanh) + 0.5 * b * (1.0 - tanh * tanh) * root * (
            1.0 + 3.0 * 0.044715 * b * b
        )
        lru[...] = (total * gelu).astype(BF)
        branch_grad[...] = lru_grad * total * slope
        state_grad = lru_grad * gelu
        def pair_to(q):
            return remote(
                pieces.at[q, :, 1 - core],
                pair.at[q],
                pair_send.at[q],
                pair_recv.at[q],
                (s + 1 - 2 * core, x),
            )

        def proj(q):
            pieces[q] = (
                contract(sgb[q], lru[...], 0, 0).astype(BF).reshape(TPN, 2, 128, FFQ)
            )
            pair_to(q).start()

        loop(0, TPN, proj)
        for d in range(2):
            reach, inner = scan_rows(coeffs[d], state_grad, d == 0)
            edge = slice(0, 1) if d == 0 else slice(TOK - 1, TOK)
            decay = ends[2 * d : 2 * d + 1, :]
            ends[2 * d : 2 * d + 1, :] = decay * reach[edge]
            ends[2 * d + 1 : 2 * d + 2, :] = decay * inner[edge]
            linear[d, 3] = reach
            linear[d, 4] = inner

        def ends_to(k, target):
            return remote(ends, edges.at[s], end_send.at[k], end_recv.at[k], (target, x))

        for k in range(1, SPN):
            ends_to(k, peer(s, k)).start()
        edges[s] = ends[...]


        def meet(q):
            pair_to(q).wait_recv()
            paired[q] = (pieces[q, :, core].astype(F32) + pair[q].astype(F32)).astype(BF)

        loop(0, TPN, meet)
        first, second = pl.ds(0, 64), pl.ds(64, 64)

        def along_y(k):
            return lax.rem(y + k, 4), (z * 8 + lax.rem(y + k, 4) * 2 + core, x)

        def along_z(k):
            return lax.rem(z + k, 4), (lax.rem(z + k, 4) * 8 + y * 2 + core, x)

        def one(side, k):
            place, target = (along_y, along_z)[side](k)
            if side == 0:
                src, dst = paired.at[:, place, first, :], far_y.at[k - 1]
            else:
                src, dst = paired.at[place, :, second, :], far_z.at[k - 1]
            return remote(src, dst, one_send.at[side, k], one_recv.at[side, k], target)

        def two(side, k):
            place, target = (along_z, along_y)[side](k)
            if side == 0:
                src, dst = sum_y.at[place], last_y.at[k - 1]
            else:
                src, dst = sum_z.at[place], last_z.at[k - 1]
            return remote(src, dst, two_send.at[side, k], two_recv.at[side, k], target)

        for k in (1, 3, 2):
            for side in range(2):
                one(side, k).start()

        for k in range(1, SPN):
            ends_to(k, s ^ 1).wait_recv()

        def carry_in(j, carry):
            later = SPN - 1 - j
            e0, e1 = edges[later], edges[j]
            from_right = jnp.where(later > s, e0[1:2] + e0[0:1] * carry[0], carry[0])
            from_left = jnp.where(j < s, e1[3:4] + e1[2:3] * carry[1], carry[1])
            return from_right, from_left

        none = jnp.zeros((1, FFQ), F32)
        incoming = lax.fori_loop(0, SPN, carry_in, (none, none))

        def back_maps(d):
            adjoint = linear[d, 4] + linear[d, 3] * incoming[d]
            highest = lax.Precision.HIGHEST
            return (
                adjoint * linear[d, 0]
                + contract(adjoint * linear[d, 1], v_decay[d].astype(F32), 1, 1, highest)
                + contract(adjoint * linear[d, 2], v_input[d].astype(F32), 1, 1, highest)
            )

        conv_grad[...] = back_maps(0) + back_maps(1)

        for side in range(2):
            for k in (1, 3, 2):
                one(side, k).wait_recv()
            if side == 0:
                acc = paired[:, y, first, :].astype(F32)
            else:
                acc = paired[z, :, second, :].astype(F32)
            came = (far_y, far_z)[side]
            acc = acc + came[0].astype(F32) + came[1].astype(F32) + came[2].astype(F32)
            (sum_y, sum_z)[side][...] = acc.astype(BF)
            for k in (1, 3, 2):
                two(side, k).start()

        for side in range(2):
            for k in (1, 3, 2):
                two(side, k).wait_recv()
            came = (last_y, last_z)[side]
            acc = (sum_y[z] if side == 0 else sum_z[y]).astype(F32)
            acc = acc + came[0].astype(F32) + came[1].astype(F32) + came[2].astype(F32)
            proj_grad[pl.ds(side * 64, 64), :] = acc

        for side in range(2):
            for k in (1, 3, 2):
                one(side, k).wait_send()
                two(side, k).wait_send()
        loop(1, SPN, lambda k: ends_to(k, s ^ 1).wait_send())
        loop(0, TPN, lambda q: pair_to(q).wait_send())

    return gates, rest


def tail_kernel(
    part, combine, stream, out_grad, gain, states, branch, out_proj, conv, decay_map, input_map,
    base, shift, branch_grad, conv_grad, proj_grad, grad, *scratch,
):
    hello_all(lax.axis_index("sp"), lax.axis_index("tp"))
    gates, rest = mixer_steps(
        stream, out_grad, gain, grad, states, branch, out_proj, conv, decay_map, input_map, base,
        shift, branch_grad, conv_grad, proj_grad, *scratch[17:],
    )
    back_steps(gates, part, combine, grad, *scratch[:17])
    rest()


def tail(*operands):
    whole = (TPN, TOK, QW)
    square = (TOK, FFQ)
    dma = pltpu.SemaphoreType.DMA
    return pl.pallas_call(
        tail_kernel,
        in_specs=[ANY, VM, ANY, ANY, VM, ANY, ANY, ANY, ANY, ANY, ANY, VM, ANY],
        out_specs=[VM] * 3,
        out_shape=[
            jax.ShapeDtypeStruct(square, F32),
            jax.ShapeDtypeStruct(square, F32),
            jax.ShapeDtypeStruct((128, FFQ), F32),
        ],
        scratch_shapes=[
            pltpu.VMEM((TPN, CHUNKS, TOK, CW), BF),
            pltpu.VMEM((CHUNKS, 2, 640, CW), BF),
            pltpu.VMEM((CHUNKS, 2, 640, CW), BF),
            pltpu.VMEM((CHUNKS, SPN, 24, 2 * CW), BF),
            pltpu.VMEM((CHUNKS, SPN, 24, 2 * CW), BF),
            pltpu.VMEM((CHUNKS, TOK, CW), F32),
            pltpu.VMEM((CHUNKS, TOK, CW), BF),
            pltpu.VMEM((CHUNKS, TOK, CW), BF),
            dma((CHUNKS, 2)),
            dma((CHUNKS, 2)),
            dma((CHUNKS,)),
            dma((CHUNKS, SPN)),
            dma((CHUNKS, SPN)),
            dma((CHUNKS,)),
            dma((CHUNKS,)),
            dma((2, 2, CHUNKS)),
            dma((2, 2, CHUNKS)),
            dma((CHUNKS, 2)),
            pltpu.VMEM(whole, BF),
            pltpu.VMEM(whole, BF),
            pltpu.VMEM((TPN, QW, FFQ), BF),
            pltpu.VMEM((2,) + square, F32),
            pltpu.VMEM((2,) + square, F32),
            pltpu.VMEM(square, BF),
            pltpu.VMEM(square, BF),
            pltpu.VMEM((2, FFQ, FFQ), BF),
            pltpu.VMEM((2, FFQ, FFQ), BF),
            pltpu.VMEM(whole, BF),
            pltpu.VMEM((TOK, 128), F32),
            pltpu.VMEM((TOK, 128), F32),
            pltpu.VMEM(square, BF),
            pltpu.VMEM(square, F32),
            pltpu.VMEM((2, 5) + square, F32),
            pltpu.VMEM((2,) + square, F32),
            pltpu.VMEM((4, FFQ), F32),
            pltpu.VMEM((SPN, 4, FFQ), F32),
            pltpu.VMEM((4, 4, 2, 128, FFQ), BF),
            pltpu.VMEM((4, 4, 128, FFQ), BF),
            pltpu.VMEM((4, 4, 128, FFQ), BF),
            pltpu.VMEM((3, 4, 64, FFQ), BF),
            pltpu.VMEM((3, 4, 64, FFQ), BF),
            pltpu.VMEM((4, 64, FFQ), BF),
            pltpu.VMEM((4, 64, FFQ), BF),
            pltpu.VMEM((3, 64, FFQ), BF),
            pltpu.VMEM((3, 64, FFQ), BF),
            dma((3, TPN)),
            dma((6,)),
            dma((SPN,)),
            dma((SPN,)),
            dma((TPN,)),
            dma((TPN,)),
            dma((2, 4)),
            dma((2, 4)),
            dma((2, 4)),
            dma((2, 4)),
        ],
        compiler_params=pltpu.CompilerParams(
            collective_id=1, has_side_effects=True, vmem_limit_bytes=60 * 1024 * 1024
        ),
        name="tail",
    )(*operands)


def body(
    out_grad,
    stream,
    norm_gain,
    routes,
    route_weight,
    gate_weight,
    up_weight,
    down_weight,
    out_proj,
    conv_out,
    gate_branch,
    decay_map,
    input_map,
    decay_param,
    decay_shift,
    states,
):
    gain = norm_gain[None, :]
    got, combine = dispatch(stream, out_grad, gain, routes.T, route_weight.T)
    part, gate_wgrad, up_wgrad, down_wgrad = expert(
        got, gate_weight[0], up_weight[0], down_weight[0]
    )
    base = jax.nn.softplus(-decay_param)
    branch_grad, conv_grad, proj_grad = tail(
        part, combine, stream, out_grad, gain, states, gate_branch, out_proj, conv_out,
        decay_map[:, 0], input_map[:, 0], base, decay_shift,
    )
    return (
        conv_grad, branch_grad, proj_grad, gate_wgrad[None], up_wgrad[None], down_wgrad[None]
    )


def solution(mesh):
    in_specs = (
        P(SP, None),
        P(SP, None),
        P(),
        P(SP, None),
        P(SP, None),
        P(SP, None, "tp"),
        P(SP, None, "tp"),
        P(SP, "tp", None),
        P(None, "tp"),
        P(SP, "tp"),
        P(SP, "tp"),
        P(None, "tp", None, None),
        P(None, "tp", None, None),
        P(None, "tp"),
        P(None, SP, "tp"),
        P(None, SP, "tp"),
    )
    out_specs = (
        P(SP, "tp"),
        P(SP, "tp"),
        P(SP, "tp"),
        P(SP, None, "tp"),
        P(SP, None, "tp"),
        P(SP, "tp", None),
    )
    return jax.shard_map(body, mesh=mesh, in_specs=in_specs, out_specs=out_specs, check_vma=False)
```

```python
import functools

import jax
import jax.numpy as jnp
from jax import lax
from jax.experimental import pallas as pl
from jax.experimental.pallas import tpu as pltpu
from jax.sharding import PartitionSpec as P

BF = jnp.bfloat16
F32 = jnp.float32
I32 = jnp.int32
MESH = pl.DeviceIdType.MESH
ANY = pl.BlockSpec(memory_space=pl.ANY)
VM = pl.BlockSpec(memory_space=pltpu.VMEM)

SPN = 32
TPN = 4
TOK = 256
QW = 1024
FFQ = 256
CHUNKS = 8
SP = "sp"
CW = QW // CHUNKS
rate_scale = 8.0
norm_eps = 1e-06
NBACK = 22


def contract(left, right, left_dim, right_dim, precision=None):
    return lax.dot_general(
        left,
        right,
        (((left_dim,), (right_dim,)), ((), ())),
        preferred_element_type=F32,
        precision=precision,
    )


NEAR = (
    (0, 1), (1, 0), (0, 3), (3, 0), (1, 1), (3, 3), (1, 3), (3, 1),
    (0, 2), (2, 0), (1, 2), (2, 1), (3, 2), (2, 3), (2, 2),
)
STEPS = ((0, 0, 1),) + tuple((z, y, c) for c in (0, 1) for z, y in NEAR)


def peer(s, k, sign=1):
    z, y, c = STEPS[k - 1]
    return (
        lax.rem(s // 8 + (z if sign > 0 else 4 - z), 4) * 8
        + lax.rem((s // 2) % 4 + (y if sign > 0 else 4 - y), 4) * 2
        + lax.rem(s % 2 + c, 2)
    )


def tell(sem, target):
    pl.semaphore_signal(sem, inc=1, device_id=target, device_id_type=MESH)


def line_y(s, k):
    return s // 8 * 8 + lax.rem((s // 2) % 4 + k, 4) * 2 + s % 2


def line_z(s, k):
    return lax.rem(s // 8 + k, 4) * 8 + s % 8


def hello(s, x):
    barrier = pltpu.get_barrier_semaphore()
    for k in (1, 3, 2):
        tell(barrier, (line_y(s, k), x))
        tell(barrier, (line_z(s, k), x))
    tell(barrier, (s + 1 - 2 * (s % 2), x))
    for step in (1, TPN - 1):
        tell(barrier, (s, lax.rem(x + step, TPN)))


def hello_lines(s, x, sem):
    pl.semaphore_wait(pltpu.get_barrier_semaphore(), 9)
    for k in (1, 3, 2):
        tell(sem.at[0], (line_y(s, k), x))


def hello_cores(s, x, sem):
    pl.semaphore_wait(sem.at[0], 3)
    tell(sem.at[1], (s + 1 - 2 * (s % 2), x))


def met(sem):
    pl.semaphore_wait(sem.at[1], 1)


def remote(src, dst, send_sem, recv_sem, target):
    return pltpu.make_async_remote_copy(
        src_ref=src,
        dst_ref=dst,
        send_sem=send_sem,
        recv_sem=recv_sem,
        device_id=target,
        device_id_type=MESH,
    )


def loop(lower, upper, step):
    def run(d, carry):
        step(d)
        return carry

    lax.fori_loop(lower, upper, run, 0)


def dispatch_kernel(
    stream, out_grad, gain, routes, weight, got, combine,
    send, v_stream, v_out, qi, qc0, qc1, scale,
    load_sem, own_sem, send_sem, recv_sem, fwd_send, fwd_recv, met_sem,
):
    s = lax.axis_index("sp")
    x = lax.axis_index("tp")
    high, low = x // 2, x % 2
    right, left = lax.rem(x + 1, TPN), lax.rem(x + TPN - 1, TPN)
    hello(s, x)

    def columns(h):
        return pl.ds(pl.multiple_of((2 * h + low) * QW, QW), QW)

    def load(h):
        return pltpu.make_async_copy(out_grad.at[:, columns(h)], v_out.at[h], load_sem.at[1 + h])

    whole = pltpu.make_async_copy(stream, v_stream, load_sem.at[0])
    whole.start()
    load(high).start()
    load(1 - high).start()
    diagonal = lax.broadcasted_iota(I32, (TOK, TOK), 0) == lax.broadcasted_iota(
        I32, (TOK, TOK), 1
    )

    def column(row):
        return jnp.sum(jnp.where(diagonal, row.astype(F32), 0.0), axis=1, keepdims=True)

    lanes = lax.broadcasted_iota(I32, (TOK, 128), 1)
    r0 = column(routes[0:1, :]).astype(I32)
    r1 = column(routes[1:2, :]).astype(I32)
    w0, w1 = column(weight[0:1, :]), column(weight[1:2, :])
    hot0 = (r0 == lanes).astype(F32)
    hot1 = (r1 == lanes).astype(F32)
    before = (
        lax.broadcasted_iota(I32, (TOK, TOK), 1) < lax.broadcasted_iota(I32, (TOK, TOK), 0)
    ).astype(F32)
    counts = contract(before.astype(BF), (hot0 + hot1).astype(BF), 1, 0)
    upper = s // 16
    slots = lax.broadcasted_iota(I32, (TOK, 768), 1)

    def places(route, hot):
        rank = jnp.sum(counts * hot, axis=1, keepdims=True).astype(I32)
        pure = (rank // 8) * 256 + route * 8 + rank % 8
        mixed = 512 + route * 8 + (rank - 16)
        of_input = jnp.where(rank < 16, pure, mixed + 4 * upper)
        of_cotan = jnp.where(rank < 16, pure, mixed + 4 * (1 - upper))
        of_return = route * 24 + rank + jnp.where(rank < 16, 0, 4 * upper)
        return tuple((slots == place).astype(F32) for place in (of_input, of_cotan, of_return))

    in0, cot0, ret0 = places(r0, hot0)
    in1, cot1, ret1 = places(r1, hot1)
    qi[...] = (in0 + in1).astype(BF)
    combine[...] = (ret0 + ret1).astype(BF)
    qc0[...] = cot0.astype(BF)
    qc1[...] = cot1.astype(BF)
    hello_lines(s, x, met_sem)
    whole.wait()
    wide = v_stream[...].astype(F32)
    mean = jnp.sum(wide * wide, axis=1, keepdims=True) * (1.0 / (TPN * QW))
    scale[...] = jnp.broadcast_to(lax.rsqrt(mean + norm_eps), (TOK, 128))

    def gather_rows(h):
        load(h).wait()
        cols = columns(h)
        normed = (
            v_stream[:, cols].astype(F32) * scale[:, 0:1] * gain[:, cols].astype(F32)
        ).astype(BF)
        grad = v_out[h].astype(F32)
        scaled0 = (w0 * grad).astype(BF)
        scaled1 = (w1 * grad).astype(BF)
        for plane in range(3):
            span = slice(plane * 256, plane * 256 + 256)
            rows_in = contract(qi[:, span], normed, 0, 0)
            rows_cot = contract(qc0[:, span], scaled0, 0, 0) + contract(
                qc1[:, span], scaled1, 0, 0
            )
            if plane < 2:
                send[h, plane] = rows_in.astype(BF)
                send[h, plane + 2] = rows_cot.astype(BF)
            else:
                send[h, 4] = (rows_in + rows_cot).astype(BF)

    def rows(i):
        return pl.ds(pl.multiple_of(i * 8, 8), 8)

    def half(turn):
        return high if turn == 0 else 1 - high

    def over(turn, k, target):
        return remote(
            send.at[half(turn), :, rows(target), :],
            got.at[half(turn), low, :, rows(s), :],
            send_sem.at[turn, k],
            recv_sem.at[turn, k],
            (target, x),
        )

    def own(turn):
        return pltpu.make_async_copy(
            send.at[half(turn), :, rows(s), :],
            got.at[half(turn), low, :, rows(s), :],
            own_sem.at[turn],
        )

    def onward(src, dst, k, side):
        return remote(
            src, dst, fwd_send.at[side, k], fwd_recv.at[side, k], (s, (right, left)[side])
        )

    def block(i):
        return got.at[high, low, :, rows(i), :]

    hello_cores(s, x, met_sem)
    gather_rows(high)
    met(met_sem)
    for side in range(2):
        onward(send.at[high, :, rows(s), :], block(s), 0, side).start()
    for turn in range(2):
        if turn == 1:
            gather_rows(1 - high)
        own(turn).start()
        for k in range(1, SPN):
            over(turn, k, peer(s, k)).start()
    for k in range(1, SPN):
        source = peer(s, k, -1)
        over(0, k, source).wait_recv()
        for side in range(2):
            onward(block(source), block(source), k, side).start()
    own(0).wait()
    own(1).wait()

    def finish(k):
        for turn in range(2):
            over(turn, k, s ^ 1).wait_send()
        over(1, k, s ^ 1).wait_recv()

    def finish_onward(k):
        for side in range(2):
            copy = onward(block(s), block(s), k, side)
            copy.wait_send()
            copy.wait_recv()

    loop(1, SPN, finish)
    loop(0, SPN, finish_onward)


def dispatch(stream, out_grad, gain, routes, weight):
    dma = pltpu.SemaphoreType.DMA
    return pl.pallas_call(
        dispatch_kernel,
        in_specs=[ANY, ANY, VM, VM, VM],
        out_specs=[ANY, VM],
        out_shape=[
            jax.ShapeDtypeStruct((2, 2, 5, 256, QW), BF),
            jax.ShapeDtypeStruct((TOK, 768), BF),
        ],
        scratch_shapes=[
            pltpu.VMEM((2, 5, 256, QW), BF),
            pltpu.VMEM((TOK, 4 * QW), BF),
            pltpu.VMEM((2, TOK, QW), BF),
            pltpu.VMEM((TOK, 768), BF),
            pltpu.VMEM((TOK, 768), BF),
            pltpu.VMEM((TOK, 768), BF),
            pltpu.VMEM((TOK, 128), F32),
            dma((3,)),
            dma((2,)),
            dma((2, SPN)),
            dma((2, SPN)),
            dma((2, SPN)),
            dma((2, SPN)),
            pltpu.SemaphoreType.REGULAR((2,)),
        ],
        compiler_params=pltpu.CompilerParams(
            collective_id=0, has_side_effects=True, vmem_limit_bytes=62 * 1024 * 1024
        ),
        name="dispatch",
    )(stream, out_grad, gain, routes, weight)


def swap_halves(v):
    tiles = v.reshape(16, 8, v.shape[1])
    return pltpu.roll(tiles, 4, 1).reshape(v.shape)


def expert_kernel(
    got, gate, up, down, slopes, gate_wg, up_wg, down_wg,
    vin, vcot, vmix, vg, vu, vd, ogu, od, gp, upre, hg, gu, hid,
    in_sem, w_sem, slope_sem, o_sem,
):
    def loads(q):
        hi, lo = q // 2, q % 2
        out = []
        for plane in range(5):
            if plane < 2:
                dst = vin.at[q, pl.ds(plane * 256, 256), :]
            elif plane < 4:
                dst = vcot.at[q, pl.ds((plane - 2) * 256, 256), :]
            else:
                dst = vmix.at[q]
            out.append(pltpu.make_async_copy(got.at[hi, lo, plane], dst, in_sem.at[q, plane]))
        rows = pl.ds(pl.multiple_of(q * QW, QW), QW)
        out.append(pltpu.make_async_copy(gate.at[rows, :], vg.at[q], w_sem.at[0, q]))
        out.append(pltpu.make_async_copy(up.at[rows, :], vu.at[q], w_sem.at[1, q]))
        out.append(pltpu.make_async_copy(down.at[:, rows], vd.at[q], w_sem.at[2, q]))
        return out

    loop(0, TPN, lambda q: [c.start() for c in loads(q)])
    gp[...] = jnp.zeros_like(gp)
    upre[...] = jnp.zeros_like(upre)
    hg[...] = jnp.zeros_like(hg)

    def forward(q):
        for c in loads(q):
            c.wait()
        first = lax.broadcasted_iota(I32, (128, QW), 0) % 8 < 4
        a = vmix[q, 0:128, :].astype(F32)
        b = vmix[q, 128:256, :].astype(F32)
        vin[q, 512:640, :] = jnp.where(first, a, b).astype(BF)
        vcot[q, 512:640, :] = jnp.where(first, b, a).astype(BF)
        rows = vin[q]
        gp[...] += contract(rows, vg[q], 1, 0)
        upre[...] += contract(rows, vu[q], 1, 0)
        hg[...] += contract(vcot[q], vd[q], 1, 1)

    loop(0, TPN, forward)
    hg[512:640, :] = swap_halves(hg[512:640, :])
    gate_pre, up_pre, hidden_grad = gp[...], upre[...], hg[...]
    logistic = jax.nn.sigmoid(gate_pre)
    silu = gate_pre * logistic
    hidden = silu * up_pre
    hid[0:512, :] = hidden[0:512, :].astype(BF)
    hid[512:640, :] = swap_halves(hidden[512:640, :]).astype(BF)
    gu[:, 0:FFQ] = (
        hidden_grad * up_pre * (logistic * (1.0 + gate_pre * (1.0 - logistic)))
    ).astype(BF)
    gu[:, FFQ : 2 * FFQ] = (hidden_grad * silu).astype(BF)

    out = pltpu.make_async_copy(gu, slopes, slope_sem)
    out.start()

    def grads_out(q):
        rows = pl.ds(pl.multiple_of(q * QW, QW), QW)
        return (
            pltpu.make_async_copy(ogu.at[0, q], gate_wg.at[rows, :], o_sem.at[0, q]),
            pltpu.make_async_copy(ogu.at[1, q], up_wg.at[rows, :], o_sem.at[1, q]),
            pltpu.make_async_copy(od.at[q], down_wg.at[:, rows], o_sem.at[2, q]),
        )

    def weights(q):
        both = contract(vin[q], gu[...], 0, 0)
        ogu[0, q] = both[:, 0:FFQ].astype(BF)
        ogu[1, q] = both[:, FFQ : 2 * FFQ].astype(BF)
        od[q] = contract(hid[...], vcot[q], 0, 0).astype(BF)
        for c in grads_out(q):
            c.start()

    loop(0, TPN, weights)
    out.wait()
    loop(0, TPN, lambda q: [c.wait() for c in grads_out(q)])


def expert(got, gate, up, down):
    full = TPN * QW
    return pl.pallas_call(
        expert_kernel,
        in_specs=[ANY] * 4,
        out_specs=[ANY] * 4,
        out_shape=[
            jax.ShapeDtypeStruct((640, 2 * FFQ), BF),
            jax.ShapeDtypeStruct((full, FFQ), BF),
            jax.ShapeDtypeStruct((full, FFQ), BF),
            jax.ShapeDtypeStruct((FFQ, full), BF),
        ],
        scratch_shapes=[
            pltpu.VMEM((TPN, 640, QW), BF),
            pltpu.VMEM((TPN, 640, QW), BF),
            pltpu.VMEM((TPN, 256, QW), BF),
            pltpu.VMEM((TPN, QW, FFQ), BF),
            pltpu.VMEM((TPN, QW, FFQ), BF),
            pltpu.VMEM((TPN, FFQ, QW), BF),
            pltpu.VMEM((2, TPN, QW, FFQ), BF),
            pltpu.VMEM((TPN, FFQ, QW), BF),
            pltpu.VMEM((640, FFQ), F32),
            pltpu.VMEM((640, FFQ), F32),
            pltpu.VMEM((640, FFQ), F32),
            pltpu.VMEM((640, 2 * FFQ), BF),
            pltpu.VMEM((640, FFQ), BF),
            pltpu.SemaphoreType.DMA((TPN, 5)),
            pltpu.SemaphoreType.DMA((3, TPN)),
            pltpu.SemaphoreType.DMA,
            pltpu.SemaphoreType.DMA((3, TPN)),
        ],
        compiler_params=pltpu.CompilerParams(vmem_limit_bytes=60 * 1024 * 1024),
        name="expert",
    )(got, gate, up, down)


def back_steps(
    start, fill, slopes, gate, up, combine, grad,
    part, v_gate, v_up, v_slopes, near, final, back, held, give, second,
    near_send, near_recv, own_sem, ret_send, ret_recv, two_send, two_recv, all_send, all_recv,
    w_sem, slope_sem, met_sem,
):
    s = lax.axis_index("sp")
    x = lax.axis_index("tp")
    right, left = lax.rem(x + 1, TPN), lax.rem(x + 3, TPN)

    def partners(c):
        odd = lax.rem(c, 2)
        one = x + 1 - 2 * lax.rem(x, 2)
        other = TPN - 1 - x
        return one + odd * (other - one), other + odd * (one - other)

    def to_pair(c, j):
        pair, _ = partners(c)
        quarter = pair if j == 0 else lax.rem(x + 2, TPN)
        return remote(
            part.at[quarter, c],
            near.at[c, j],
            near_send.at[c, j],
            near_recv.at[c, j],
            (s, pair),
        )

    def own_back(c):
        return pltpu.make_async_copy(final.at[c, s], back.at[c, s], own_sem.at[c])

    def home(c, k, target):
        return remote(
            final.at[c, target], back.at[c, s], ret_send.at[c, k], ret_recv.at[c, k], (target, x)
        )

    def to_other(c):
        _, other = partners(c)
        return remote(give.at[c], second.at[c], two_send.at[c], two_recv.at[c], (s, other))

    def spread(c, side):
        src = grad.at[x, c]
        return remote(
            src, src, all_send.at[side, 0, c], all_recv.at[side, 0, c], (s, (right, left)[side])
        )

    def spread_on(c, side):
        src = grad.at[(left, right)[side], c, pl.ds(side * 128, 128), :]
        return remote(
            src, src, all_send.at[side, 1, c], all_recv.at[side, 1, c], (s, (right, left)[side])
        )

    def begin(c):
        for j in range(2):
            to_pair(c, j).start()

    def load(q):
        rows = pl.ds(pl.multiple_of(q * QW, QW), QW)
        return (
            pltpu.make_async_copy(gate.at[rows, :], v_gate.at[q], w_sem.at[0, q]),
            pltpu.make_async_copy(up.at[rows, :], v_up.at[q], w_sem.at[1, q]),
        )

    def begin_load(q):
        for copy in load(q):
            copy.start()

    def rows_of(q):
        for copy in load(q):
            copy.wait()
        rows = (
            contract(v_slopes[:, 0:FFQ], v_gate[q], 1, 1)
            + contract(v_slopes[:, FFQ : 2 * FFQ], v_up[q], 1, 1)
        ).astype(BF)
        for c in range(CHUNKS):
            part[q, c] = rows[:, c * CW : (c + 1) * CW]

    take = pltpu.make_async_copy(slopes, v_slopes, slope_sem)
    take.start()
    loop(0, TPN, begin_load)
    start()
    take.wait()
    loop(0, TPN // 2, rows_of)
    hello_lines(s, x, met_sem)
    loop(TPN // 2, TPN, rows_of)
    hello_cores(s, x, met_sem)
    met(met_sem)
    loop(0, CHUNKS, begin)
    fill()

    def open_chunk(t):
        _, other = partners(t)
        for j in range(2):
            to_pair(t, j).wait_recv()
            mine = part[x if j == 0 else other, t]
            total = (mine.astype(F32) + near[t, j].astype(F32)).astype(BF)
            lanes = slice(j * CW, (j + 1) * CW)
            final[t, :, 0:8, lanes] = total[0:256].reshape(32, 8, CW)
            final[t, :, 8:16, lanes] = total[256:512].reshape(32, 8, CW)
            mixed = total[512:640].reshape(16, 8, CW)
            final[t, 0:16, 16:24, lanes] = mixed
            final[t, 16:32, 16:24, lanes] = mixed
        own_back(t).start()
        for k in range(1, SPN):
            home(t, k, peer(s, k)).start()

    def close_chunk(c):
        own_back(c).wait()
        loop(1, SPN, lambda k: home(c, k, s ^ 1).wait_recv())
        summed = contract(combine[...], back[c].reshape(768, 2 * CW), 1, 0)
        held[c] = summed[:, 0:CW]
        give[c] = summed[:, CW : 2 * CW].astype(BF)
        to_other(c).start()

    def share(c):
        to_other(c).wait_recv()
        grad[x, c] = (held[c] + second[c].astype(F32)).astype(BF)
        for side in range(2):
            spread(c, side).start()

    def share_on(c):
        for side in range(2):
            spread(c, side).wait_recv()
            spread_on(c, side).start()

    lag = 3

    def stage(t):
        open_chunk(t)

        @pl.when(t >= lag)
        def _():
            close_chunk(t - lag)

    loop(0, CHUNKS, stage)
    loop(0, CHUNKS - lag, share)
    loop(CHUNKS - lag, CHUNKS, close_chunk)
    loop(0, CHUNKS - lag, share_on)
    loop(CHUNKS - lag, CHUNKS, share)
    loop(CHUNKS - lag, CHUNKS, share_on)

    def finish(c):
        for j in range(2):
            to_pair(c, j).wait_send()
        to_other(c).wait_send()
        for side in range(2):
            spread(c, side).wait_send()
            spread_on(c, side).wait_send()
            spread_on(c, side).wait_recv()
        loop(1, SPN, lambda k: home(c, k, s ^ 1).wait_send())

    loop(0, CHUNKS, finish)


def expm1_negative(v):
    series = 1.0 + v * (1.0 / 9.0)
    for k in (8, 7, 6, 5, 4, 3, 2):
        series = 1.0 + v * (1.0 / k) * series
    return jnp.where(v > -0.5, v * series, jnp.exp(v) - 1.0)


def scan_rows(coeff, value, reverse):
    rows = lax.broadcasted_iota(I32, coeff.shape, 0)
    for k in (1, 2, 4, 8, 16, 32, 64, 128):
        if reverse:
            inside = rows < TOK - k
            shift = TOK - k
        else:
            inside = rows >= k
            shift = k
        coeff_far = jnp.where(inside, pltpu.roll(coeff, shift, 0), 1.0)
        value_far = jnp.where(inside, pltpu.roll(value, shift, 0), 0.0)
        value = value + coeff * value_far
        coeff = coeff * coeff_far
    return coeff, value


def mixer_steps(
    stream, out_grad, gain, grad, states, branch, out_proj, conv, decay_map, input_map, base, shift,
    branch_grad, conv_grad, proj_grad,
    v_stream, v_out, v_proj, v_states, v_shift, v_branch, v_conv, v_decay, v_input,
    sgb, dot, scale, lru, pulled, linear, coeffs, factors,
    ends, edges, pieces, pair, paired, far_y, far_z, sum_y, sum_z, last_y, last_z,
    big_sem, small_sem, end_send, end_recv, pair_send, pair_recv, one_send, one_recv,
    two_send, two_recv,
):
    s = lax.axis_index("sp")
    x = lax.axis_index("tp")
    z, y, core = s // 8, (s // 2) % 4, s % 2

    def big(which, q):
        cols = pl.ds(pl.multiple_of(q * QW, QW), QW)
        src, dst = (
            (stream.at[:, cols], v_stream.at[q]),
            (out_grad.at[:, cols], v_out.at[q]),
            (out_proj.at[cols, :], v_proj.at[q]),
        )[which]
        return pltpu.make_async_copy(src, dst, big_sem.at[which, q])

    small = [
        pltpu.make_async_copy(src, dst, small_sem.at[k])
        for k, (src, dst) in enumerate(
            (
                (conv, v_conv),
                (decay_map, v_decay),
                (input_map, v_input),
                (shift, v_shift),
                (states, v_states),
                (branch, v_branch),
            )
        )
    ]
    def begin(q):
        for which in range(3):
            big(which, q).start()

    def start():
        for copy in small:
            copy.start()
        loop(0, TPN, begin)

    def gates():
        for copy in small:
            copy.wait()

        c = v_conv[...].astype(F32)
        rows = lax.broadcasted_iota(I32, (TOK, FFQ), 0)
        for d in range(2):
            r = jax.nn.sigmoid(contract(v_conv[...], v_decay[d], 1, 0))
            i = jax.nn.sigmoid(contract(v_conv[...], v_input[d], 1, 0))
            rate = (-rate_scale) * base[d : d + 1, :]
            log_decay = r * rate + v_shift[d]
            decay = jnp.exp(log_decay)
            width = jnp.sqrt(-expm1_negative(2.0 * log_decay))
            drive = width * i * c
            if d == 0:
                coeffs[d] = jnp.where(rows == TOK - 1, 1.0, pltpu.roll(decay, TOK - 1, 0))
                ends[0:1, :] = decay[0:1]
            else:
                coeffs[d] = jnp.where(rows == 0, 1.0, pltpu.roll(decay, 1, 0))
                ends[2:3, :] = decay[TOK - 1 : TOK]
            linear[d, 0] = width * i
            linear[d, 1] = (
                ((v_states[d] - drive) - i * c * decay * decay / width) * rate * r * (1.0 - r)
            )
            linear[d, 2] = width * c * i * (1.0 - i)
        total = v_states[0] + v_states[1]
        b = v_branch[...].astype(F32)
        root = 0.7978845608028654
        tanh = jnp.tanh(root * (b + 0.044715 * b * b * b))
        gelu = 0.5 * b * (1.0 + tanh)
        slope = 0.5 * (1.0 + tanh) + 0.5 * b * (1.0 - tanh * tanh) * root * (
            1.0 + 3.0 * 0.044715 * b * b
        )
        lru[...] = (total * gelu).astype(BF)
        factors[0] = total * slope
        factors[1] = gelu

        def squares(q, carry):
            big(0, q).wait()
            v = v_stream[q].astype(F32)
            return carry + jnp.sum(v * v, axis=1, keepdims=True)

        square = lax.fori_loop(0, TPN, squares, jnp.zeros((TOK, 1), F32))
        scale[...] = jnp.broadcast_to(
            lax.rsqrt(square * (1.0 / (TPN * QW)) + norm_eps), (TOK, 128)
        )

    def rest():
        def grad_of(q):
            return jnp.concatenate([grad[q, c] for c in range(CHUNKS)], axis=1).astype(F32)

        def projected(q, carry):
            g = gain[:, pl.ds(pl.multiple_of(q * QW, QW), QW)].astype(F32)
            w = v_stream[q].astype(F32) * (g * grad_of(q))
            return carry + jnp.sum(w, axis=1, keepdims=True)

        along = lax.fori_loop(0, TPN, projected, jnp.zeros((TOK, 1), F32))
        dot[...] = jnp.broadcast_to(along * scale[:, 0:1] * (1.0 / (TPN * QW)), (TOK, 128))
        pulled[...] = jnp.zeros_like(pulled)

        def rows_grad(q):
            big(1, q).wait()
            big(2, q).wait()
            r = scale[:, 0:1]
            unit = v_stream[q].astype(F32) * r
            scaled = gain[:, pl.ds(pl.multiple_of(q * QW, QW), QW)].astype(F32) * grad_of(q)
            v = (v_out[q].astype(F32) + r * (scaled - unit * dot[:, 0:1])).astype(BF)
            sgb[q] = v
            pulled[...] += contract(v, v_proj[q], 1, 0)

        loop(0, TPN, rows_grad)
        lru_grad = pulled[...]
        branch_grad[...] = lru_grad * factors[0]
        state_grad = lru_grad * factors[1]
        def pair_to(q):
            return remote(
                pieces.at[q, :, 1 - core],
                pair.at[q],
                pair_send.at[q],
                pair_recv.at[q],
                (s + 1 - 2 * core, x),
            )

        def proj(q):
            pieces[q] = (
                contract(sgb[q], lru[...], 0, 0).astype(BF).reshape(TPN, 2, 128, FFQ)
            )
            pair_to(q).start()

        loop(0, TPN, proj)
        for d in range(2):
            reach, inner = scan_rows(coeffs[d], state_grad, d == 0)
            edge = slice(0, 1) if d == 0 else slice(TOK - 1, TOK)
            decay = ends[2 * d : 2 * d + 1, :]
            ends[2 * d : 2 * d + 1, :] = decay * reach[edge]
            ends[2 * d + 1 : 2 * d + 2, :] = decay * inner[edge]
            linear[d, 3] = reach
            linear[d, 4] = inner

        def ends_to(k, target):
            return remote(ends, edges.at[s], end_send.at[k], end_recv.at[k], (target, x))

        for k in range(1, SPN):
            ends_to(k, peer(s, k)).start()
        edges[s] = ends[...]


        def meet(q):
            pair_to(q).wait_recv()
            paired[q] = (pieces[q, :, core].astype(F32) + pair[q].astype(F32)).astype(BF)

        loop(0, TPN, meet)
        first, second = pl.ds(0, 64), pl.ds(64, 64)

        def along_y(k):
            return lax.rem(y + k, 4), (z * 8 + lax.rem(y + k, 4) * 2 + core, x)

        def along_z(k):
            return lax.rem(z + k, 4), (lax.rem(z + k, 4) * 8 + y * 2 + core, x)

        def one(side, k):
            place, target = (along_y, along_z)[side](k)
            if side == 0:
                src, dst = paired.at[:, place, first, :], far_y.at[k - 1]
            else:
                src, dst = paired.at[place, :, second, :], far_z.at[k - 1]
            return remote(src, dst, one_send.at[side, k], one_recv.at[side, k], target)

        def two(side, k):
            place, target = (along_z, along_y)[side](k)
            if side == 0:
                src, dst = sum_y.at[place], last_y.at[k - 1]
            else:
                src, dst = sum_z.at[place], last_z.at[k - 1]
            return remote(src, dst, two_send.at[side, k], two_recv.at[side, k], target)

        for k in (1, 3, 2):
            for side in range(2):
                one(side, k).start()

        for k in range(1, SPN):
            ends_to(k, s ^ 1).wait_recv()

        def carry_in(j, carry):
            later = SPN - 1 - j
            e0, e1 = edges[later], edges[j]
            from_right = jnp.where(later > s, e0[1:2] + e0[0:1] * carry[0], carry[0])
            from_left = jnp.where(j < s, e1[3:4] + e1[2:3] * carry[1], carry[1])
            return from_right, from_left

        none = jnp.zeros((1, FFQ), F32)
        incoming = lax.fori_loop(0, SPN, carry_in, (none, none))

        def back_maps(d):
            adjoint = linear[d, 4] + linear[d, 3] * incoming[d]
            highest = lax.Precision.HIGHEST
            return (
                adjoint * linear[d, 0]
                + contract(adjoint * linear[d, 1], v_decay[d].astype(F32), 1, 1, highest)
                + contract(adjoint * linear[d, 2], v_input[d].astype(F32), 1, 1, highest)
            )

        conv_grad[...] = back_maps(0) + back_maps(1)

        for side in range(2):
            for k in (1, 3, 2):
                one(side, k).wait_recv()
            if side == 0:
                acc = paired[:, y, first, :].astype(F32)
            else:
                acc = paired[z, :, second, :].astype(F32)
            came = (far_y, far_z)[side]
            acc = acc + came[0].astype(F32) + came[1].astype(F32) + came[2].astype(F32)
            (sum_y, sum_z)[side][...] = acc.astype(BF)
            for k in (1, 3, 2):
                two(side, k).start()

        for side in range(2):
            for k in (1, 3, 2):
                two(side, k).wait_recv()
            came = (last_y, last_z)[side]
            acc = (sum_y[z] if side == 0 else sum_z[y]).astype(F32)
            acc = acc + came[0].astype(F32) + came[1].astype(F32) + came[2].astype(F32)
            proj_grad[pl.ds(side * 64, 64), :] = acc

        for side in range(2):
            for k in (1, 3, 2):
                one(side, k).wait_send()
                two(side, k).wait_send()
        loop(1, SPN, lambda k: ends_to(k, s ^ 1).wait_send())
        loop(0, TPN, lambda q: pair_to(q).wait_send())

    return start, gates, rest


def tail_kernel(
    slopes, gate, up, combine, stream, out_grad, gain, states, branch, out_proj, conv, decay_map,
    input_map, base, shift, branch_grad, conv_grad, proj_grad, grad, *scratch,
):
    hello(lax.axis_index("sp"), lax.axis_index("tp"))
    start, gates, rest = mixer_steps(
        stream, out_grad, gain, grad, states, branch, out_proj, conv, decay_map, input_map, base,
        shift, branch_grad, conv_grad, proj_grad, *scratch[NBACK:],
    )
    back_steps(start, gates, slopes, gate, up, combine, grad, *scratch[:NBACK])
    rest()


def tail(*operands):
    whole = (TPN, TOK, QW)
    square = (TOK, FFQ)
    dma = pltpu.SemaphoreType.DMA
    return pl.pallas_call(
        tail_kernel,
        in_specs=[ANY, ANY, ANY, VM, ANY, ANY, VM, ANY, ANY, ANY, ANY, ANY, ANY, VM, ANY],
        out_specs=[VM] * 3,
        out_shape=[
            jax.ShapeDtypeStruct(square, F32),
            jax.ShapeDtypeStruct(square, F32),
            jax.ShapeDtypeStruct((128, FFQ), F32),
        ],
        scratch_shapes=[
            pltpu.VMEM((TPN, CHUNKS, TOK, CW), BF),
            pltpu.VMEM((TPN, CHUNKS, 640, CW), BF),
            pltpu.VMEM((TPN, QW, FFQ), BF),
            pltpu.VMEM((TPN, QW, FFQ), BF),
            pltpu.VMEM((640, 2 * FFQ), BF),
            pltpu.VMEM((CHUNKS, 2, 640, CW), BF),
            pltpu.VMEM((CHUNKS, SPN, 24, 2 * CW), BF),
            pltpu.VMEM((CHUNKS, SPN, 24, 2 * CW), BF),
            pltpu.VMEM((CHUNKS, TOK, CW), F32),
            pltpu.VMEM((CHUNKS, TOK, CW), BF),
            pltpu.VMEM((CHUNKS, TOK, CW), BF),
            dma((CHUNKS, 2)),
            dma((CHUNKS, 2)),
            dma((CHUNKS,)),
            dma((CHUNKS, SPN)),
            dma((CHUNKS, SPN)),
            dma((CHUNKS,)),
            dma((CHUNKS,)),
            dma((2, 2, CHUNKS)),
            dma((2, 2, CHUNKS)),
            dma((2, TPN)),
            dma,
            pltpu.SemaphoreType.REGULAR((2,)),
            pltpu.VMEM(whole, BF),
            pltpu.VMEM(whole, BF),
            pltpu.VMEM((TPN, QW, FFQ), BF),
            pltpu.VMEM((2,) + square, F32),
            pltpu.VMEM((2,) + square, F32),
            pltpu.VMEM(square, BF),
            pltpu.VMEM(square, BF),
            pltpu.VMEM((2, FFQ, FFQ), BF),
            pltpu.VMEM((2, FFQ, FFQ), BF),
            pltpu.VMEM(whole, BF),
            pltpu.VMEM((TOK, 128), F32),
            pltpu.VMEM((TOK, 128), F32),
            pltpu.VMEM(square, BF),
            pltpu.VMEM(square, F32),
            pltpu.VMEM((2, 5) + square, F32),
            pltpu.VMEM((2,) + square, F32),
            pltpu.VMEM((2,) + square, F32),
            pltpu.VMEM((4, FFQ), F32),
            pltpu.VMEM((SPN, 4, FFQ), F32),
            pltpu.VMEM((4, 4, 2, 128, FFQ), BF),
            pltpu.VMEM((4, 4, 128, FFQ), BF),
            pltpu.VMEM((4, 4, 128, FFQ), BF),
            pltpu.VMEM((3, 4, 64, FFQ), BF),
            pltpu.VMEM((3, 4, 64, FFQ), BF),
            pltpu.VMEM((4, 64, FFQ), BF),
            pltpu.VMEM((4, 64, FFQ), BF),
            pltpu.VMEM((3, 64, FFQ), BF),
            pltpu.VMEM((3, 64, FFQ), BF),
            dma((3, TPN)),
            dma((6,)),
            dma((SPN,)),
            dma((SPN,)),
            dma((TPN,)),
            dma((TPN,)),
            dma((2, 4)),
            dma((2, 4)),
            dma((2, 4)),
            dma((2, 4)),
        ],
        compiler_params=pltpu.CompilerParams(
            collective_id=1, has_side_effects=True, vmem_limit_bytes=52 * 1024 * 1024
        ),
        name="tail",
    )(*operands)


def body(
    out_grad,
    stream,
    norm_gain,
    routes,
    route_weight,
    gate_weight,
    up_weight,
    down_weight,
    out_proj,
    conv_out,
    gate_branch,
    decay_map,
    input_map,
    decay_param,
    decay_shift,
    states,
):
    gain = norm_gain[None, :]
    got, combine = dispatch(stream, out_grad, gain, routes.T, route_weight.T)
    slopes, gate_wgrad, up_wgrad, down_wgrad = expert(
        got, gate_weight[0], up_weight[0], down_weight[0]
    )
    base = jax.nn.softplus(-decay_param)
    branch_grad, conv_grad, proj_grad = tail(
        slopes, gate_weight[0], up_weight[0], combine, stream, out_grad, gain, states, gate_branch, out_proj, conv_out,
        decay_map[:, 0], input_map[:, 0], base, decay_shift,
    )
    return (
        conv_grad, branch_grad, proj_grad, gate_wgrad[None], up_wgrad[None], down_wgrad[None]
    )


def solution(mesh):
    in_specs = (
        P(SP, None),
        P(SP, None),
        P(),
        P(SP, None),
        P(SP, None),
        P(SP, None, "tp"),
        P(SP, None, "tp"),
        P(SP, "tp", None),
        P(None, "tp"),
        P(SP, "tp"),
        P(SP, "tp"),
        P(None, "tp", None, None),
        P(None, "tp", None, None),
        P(None, "tp"),
        P(None, SP, "tp"),
        P(None, SP, "tp"),
    )
    out_specs = (
        P(SP, "tp"),
        P(SP, "tp"),
        P(SP, "tp"),
        P(SP, None, "tp"),
        P(SP, None, "tp"),
        P(SP, "tp", None),
    )
    return jax.shard_map(body, mesh=mesh, in_specs=in_specs, out_specs=out_specs, check_vma=False)
```

```python
import functools

import jax
import jax.numpy as jnp
from jax import lax
from jax.experimental import pallas as pl
from jax.experimental.pallas import tpu as pltpu
from jax.sharding import PartitionSpec as P

BF = jnp.bfloat16
F32 = jnp.float32
I32 = jnp.int32
MESH = pl.DeviceIdType.MESH
ANY = pl.BlockSpec(memory_space=pl.ANY)
VM = pl.BlockSpec(memory_space=pltpu.VMEM)

SPN = 32
TPN = 4
TOK = 256
QW = 1024
FFQ = 256
CHUNKS = 8
SP = "sp"
CW = QW // CHUNKS
rate_scale = 8.0
norm_eps = 1e-06
NBACK = 22


def contract(left, right, left_dim, right_dim, precision=None):
    return lax.dot_general(
        left,
        right,
        (((left_dim,), (right_dim,)), ((), ())),
        preferred_element_type=F32,
        precision=precision,
    )


NEAR = (
    (0, 1), (1, 0), (0, 3), (3, 0), (1, 1), (3, 3), (1, 3), (3, 1),
    (0, 2), (2, 0), (1, 2), (2, 1), (3, 2), (2, 3), (2, 2),
)
STEPS = ((0, 0, 1),) + tuple((z, y, c) for c in (0, 1) for z, y in NEAR)


def peer(s, k, sign=1):
    z, y, c = STEPS[k - 1]
    return (
        lax.rem(s // 8 + (z if sign > 0 else 4 - z), 4) * 8
        + lax.rem((s // 2) % 4 + (y if sign > 0 else 4 - y), 4) * 2
        + lax.rem(s % 2 + c, 2)
    )


def tell(sem, target):
    pl.semaphore_signal(sem, inc=1, device_id=target, device_id_type=MESH)


def line_y(s, k):
    return s // 8 * 8 + lax.rem((s // 2) % 4 + k, 4) * 2 + s % 2


def line_z(s, k):
    return lax.rem(s // 8 + k, 4) * 8 + s % 8


def hello(s, x):
    barrier = pltpu.get_barrier_semaphore()
    for k in (1, 3, 2):
        tell(barrier, (line_y(s, k), x))
        tell(barrier, (line_z(s, k), x))
    tell(barrier, (s + 1 - 2 * (s % 2), x))
    for step in (1, TPN - 1):
        tell(barrier, (s, lax.rem(x + step, TPN)))


def hello_lines(s, x, sem):
    pl.semaphore_wait(pltpu.get_barrier_semaphore(), 9)
    for k in (1, 3, 2):
        tell(sem.at[0], (line_y(s, k), x))


def hello_cores(s, x, sem):
    pl.semaphore_wait(sem.at[0], 3)
    tell(sem.at[1], (s + 1 - 2 * (s % 2), x))


def met(sem):
    pl.semaphore_wait(sem.at[1], 1)


def remote(src, dst, send_sem, recv_sem, target):
    return pltpu.make_async_remote_copy(
        src_ref=src,
        dst_ref=dst,
        send_sem=send_sem,
        recv_sem=recv_sem,
        device_id=target,
        device_id_type=MESH,
    )


def loop(lower, upper, step):
    def run(d, carry):
        step(d)
        return carry

    lax.fori_loop(lower, upper, run, 0)


def dispatch_kernel(
    stream, out_grad, gain, routes, weight, got, combine,
    send, v_stream, v_out, qi, qc0, qc1, scale,
    load_sem, own_sem, send_sem, recv_sem, fwd_send, fwd_recv, met_sem,
):
    s = lax.axis_index("sp")
    x = lax.axis_index("tp")
    high, low = x // 2, x % 2
    right, left = lax.rem(x + 1, TPN), lax.rem(x + TPN - 1, TPN)
    hello(s, x)

    def columns(h):
        return pl.ds(pl.multiple_of((2 * h + low) * QW, QW), QW)

    def load(h):
        return pltpu.make_async_copy(out_grad.at[:, columns(h)], v_out.at[h], load_sem.at[1 + h])

    whole = pltpu.make_async_copy(stream, v_stream, load_sem.at[0])
    whole.start()
    load(high).start()
    load(1 - high).start()
    diagonal = lax.broadcasted_iota(I32, (TOK, TOK), 0) == lax.broadcasted_iota(
        I32, (TOK, TOK), 1
    )

    def column(row):
        return jnp.sum(jnp.where(diagonal, row.astype(F32), 0.0), axis=1, keepdims=True)

    lanes = lax.broadcasted_iota(I32, (TOK, 128), 1)
    r0 = column(routes[0:1, :]).astype(I32)
    r1 = column(routes[1:2, :]).astype(I32)
    w0, w1 = column(weight[0:1, :]), column(weight[1:2, :])
    hot0 = (r0 == lanes).astype(F32)
    hot1 = (r1 == lanes).astype(F32)
    before = (
        lax.broadcasted_iota(I32, (TOK, TOK), 1) < lax.broadcasted_iota(I32, (TOK, TOK), 0)
    ).astype(F32)
    counts = contract(before.astype(BF), (hot0 + hot1).astype(BF), 1, 0)
    upper = s // 16
    slots = lax.broadcasted_iota(I32, (TOK, 768), 1)

    def places(route, hot):
        rank = jnp.sum(counts * hot, axis=1, keepdims=True).astype(I32)
        pure = (rank // 8) * 256 + route * 8 + rank % 8
        mixed = 512 + route * 8 + (rank - 16)
        of_input = jnp.where(rank < 16, pure, mixed + 4 * upper)
        of_cotan = jnp.where(rank < 16, pure, mixed + 4 * (1 - upper))
        of_return = route * 24 + rank + jnp.where(rank < 16, 0, 4 * upper)
        return tuple((slots == place).astype(F32) for place in (of_input, of_cotan, of_return))

    in0, cot0, ret0 = places(r0, hot0)
    in1, cot1, ret1 = places(r1, hot1)
    qi[...] = (in0 + in1).astype(BF)
    combine[...] = (ret0 + ret1).astype(BF)
    qc0[...] = cot0.astype(BF)
    qc1[...] = cot1.astype(BF)
    hello_lines(s, x, met_sem)
    whole.wait()
    wide = v_stream[...].astype(F32)
    mean = jnp.sum(wide * wide, axis=1, keepdims=True) * (1.0 / (TPN * QW))
    scale[...] = jnp.broadcast_to(lax.rsqrt(mean + norm_eps), (TOK, 128))

    def gather_rows(h):
        load(h).wait()
        cols = columns(h)
        normed = (
            v_stream[:, cols].astype(F32) * scale[:, 0:1] * gain[cols].astype(F32).reshape(1, QW)
        ).astype(BF)
        grad = v_out[h].astype(F32)
        scaled0 = (w0 * grad).astype(BF)
        scaled1 = (w1 * grad).astype(BF)
        for plane in range(3):
            span = slice(plane * 256, plane * 256 + 256)
            rows_in = contract(qi[:, span], normed, 0, 0)
            rows_cot = contract(qc0[:, span], scaled0, 0, 0) + contract(
                qc1[:, span], scaled1, 0, 0
            )
            if plane < 2:
                send[h, plane] = rows_in.astype(BF)
                send[h, plane + 2] = rows_cot.astype(BF)
            else:
                send[h, 4] = (rows_in + rows_cot).astype(BF)

    def rows(i):
        return pl.ds(pl.multiple_of(i * 8, 8), 8)

    def half(turn):
        return high if turn == 0 else 1 - high

    def over(turn, k, target):
        return remote(
            send.at[half(turn), :, rows(target), :],
            got.at[half(turn), low, :, rows(s), :],
            send_sem.at[turn, k],
            recv_sem.at[turn, k],
            (target, x),
        )

    def own(turn):
        return pltpu.make_async_copy(
            send.at[half(turn), :, rows(s), :],
            got.at[half(turn), low, :, rows(s), :],
            own_sem.at[turn],
        )

    def onward(src, dst, k, side):
        return remote(
            src, dst, fwd_send.at[side, k], fwd_recv.at[side, k], (s, (right, left)[side])
        )

    def block(i):
        return got.at[high, low, :, rows(i), :]

    hello_cores(s, x, met_sem)
    gather_rows(high)
    met(met_sem)
    for side in range(2):
        onward(send.at[high, :, rows(s), :], block(s), 0, side).start()
    for turn in range(2):
        if turn == 1:
            gather_rows(1 - high)
        own(turn).start()
        for k in range(1, SPN):
            over(turn, k, peer(s, k)).start()
    for k in range(1, SPN):
        source = peer(s, k, -1)
        over(0, k, source).wait_recv()
        for side in range(2):
            onward(block(source), block(source), k, side).start()
    own(0).wait()
    own(1).wait()

    def finish(k):
        for turn in range(2):
            over(turn, k, s ^ 1).wait_send()
        over(1, k, s ^ 1).wait_recv()

    def finish_onward(k):
        for side in range(2):
            copy = onward(block(s), block(s), k, side)
            copy.wait_send()
            copy.wait_recv()

    loop(1, SPN, finish)
    loop(0, SPN, finish_onward)


def dispatch(stream, out_grad, gain, routes, weight):
    dma = pltpu.SemaphoreType.DMA
    return pl.pallas_call(
        dispatch_kernel,
        in_specs=[ANY, ANY, VM, VM, VM],
        out_specs=[ANY, VM],
        out_shape=[
            jax.ShapeDtypeStruct((2, 2, 5, 256, QW), BF),
            jax.ShapeDtypeStruct((TOK, 768), BF),
        ],
        scratch_shapes=[
            pltpu.VMEM((2, 5, 256, QW), BF),
            pltpu.VMEM((TOK, 4 * QW), BF),
            pltpu.VMEM((2, TOK, QW), BF),
            pltpu.VMEM((TOK, 768), BF),
            pltpu.VMEM((TOK, 768), BF),
            pltpu.VMEM((TOK, 768), BF),
            pltpu.VMEM((TOK, 128), F32),
            dma((3,)),
            dma((2,)),
            dma((2, SPN)),
            dma((2, SPN)),
            dma((2, SPN)),
            dma((2, SPN)),
            pltpu.SemaphoreType.REGULAR((2,)),
        ],
        compiler_params=pltpu.CompilerParams(
            collective_id=0, has_side_effects=True, vmem_limit_bytes=62 * 1024 * 1024
        ),
        name="dispatch",
    )(stream, out_grad, gain, routes, weight)


def swap_halves(v):
    tiles = v.reshape(16, 8, v.shape[1])
    return pltpu.roll(tiles, 4, 1).reshape(v.shape)


def expert_kernel(
    got, gate, up, down, slopes, gate_wg, up_wg, down_wg,
    vin, vcot, vmix, vg, vu, vd, ogu, od, gp, upre, hg, gu, hid,
    in_sem, w_sem, slope_sem, o_sem,
):
    def loads(q):
        hi, lo = q // 2, q % 2
        out = []
        for plane in range(5):
            if plane < 2:
                dst = vin.at[q, pl.ds(plane * 256, 256), :]
            elif plane < 4:
                dst = vcot.at[q, pl.ds((plane - 2) * 256, 256), :]
            else:
                dst = vmix.at[q]
            out.append(pltpu.make_async_copy(got.at[hi, lo, plane], dst, in_sem.at[q, plane]))
        rows = pl.ds(pl.multiple_of(q * QW, QW), QW)
        out.append(pltpu.make_async_copy(gate.at[rows, :], vg.at[q], w_sem.at[0, q]))
        out.append(pltpu.make_async_copy(up.at[rows, :], vu.at[q], w_sem.at[1, q]))
        out.append(pltpu.make_async_copy(down.at[:, rows], vd.at[q], w_sem.at[2, q]))
        return out

    loop(0, TPN, lambda q: [c.start() for c in loads(q)])
    gp[...] = jnp.zeros_like(gp)
    upre[...] = jnp.zeros_like(upre)
    hg[...] = jnp.zeros_like(hg)

    def forward(q):
        for c in loads(q):
            c.wait()
        first = lax.broadcasted_iota(I32, (128, QW), 0) % 8 < 4
        a = vmix[q, 0:128, :].astype(F32)
        b = vmix[q, 128:256, :].astype(F32)
        vin[q, 512:640, :] = jnp.where(first, a, b).astype(BF)
        vcot[q, 512:640, :] = jnp.where(first, b, a).astype(BF)
        rows = vin[q]
        gp[...] += contract(rows, vg[q], 1, 0)
        upre[...] += contract(rows, vu[q], 1, 0)
        hg[...] += contract(vcot[q], vd[q], 1, 1)

    loop(0, TPN, forward)
    hg[512:640, :] = swap_halves(hg[512:640, :])
    gate_pre, up_pre, hidden_grad = gp[...], upre[...], hg[...]
    logistic = jax.nn.sigmoid(gate_pre)
    silu = gate_pre * logistic
    hidden = silu * up_pre
    hid[0:512, :] = hidden[0:512, :].astype(BF)
    hid[512:640, :] = swap_halves(hidden[512:640, :]).astype(BF)
    gu[:, 0:FFQ] = (
        hidden_grad * up_pre * (logistic * (1.0 + gate_pre * (1.0 - logistic)))
    ).astype(BF)
    gu[:, FFQ : 2 * FFQ] = (hidden_grad * silu).astype(BF)

    out = pltpu.make_async_copy(gu, slopes, slope_sem)
    out.start()

    def grads_out(q):
        rows = pl.ds(pl.multiple_of(q * QW, QW), QW)
        return (
            pltpu.make_async_copy(ogu.at[0, q], gate_wg.at[rows, :], o_sem.at[0, q]),
            pltpu.make_async_copy(ogu.at[1, q], up_wg.at[rows, :], o_sem.at[1, q]),
            pltpu.make_async_copy(od.at[q], down_wg.at[:, rows], o_sem.at[2, q]),
        )

    def weights(q):
        both = contract(vin[q], gu[...], 0, 0)
        ogu[0, q] = both[:, 0:FFQ].astype(BF)
        ogu[1, q] = both[:, FFQ : 2 * FFQ].astype(BF)
        od[q] = contract(hid[...], vcot[q], 0, 0).astype(BF)
        for c in grads_out(q):
            c.start()

    loop(0, TPN, weights)
    out.wait()
    loop(0, TPN, lambda q: [c.wait() for c in grads_out(q)])


def expert(got, gate, up, down):
    full = TPN * QW
    return pl.pallas_call(
        expert_kernel,
        in_specs=[ANY] * 4,
        out_specs=[ANY] * 4,
        out_shape=[
            jax.ShapeDtypeStruct((640, 2 * FFQ), BF),
            jax.ShapeDtypeStruct((full, FFQ), BF),
            jax.ShapeDtypeStruct((full, FFQ), BF),
            jax.ShapeDtypeStruct((FFQ, full), BF),
        ],
        scratch_shapes=[
            pltpu.VMEM((TPN, 640, QW), BF),
            pltpu.VMEM((TPN, 640, QW), BF),
            pltpu.VMEM((TPN, 256, QW), BF),
            pltpu.VMEM((TPN, QW, FFQ), BF),
            pltpu.VMEM((TPN, QW, FFQ), BF),
            pltpu.VMEM((TPN, FFQ, QW), BF),
            pltpu.VMEM((2, TPN, QW, FFQ), BF),
            pltpu.VMEM((TPN, FFQ, QW), BF),
            pltpu.VMEM((640, FFQ), F32),
            pltpu.VMEM((640, FFQ), F32),
            pltpu.VMEM((640, FFQ), F32),
            pltpu.VMEM((640, 2 * FFQ), BF),
            pltpu.VMEM((640, FFQ), BF),
            pltpu.SemaphoreType.DMA((TPN, 5)),
            pltpu.SemaphoreType.DMA((3, TPN)),
            pltpu.SemaphoreType.DMA,
            pltpu.SemaphoreType.DMA((3, TPN)),
        ],
        compiler_params=pltpu.CompilerParams(vmem_limit_bytes=60 * 1024 * 1024),
        name="expert",
    )(got, gate, up, down)


def back_steps(
    start, fill, slopes, gate, up, combine, grad,
    part, v_gate, v_up, v_slopes, near, final, back, held, give, second,
    near_send, near_recv, own_sem, ret_send, ret_recv, two_send, two_recv, all_send, all_recv,
    w_sem, slope_sem, met_sem,
):
    s = lax.axis_index("sp")
    x = lax.axis_index("tp")
    right, left = lax.rem(x + 1, TPN), lax.rem(x + 3, TPN)

    def partners(c):
        odd = lax.rem(c, 2)
        one = x + 1 - 2 * lax.rem(x, 2)
        other = TPN - 1 - x
        return one + odd * (other - one), other + odd * (one - other)

    def to_pair(c, j):
        pair, _ = partners(c)
        quarter = pair if j == 0 else lax.rem(x + 2, TPN)
        return remote(
            part.at[quarter, c],
            near.at[c, j],
            near_send.at[c, j],
            near_recv.at[c, j],
            (s, pair),
        )

    def own_back(c):
        return pltpu.make_async_copy(final.at[c, s], back.at[c, s], own_sem.at[c])

    def home(c, k, target):
        return remote(
            final.at[c, target], back.at[c, s], ret_send.at[c, k], ret_recv.at[c, k], (target, x)
        )

    def to_other(c):
        _, other = partners(c)
        return remote(give.at[c], second.at[c], two_send.at[c], two_recv.at[c], (s, other))

    def spread(c, side):
        src = grad.at[x, c]
        return remote(
            src, src, all_send.at[side, 0, c], all_recv.at[side, 0, c], (s, (right, left)[side])
        )

    def spread_on(c, side):
        src = grad.at[(left, right)[side], c, pl.ds(side * 128, 128), :]
        return remote(
            src, src, all_send.at[side, 1, c], all_recv.at[side, 1, c], (s, (right, left)[side])
        )

    def begin(c):
        for j in range(2):
            to_pair(c, j).start()

    def load(q):
        rows = pl.ds(pl.multiple_of(q * QW, QW), QW)
        return (
            pltpu.make_async_copy(gate.at[rows, :], v_gate.at[q], w_sem.at[0, q]),
            pltpu.make_async_copy(up.at[rows, :], v_up.at[q], w_sem.at[1, q]),
        )

    def begin_load(q):
        for copy in load(q):
            copy.start()

    def rows_of(q):
        for copy in load(q):
            copy.wait()
        rows = (
            contract(v_slopes[:, 0:FFQ], v_gate[q], 1, 1)
            + contract(v_slopes[:, FFQ : 2 * FFQ], v_up[q], 1, 1)
        ).astype(BF)
        for c in range(CHUNKS):
            part[q, c] = rows[:, c * CW : (c + 1) * CW]

    take = pltpu.make_async_copy(slopes, v_slopes, slope_sem)
    take.start()
    loop(0, TPN, begin_load)
    start()
    take.wait()
    loop(0, TPN // 2, rows_of)
    hello_lines(s, x, met_sem)
    loop(TPN // 2, TPN, rows_of)
    hello_cores(s, x, met_sem)
    met(met_sem)
    loop(0, CHUNKS, begin)
    fill()

    def open_chunk(t):
        _, other = partners(t)
        for j in range(2):
            to_pair(t, j).wait_recv()
            mine = part[x if j == 0 else other, t]
            total = (mine.astype(F32) + near[t, j].astype(F32)).astype(BF)
            lanes = slice(j * CW, (j + 1) * CW)
            final[t, :, 0:8, lanes] = total[0:256].reshape(32, 8, CW)
            final[t, :, 8:16, lanes] = total[256:512].reshape(32, 8, CW)
            mixed = total[512:640].reshape(16, 8, CW)
            final[t, 0:16, 16:24, lanes] = mixed
            final[t, 16:32, 16:24, lanes] = mixed
        own_back(t).start()
        for k in range(1, SPN):
            home(t, k, peer(s, k)).start()

    def close_chunk(c):
        own_back(c).wait()
        loop(1, SPN, lambda k: home(c, k, s ^ 1).wait_recv())
        summed = contract(combine[...], back[c].reshape(768, 2 * CW), 1, 0)
        held[c] = summed[:, 0:CW]
        give[c] = summed[:, CW : 2 * CW].astype(BF)
        to_other(c).start()

    def share(c):
        to_other(c).wait_recv()
        grad[x, c] = (held[c] + second[c].astype(F32)).astype(BF)
        for side in range(2):
            spread(c, side).start()

    def share_on(c):
        for side in range(2):
            spread(c, side).wait_recv()
            spread_on(c, side).start()

    lag = 2

    def stage(t):
        open_chunk(t)

        @pl.when(t >= lag)
        def _():
            close_chunk(t - lag)

    loop(0, CHUNKS, stage)
    early = CHUNKS - 3
    loop(0, early, share)
    close_chunk(CHUNKS - 2)
    loop(0, early, share_on)
    share(CHUNKS - 3)
    close_chunk(CHUNKS - 1)
    share(CHUNKS - 2)
    share_on(CHUNKS - 3)
    share(CHUNKS - 1)
    share_on(CHUNKS - 2)
    share_on(CHUNKS - 1)

    def finish(c):
        for j in range(2):
            to_pair(c, j).wait_send()
        to_other(c).wait_send()
        for side in range(2):
            spread(c, side).wait_send()
            spread_on(c, side).wait_send()
            spread_on(c, side).wait_recv()
        loop(1, SPN, lambda k: home(c, k, s ^ 1).wait_send())

    loop(0, CHUNKS, finish)


def expm1_negative(v):
    series = 1.0 + v * (1.0 / 9.0)
    for k in (8, 7, 6, 5, 4, 3, 2):
        series = 1.0 + v * (1.0 / k) * series
    return jnp.where(v > -0.5, v * series, jnp.exp(v) - 1.0)


def scan_rows(coeff, value, reverse):
    rows = lax.broadcasted_iota(I32, coeff.shape, 0)
    for k in (1, 2, 4, 8, 16, 32, 64, 128):
        if reverse:
            inside = rows < TOK - k
            shift = TOK - k
        else:
            inside = rows >= k
            shift = k
        coeff_far = jnp.where(inside, pltpu.roll(coeff, shift, 0), 1.0)
        value_far = jnp.where(inside, pltpu.roll(value, shift, 0), 0.0)
        value = value + coeff * value_far
        coeff = coeff * coeff_far
    return coeff, value


def mixer_steps(
    stream, out_grad, gain, grad, states, branch, out_proj, conv, decay_map, input_map, base, shift,
    branch_grad, conv_grad, proj_grad,
    v_stream, v_out, v_proj, v_states, v_shift, v_branch, v_conv, v_decay, v_input,
    sgb, dot, scale, lru, pulled, linear, coeffs, factors,
    ends, edges, pieces, pair, paired, far_y, far_z, sum_y, sum_z, last_y, last_z,
    big_sem, small_sem, end_send, end_recv, pair_send, pair_recv, one_send, one_recv,
    two_send, two_recv,
):
    s = lax.axis_index("sp")
    x = lax.axis_index("tp")
    z, y, core = s // 8, (s // 2) % 4, s % 2

    def big(which, q):
        cols = pl.ds(pl.multiple_of(q * QW, QW), QW)
        src, dst = (
            (stream.at[:, cols], v_stream.at[q]),
            (out_grad.at[:, cols], v_out.at[q]),
            (out_proj.at[cols, :], v_proj.at[q]),
        )[which]
        return pltpu.make_async_copy(src, dst, big_sem.at[which, q])

    small = [
        pltpu.make_async_copy(src, dst, small_sem.at[k])
        for k, (src, dst) in enumerate(
            (
                (conv, v_conv),
                (decay_map, v_decay),
                (input_map, v_input),
                (shift, v_shift),
                (states, v_states),
                (branch, v_branch),
            )
        )
    ]
    def begin(q):
        for which in range(3):
            big(which, q).start()

    def start():
        for copy in small:
            copy.start()
        loop(0, TPN, begin)

    def gates():
        for copy in small:
            copy.wait()

        c = v_conv[...].astype(F32)
        rows = lax.broadcasted_iota(I32, (TOK, FFQ), 0)
        for d in range(2):
            r = jax.nn.sigmoid(contract(v_conv[...], v_decay[d], 1, 0))
            i = jax.nn.sigmoid(contract(v_conv[...], v_input[d], 1, 0))
            rate = (-rate_scale) * base[d : d + 1, :]
            log_decay = r * rate + v_shift[d]
            decay = jnp.exp(log_decay)
            width = jnp.sqrt(-expm1_negative(2.0 * log_decay))
            drive = width * i * c
            if d == 0:
                coeffs[d] = jnp.where(rows == TOK - 1, 1.0, pltpu.roll(decay, TOK - 1, 0))
                ends[0:1, :] = decay[0:1]
            else:
                coeffs[d] = jnp.where(rows == 0, 1.0, pltpu.roll(decay, 1, 0))
                ends[2:3, :] = decay[TOK - 1 : TOK]
            linear[d, 0] = width * i
            linear[d, 1] = (
                ((v_states[d] - drive) - i * c * decay * decay / width) * rate * r * (1.0 - r)
            )
            linear[d, 2] = width * c * i * (1.0 - i)
        total = v_states[0] + v_states[1]
        b = v_branch[...].astype(F32)
        root = 0.7978845608028654
        tanh = jnp.tanh(root * (b + 0.044715 * b * b * b))
        gelu = 0.5 * b * (1.0 + tanh)
        slope = 0.5 * (1.0 + tanh) + 0.5 * b * (1.0 - tanh * tanh) * root * (
            1.0 + 3.0 * 0.044715 * b * b
        )
        lru[...] = (total * gelu).astype(BF)
        factors[0] = total * slope
        factors[1] = gelu

        def squares(q, carry):
            big(0, q).wait()
            v = v_stream[q].astype(F32)
            return carry + jnp.sum(v * v, axis=1, keepdims=True)

        square = lax.fori_loop(0, TPN, squares, jnp.zeros((TOK, 1), F32))
        scale[...] = jnp.broadcast_to(
            lax.rsqrt(square * (1.0 / (TPN * QW)) + norm_eps), (TOK, 128)
        )

    def rest():
        def grad_of(q):
            return jnp.concatenate([grad[q, c] for c in range(CHUNKS)], axis=1).astype(F32)

        def projected(q, carry):
            g = gain[pl.ds(pl.multiple_of(q * QW, QW), QW)].astype(F32).reshape(1, QW)
            w = v_stream[q].astype(F32) * (g * grad_of(q))
            return carry + jnp.sum(w, axis=1, keepdims=True)

        along = lax.fori_loop(0, TPN, projected, jnp.zeros((TOK, 1), F32))
        dot[...] = jnp.broadcast_to(along * scale[:, 0:1] * (1.0 / (TPN * QW)), (TOK, 128))
        pulled[...] = jnp.zeros_like(pulled)

        def rows_grad(q):
            big(1, q).wait()
            big(2, q).wait()
            r = scale[:, 0:1]
            unit = v_stream[q].astype(F32) * r
            scaled = gain[pl.ds(pl.multiple_of(q * QW, QW), QW)].astype(F32).reshape(1, QW) * grad_of(q)
            v = (v_out[q].astype(F32) + r * (scaled - unit * dot[:, 0:1])).astype(BF)
            sgb[q] = v
            pulled[...] += contract(v, v_proj[q], 1, 0)

        loop(0, TPN, rows_grad)
        lru_grad = pulled[...]
        branch_grad[...] = lru_grad * factors[0]
        state_grad = lru_grad * factors[1]
        def pair_to(q):
            return remote(
                pieces.at[q, :, 1 - core],
                pair.at[q],
                pair_send.at[q],
                pair_recv.at[q],
                (s + 1 - 2 * core, x),
            )

        def proj(q):
            pieces[q] = (
                contract(sgb[q], lru[...], 0, 0).astype(BF).reshape(TPN, 2, 128, FFQ)
            )
            pair_to(q).start()

        loop(0, TPN, proj)
        for d in range(2):
            reach, inner = scan_rows(coeffs[d], state_grad, d == 0)
            edge = slice(0, 1) if d == 0 else slice(TOK - 1, TOK)
            decay = ends[2 * d : 2 * d + 1, :]
            ends[2 * d : 2 * d + 1, :] = decay * reach[edge]
            ends[2 * d + 1 : 2 * d + 2, :] = decay * inner[edge]
            linear[d, 3] = reach
            linear[d, 4] = inner

        def ends_to(k, target):
            return remote(ends, edges.at[s], end_send.at[k], end_recv.at[k], (target, x))

        for k in range(1, SPN):
            ends_to(k, peer(s, k)).start()
        edges[s] = ends[...]


        def meet(q):
            pair_to(q).wait_recv()
            paired[q] = (pieces[q, :, core].astype(F32) + pair[q].astype(F32)).astype(BF)

        loop(0, TPN, meet)
        first, second = pl.ds(0, 64), pl.ds(64, 64)

        def along_y(k):
            return lax.rem(y + k, 4), (z * 8 + lax.rem(y + k, 4) * 2 + core, x)

        def along_z(k):
            return lax.rem(z + k, 4), (lax.rem(z + k, 4) * 8 + y * 2 + core, x)

        def one(side, k):
            place, target = (along_y, along_z)[side](k)
            if side == 0:
                src, dst = paired.at[:, place, first, :], far_y.at[k - 1]
            else:
                src, dst = paired.at[place, :, second, :], far_z.at[k - 1]
            return remote(src, dst, one_send.at[side, k], one_recv.at[side, k], target)

        def two(side, k):
            place, target = (along_z, along_y)[side](k)
            if side == 0:
                src, dst = sum_y.at[place], last_y.at[k - 1]
            else:
                src, dst = sum_z.at[place], last_z.at[k - 1]
            return remote(src, dst, two_send.at[side, k], two_recv.at[side, k], target)

        for k in (1, 3, 2):
            for side in range(2):
                one(side, k).start()

        for k in range(1, SPN):
            ends_to(k, s ^ 1).wait_recv()

        def carry_in(j, carry):
            later = SPN - 1 - j
            e0, e1 = edges[later], edges[j]
            from_right = jnp.where(later > s, e0[1:2] + e0[0:1] * carry[0], carry[0])
            from_left = jnp.where(j < s, e1[3:4] + e1[2:3] * carry[1], carry[1])
            return from_right, from_left

        none = jnp.zeros((1, FFQ), F32)
        incoming = lax.fori_loop(0, SPN, carry_in, (none, none))

        def back_maps(d):
            adjoint = linear[d, 4] + linear[d, 3] * incoming[d]
            highest = lax.Precision.HIGHEST
            return (
                adjoint * linear[d, 0]
                + contract(adjoint * linear[d, 1], v_decay[d].astype(F32), 1, 1, highest)
                + contract(adjoint * linear[d, 2], v_input[d].astype(F32), 1, 1, highest)
            )

        conv_grad[...] = back_maps(0) + back_maps(1)

        for side in range(2):
            for k in (1, 3, 2):
                one(side, k).wait_recv()
            if side == 0:
                acc = paired[:, y, first, :].astype(F32)
            else:
                acc = paired[z, :, second, :].astype(F32)
            came = (far_y, far_z)[side]
            acc = acc + came[0].astype(F32) + came[1].astype(F32) + came[2].astype(F32)
            (sum_y, sum_z)[side][...] = acc.astype(BF)
            for k in (1, 3, 2):
                two(side, k).start()

        for side in range(2):
            for k in (1, 3, 2):
                two(side, k).wait_recv()
            came = (last_y, last_z)[side]
            acc = (sum_y[z] if side == 0 else sum_z[y]).astype(F32)
            acc = acc + came[0].astype(F32) + came[1].astype(F32) + came[2].astype(F32)
            proj_grad[pl.ds(side * 64, 64), :] = acc

        for side in range(2):
            for k in (1, 3, 2):
                one(side, k).wait_send()
                two(side, k).wait_send()
        loop(1, SPN, lambda k: ends_to(k, s ^ 1).wait_send())
        loop(0, TPN, lambda q: pair_to(q).wait_send())

    return start, gates, rest


def tail_kernel(
    slopes, gate, up, combine, stream, out_grad, gain, states, branch, out_proj, conv, decay_map,
    input_map, base, shift, branch_grad, conv_grad, proj_grad, grad, *scratch,
):
    hello(lax.axis_index("sp"), lax.axis_index("tp"))
    start, gates, rest = mixer_steps(
        stream, out_grad, gain, grad, states, branch, out_proj, conv, decay_map, input_map, base,
        shift, branch_grad, conv_grad, proj_grad, *scratch[NBACK:],
    )
    back_steps(start, gates, slopes, gate, up, combine, grad, *scratch[:NBACK])
    rest()


def tail(*operands):
    whole = (TPN, TOK, QW)
    square = (TOK, FFQ)
    dma = pltpu.SemaphoreType.DMA
    return pl.pallas_call(
        tail_kernel,
        in_specs=[ANY, ANY, ANY, VM, ANY, ANY, VM, ANY, ANY, ANY, ANY, ANY, ANY, VM, ANY],
        out_specs=[VM] * 3,
        out_shape=[
            jax.ShapeDtypeStruct(square, F32),
            jax.ShapeDtypeStruct(square, F32),
            jax.ShapeDtypeStruct((128, FFQ), F32),
        ],
        scratch_shapes=[
            pltpu.VMEM((TPN, CHUNKS, TOK, CW), BF),
            pltpu.VMEM((TPN, CHUNKS, 640, CW), BF),
            pltpu.VMEM((TPN, QW, FFQ), BF),
            pltpu.VMEM((TPN, QW, FFQ), BF),
            pltpu.VMEM((640, 2 * FFQ), BF),
            pltpu.VMEM((CHUNKS, 2, 640, CW), BF),
            pltpu.VMEM((CHUNKS, SPN, 24, 2 * CW), BF),
            pltpu.VMEM((CHUNKS, SPN, 24, 2 * CW), BF),
            pltpu.VMEM((CHUNKS, TOK, CW), F32),
            pltpu.VMEM((CHUNKS, TOK, CW), BF),
            pltpu.VMEM((CHUNKS, TOK, CW), BF),
            dma((CHUNKS, 2)),
            dma((CHUNKS, 2)),
            dma((CHUNKS,)),
            dma((CHUNKS, SPN)),
            dma((CHUNKS, SPN)),
            dma((CHUNKS,)),
            dma((CHUNKS,)),
            dma((2, 2, CHUNKS)),
            dma((2, 2, CHUNKS)),
            dma((2, TPN)),
            dma,
            pltpu.SemaphoreType.REGULAR((2,)),
            pltpu.VMEM(whole, BF),
            pltpu.VMEM(whole, BF),
            pltpu.VMEM((TPN, QW, FFQ), BF),
            pltpu.VMEM((2,) + square, F32),
            pltpu.VMEM((2,) + square, F32),
            pltpu.VMEM(square, BF),
            pltpu.VMEM(square, BF),
            pltpu.VMEM((2, FFQ, FFQ), BF),
            pltpu.VMEM((2, FFQ, FFQ), BF),
            pltpu.VMEM(whole, BF),
            pltpu.VMEM((TOK, 128), F32),
            pltpu.VMEM((TOK, 128), F32),
            pltpu.VMEM(square, BF),
            pltpu.VMEM(square, F32),
            pltpu.VMEM((2, 5) + square, F32),
            pltpu.VMEM((2,) + square, F32),
            pltpu.VMEM((2,) + square, F32),
            pltpu.VMEM((4, FFQ), F32),
            pltpu.VMEM((SPN, 4, FFQ), F32),
            pltpu.VMEM((4, 4, 2, 128, FFQ), BF),
            pltpu.VMEM((4, 4, 128, FFQ), BF),
            pltpu.VMEM((4, 4, 128, FFQ), BF),
            pltpu.VMEM((3, 4, 64, FFQ), BF),
            pltpu.VMEM((3, 4, 64, FFQ), BF),
            pltpu.VMEM((4, 64, FFQ), BF),
            pltpu.VMEM((4, 64, FFQ), BF),
            pltpu.VMEM((3, 64, FFQ), BF),
            pltpu.VMEM((3, 64, FFQ), BF),
            dma((3, TPN)),
            dma((6,)),
            dma((SPN,)),
            dma((SPN,)),
            dma((TPN,)),
            dma((TPN,)),
            dma((2, 4)),
            dma((2, 4)),
            dma((2, 4)),
            dma((2, 4)),
        ],
        compiler_params=pltpu.CompilerParams(
            collective_id=1, has_side_effects=True, vmem_limit_bytes=52 * 1024 * 1024
        ),
        name="tail",
    )(*operands)


def body(
    out_grad,
    stream,
    norm_gain,
    routes,
    route_weight,
    gate_weight,
    up_weight,
    down_weight,
    out_proj,
    conv_out,
    gate_branch,
    decay_map,
    input_map,
    decay_param,
    decay_shift,
    states,
):
    gain = norm_gain
    got, combine = dispatch(stream, out_grad, gain, routes.T, route_weight.T)
    slopes, gate_wgrad, up_wgrad, down_wgrad = expert(
        got, gate_weight[0], up_weight[0], down_weight[0]
    )
    base = jax.nn.softplus(-decay_param)
    branch_grad, conv_grad, proj_grad = tail(
        slopes, gate_weight[0], up_weight[0], combine, stream, out_grad, gain, states, gate_branch, out_proj, conv_out,
        decay_map[:, 0], input_map[:, 0], base, decay_shift,
    )
    return (
        conv_grad, branch_grad, proj_grad, gate_wgrad[None], up_wgrad[None], down_wgrad[None]
    )


def solution(mesh):
    in_specs = (
        P(SP, None),
        P(SP, None),
        P(),
        P(SP, None),
        P(SP, None),
        P(SP, None, "tp"),
        P(SP, None, "tp"),
        P(SP, "tp", None),
        P(None, "tp"),
        P(SP, "tp"),
        P(SP, "tp"),
        P(None, "tp", None, None),
        P(None, "tp", None, None),
        P(None, "tp"),
        P(None, SP, "tp"),
        P(None, SP, "tp"),
    )
    out_specs = (
        P(SP, "tp"),
        P(SP, "tp"),
        P(SP, "tp"),
        P(SP, None, "tp"),
        P(SP, None, "tp"),
        P(SP, "tp", None),
    )
    return jax.shard_map(body, mesh=mesh, in_specs=in_specs, out_specs=out_specs, check_vma=False)
```

```python
import functools

import jax
import jax.numpy as jnp
from jax import lax
from jax.experimental import pallas as pl
from jax.experimental.pallas import tpu as pltpu
from jax.sharding import PartitionSpec as P

BF = jnp.bfloat16
F32 = jnp.float32
I32 = jnp.int32
MESH = pl.DeviceIdType.MESH
ANY = pl.BlockSpec(memory_space=pl.ANY)
VM = pl.BlockSpec(memory_space=pltpu.VMEM)

SPN = 32
TPN = 4
TOK = 256
QW = 1024
FFQ = 256
CHUNKS = 8
SP = "sp"
CW = QW // CHUNKS
rate_scale = 8.0
norm_eps = 1e-06
NBACK = 22


def contract(left, right, left_dim, right_dim, precision=None):
    return lax.dot_general(
        left,
        right,
        (((left_dim,), (right_dim,)), ((), ())),
        preferred_element_type=F32,
        precision=precision,
    )


NEAR = (
    (0, 1), (1, 0), (0, 3), (3, 0), (1, 1), (3, 3), (1, 3), (3, 1),
    (0, 2), (2, 0), (1, 2), (2, 1), (3, 2), (2, 3), (2, 2),
)
STEPS = ((0, 0, 1),) + tuple((z, y, c) for c in (0, 1) for z, y in NEAR)


def peer(s, k, sign=1):
    z, y, c = STEPS[k - 1]
    return (
        lax.rem(s // 8 + (z if sign > 0 else 4 - z), 4) * 8
        + lax.rem((s // 2) % 4 + (y if sign > 0 else 4 - y), 4) * 2
        + lax.rem(s % 2 + c, 2)
    )


def tell(sem, target):
    pl.semaphore_signal(sem, inc=1, device_id=target, device_id_type=MESH)


def line_y(s, k):
    return s // 8 * 8 + lax.rem((s // 2) % 4 + k, 4) * 2 + s % 2


def line_z(s, k):
    return lax.rem(s // 8 + k, 4) * 8 + s % 8


def hello(s, x):
    barrier = pltpu.get_barrier_semaphore()
    for k in (1, 3, 2):
        tell(barrier, (line_y(s, k), x))
        tell(barrier, (line_z(s, k), x))
    tell(barrier, (s + 1 - 2 * (s % 2), x))
    for step in (1, TPN - 1):
        tell(barrier, (s, lax.rem(x + step, TPN)))


def hello_lines(s, x, sem):
    pl.semaphore_wait(pltpu.get_barrier_semaphore(), 9)
    for k in (1, 3, 2):
        tell(sem.at[0], (line_y(s, k), x))


def hello_cores(s, x, sem):
    pl.semaphore_wait(sem.at[0], 3)
    tell(sem.at[1], (s + 1 - 2 * (s % 2), x))


def met(sem):
    pl.semaphore_wait(sem.at[1], 1)


def remote(src, dst, send_sem, recv_sem, target):
    return pltpu.make_async_remote_copy(
        src_ref=src,
        dst_ref=dst,
        send_sem=send_sem,
        recv_sem=recv_sem,
        device_id=target,
        device_id_type=MESH,
    )


def loop(lower, upper, step):
    def run(d, carry):
        step(d)
        return carry

    lax.fori_loop(lower, upper, run, 0)


def dispatch_kernel(
    stream, out_grad, gain, routes, weight, got, combine,
    send, v_stream, v_out, qi, qc0, qc1, scale,
    load_sem, own_sem, send_sem, recv_sem, fwd_send, fwd_recv, met_sem,
):
    s = lax.axis_index("sp")
    x = lax.axis_index("tp")
    high, low = x // 2, x % 2
    right, left = lax.rem(x + 1, TPN), lax.rem(x + TPN - 1, TPN)
    hello(s, x)

    def columns(h):
        return pl.ds(pl.multiple_of((2 * h + low) * QW, QW), QW)

    def load(h):
        return pltpu.make_async_copy(out_grad.at[:, columns(h)], v_out.at[h], load_sem.at[1 + h])

    whole = pltpu.make_async_copy(stream, v_stream, load_sem.at[0])
    whole.start()
    load(high).start()
    load(1 - high).start()
    diagonal = lax.broadcasted_iota(I32, (TOK, TOK), 0) == lax.broadcasted_iota(
        I32, (TOK, TOK), 1
    )

    def column(row):
        return jnp.sum(jnp.where(diagonal, row.astype(F32), 0.0), axis=1, keepdims=True)

    lanes = lax.broadcasted_iota(I32, (TOK, 128), 1)
    r0 = column(routes[0:1, :]).astype(I32)
    r1 = column(routes[1:2, :]).astype(I32)
    w0, w1 = column(weight[0:1, :]), column(weight[1:2, :])
    hot0 = (r0 == lanes).astype(F32)
    hot1 = (r1 == lanes).astype(F32)
    before = (
        lax.broadcasted_iota(I32, (TOK, TOK), 1) < lax.broadcasted_iota(I32, (TOK, TOK), 0)
    ).astype(F32)
    counts = contract(before.astype(BF), (hot0 + hot1).astype(BF), 1, 0)
    upper = s // 16
    slots = lax.broadcasted_iota(I32, (TOK, 768), 1)

    def places(route, hot):
        rank = jnp.sum(counts * hot, axis=1, keepdims=True).astype(I32)
        pure = (rank // 8) * 256 + route * 8 + rank % 8
        mixed = 512 + route * 8 + (rank - 16)
        of_input = jnp.where(rank < 16, pure, mixed + 4 * upper)
        of_cotan = jnp.where(rank < 16, pure, mixed + 4 * (1 - upper))
        of_return = route * 24 + rank + jnp.where(rank < 16, 0, 4 * upper)
        return tuple((slots == place).astype(F32) for place in (of_input, of_cotan, of_return))

    in0, cot0, ret0 = places(r0, hot0)
    in1, cot1, ret1 = places(r1, hot1)
    qi[...] = (in0 + in1).astype(BF)
    combine[...] = (ret0 + ret1).astype(BF)
    qc0[...] = cot0.astype(BF)
    qc1[...] = cot1.astype(BF)
    hello_lines(s, x, met_sem)
    whole.wait()
    wide = v_stream[...].astype(F32)
    mean = jnp.sum(wide * wide, axis=1, keepdims=True) * (1.0 / (TPN * QW))
    scale[...] = jnp.broadcast_to(lax.rsqrt(mean + norm_eps), (TOK, 128))

    def gather_rows(h):
        load(h).wait()
        cols = columns(h)
        normed = (
            v_stream[:, cols].astype(F32) * scale[:, 0:1] * gain[cols].astype(F32).reshape(1, QW)
        ).astype(BF)
        grad = v_out[h].astype(F32)
        scaled0 = (w0 * grad).astype(BF)
        scaled1 = (w1 * grad).astype(BF)
        for plane in range(3):
            span = slice(plane * 256, plane * 256 + 256)
            rows_in = contract(qi[:, span], normed, 0, 0)
            rows_cot = contract(qc0[:, span], scaled0, 0, 0) + contract(
                qc1[:, span], scaled1, 0, 0
            )
            if plane < 2:
                send[h, plane] = rows_in.astype(BF)
                send[h, plane + 2] = rows_cot.astype(BF)
            else:
                send[h, 4] = (rows_in + rows_cot).astype(BF)

    def rows(i):
        return pl.ds(pl.multiple_of(i * 8, 8), 8)

    def half(turn):
        return high if turn == 0 else 1 - high

    def over(turn, k, target):
        return remote(
            send.at[half(turn), :, rows(target), :],
            got.at[half(turn), low, :, rows(s), :],
            send_sem.at[turn, k],
            recv_sem.at[turn, k],
            (target, x),
        )

    def own(turn):
        return pltpu.make_async_copy(
            send.at[half(turn), :, rows(s), :],
            got.at[half(turn), low, :, rows(s), :],
            own_sem.at[turn],
        )

    def onward(src, dst, k, side):
        return remote(
            src, dst, fwd_send.at[side, k], fwd_recv.at[side, k], (s, (right, left)[side])
        )

    def block(i):
        return got.at[high, low, :, rows(i), :]

    hello_cores(s, x, met_sem)
    gather_rows(high)
    met(met_sem)
    for side in range(2):
        onward(send.at[high, :, rows(s), :], block(s), 0, side).start()
    for turn in range(2):
        if turn == 1:
            gather_rows(1 - high)
        own(turn).start()
        for k in range(1, SPN):
            over(turn, k, peer(s, k)).start()
    for k in range(1, SPN):
        source = peer(s, k, -1)
        over(0, k, source).wait_recv()
        for side in range(2):
            onward(block(source), block(source), k, side).start()
    own(0).wait()
    own(1).wait()

    def finish(k):
        for turn in range(2):
            over(turn, k, s ^ 1).wait_send()
        over(1, k, s ^ 1).wait_recv()

    def finish_onward(k):
        for side in range(2):
            copy = onward(block(s), block(s), k, side)
            copy.wait_send()
            copy.wait_recv()

    loop(1, SPN, finish)
    loop(0, SPN, finish_onward)


def dispatch(stream, out_grad, gain, routes, weight):
    dma = pltpu.SemaphoreType.DMA
    return pl.pallas_call(
        dispatch_kernel,
        in_specs=[ANY, ANY, VM, VM, VM],
        out_specs=[ANY, VM],
        out_shape=[
            jax.ShapeDtypeStruct((2, 2, 5, 256, QW), BF),
            jax.ShapeDtypeStruct((TOK, 768), BF),
        ],
        scratch_shapes=[
            pltpu.VMEM((2, 5, 256, QW), BF),
            pltpu.VMEM((TOK, 4 * QW), BF),
            pltpu.VMEM((2, TOK, QW), BF),
            pltpu.VMEM((TOK, 768), BF),
            pltpu.VMEM((TOK, 768), BF),
            pltpu.VMEM((TOK, 768), BF),
            pltpu.VMEM((TOK, 128), F32),
            dma((3,)),
            dma((2,)),
            dma((2, SPN)),
            dma((2, SPN)),
            dma((2, SPN)),
            dma((2, SPN)),
            pltpu.SemaphoreType.REGULAR((2,)),
        ],
        compiler_params=pltpu.CompilerParams(
            collective_id=0, has_side_effects=True, vmem_limit_bytes=62 * 1024 * 1024
        ),
        name="dispatch",
    )(stream, out_grad, gain, routes, weight)


def swap_halves(v):
    tiles = v.reshape(16, 8, v.shape[1])
    return pltpu.roll(tiles, 4, 1).reshape(v.shape)


def expert_kernel(
    got, gate, up, down, slopes, gate_wg, up_wg, down_wg,
    vin, vcot, vmix, vg, vu, vd, ogu, od, gp, upre, hg, gu, hid,
    in_sem, w_sem, slope_sem, o_sem,
):
    def loads(q):
        hi, lo = q // 2, q % 2
        out = []
        for plane in range(5):
            if plane < 2:
                dst = vin.at[q, pl.ds(plane * 256, 256), :]
            elif plane < 4:
                dst = vcot.at[q, pl.ds((plane - 2) * 256, 256), :]
            else:
                dst = vmix.at[q]
            out.append(pltpu.make_async_copy(got.at[hi, lo, plane], dst, in_sem.at[q, plane]))
        rows = pl.ds(pl.multiple_of(q * QW, QW), QW)
        out.append(pltpu.make_async_copy(gate.at[rows, :], vg.at[q], w_sem.at[0, q]))
        out.append(pltpu.make_async_copy(up.at[rows, :], vu.at[q], w_sem.at[1, q]))
        out.append(pltpu.make_async_copy(down.at[:, rows], vd.at[q], w_sem.at[2, q]))
        return out

    loop(0, TPN, lambda q: [c.start() for c in loads(q)])
    gp[...] = jnp.zeros_like(gp)
    upre[...] = jnp.zeros_like(upre)
    hg[...] = jnp.zeros_like(hg)

    def forward(q):
        for c in loads(q):
            c.wait()
        first = lax.broadcasted_iota(I32, (128, QW), 0) % 8 < 4
        a = vmix[q, 0:128, :].astype(F32)
        b = vmix[q, 128:256, :].astype(F32)
        vin[q, 512:640, :] = jnp.where(first, a, b).astype(BF)
        vcot[q, 512:640, :] = jnp.where(first, b, a).astype(BF)
        rows = vin[q]
        gp[...] += contract(rows, vg[q], 1, 0)
        upre[...] += contract(rows, vu[q], 1, 0)
        hg[...] += contract(vcot[q], vd[q], 1, 1)

    loop(0, TPN, forward)
    hg[512:640, :] = swap_halves(hg[512:640, :])
    gate_pre, up_pre, hidden_grad = gp[...], upre[...], hg[...]
    logistic = jax.nn.sigmoid(gate_pre)
    silu = gate_pre * logistic
    hidden = silu * up_pre
    hid[0:512, :] = hidden[0:512, :].astype(BF)
    hid[512:640, :] = swap_halves(hidden[512:640, :]).astype(BF)
    gu[:, 0:FFQ] = (
        hidden_grad * up_pre * (logistic * (1.0 + gate_pre * (1.0 - logistic)))
    ).astype(BF)
    gu[:, FFQ : 2 * FFQ] = (hidden_grad * silu).astype(BF)

    out = pltpu.make_async_copy(gu, slopes, slope_sem)
    out.start()

    def grads_out(q):
        rows = pl.ds(pl.multiple_of(q * QW, QW), QW)
        return (
            pltpu.make_async_copy(ogu.at[0, q], gate_wg.at[rows, :], o_sem.at[0, q]),
            pltpu.make_async_copy(ogu.at[1, q], up_wg.at[rows, :], o_sem.at[1, q]),
            pltpu.make_async_copy(od.at[q], down_wg.at[:, rows], o_sem.at[2, q]),
        )

    def weights(q):
        both = contract(vin[q], gu[...], 0, 0)
        ogu[0, q] = both[:, 0:FFQ].astype(BF)
        ogu[1, q] = both[:, FFQ : 2 * FFQ].astype(BF)
        od[q] = contract(hid[...], vcot[q], 0, 0).astype(BF)
        for c in grads_out(q):
            c.start()

    loop(0, TPN, weights)
    out.wait()
    loop(0, TPN, lambda q: [c.wait() for c in grads_out(q)])


def expert(got, gate, up, down):
    full = TPN * QW
    return pl.pallas_call(
        expert_kernel,
        in_specs=[ANY] * 4,
        out_specs=[ANY] * 4,
        out_shape=[
            jax.ShapeDtypeStruct((640, 2 * FFQ), BF),
            jax.ShapeDtypeStruct((full, FFQ), BF),
            jax.ShapeDtypeStruct((full, FFQ), BF),
            jax.ShapeDtypeStruct((FFQ, full), BF),
        ],
        scratch_shapes=[
            pltpu.VMEM((TPN, 640, QW), BF),
            pltpu.VMEM((TPN, 640, QW), BF),
            pltpu.VMEM((TPN, 256, QW), BF),
            pltpu.VMEM((TPN, QW, FFQ), BF),
            pltpu.VMEM((TPN, QW, FFQ), BF),
            pltpu.VMEM((TPN, FFQ, QW), BF),
            pltpu.VMEM((2, TPN, QW, FFQ), BF),
            pltpu.VMEM((TPN, FFQ, QW), BF),
            pltpu.VMEM((640, FFQ), F32),
            pltpu.VMEM((640, FFQ), F32),
            pltpu.VMEM((640, FFQ), F32),
            pltpu.VMEM((640, 2 * FFQ), BF),
            pltpu.VMEM((640, FFQ), BF),
            pltpu.SemaphoreType.DMA((TPN, 5)),
            pltpu.SemaphoreType.DMA((3, TPN)),
            pltpu.SemaphoreType.DMA,
            pltpu.SemaphoreType.DMA((3, TPN)),
        ],
        compiler_params=pltpu.CompilerParams(vmem_limit_bytes=60 * 1024 * 1024),
        name="expert",
    )(got, gate, up, down)


def back_steps(
    start, fill, slopes, gate, up, combine, grad,
    part, v_gate, v_up, v_slopes, near, final, back, held, give, second,
    near_send, near_recv, own_sem, ret_send, ret_recv, two_send, two_recv, all_send, all_recv,
    w_sem, slope_sem, met_sem,
):
    s = lax.axis_index("sp")
    x = lax.axis_index("tp")
    right, left = lax.rem(x + 1, TPN), lax.rem(x + 3, TPN)

    def partners(c):
        odd = lax.rem(c, 2)
        one = x + 1 - 2 * lax.rem(x, 2)
        other = TPN - 1 - x
        return one + odd * (other - one), other + odd * (one - other)

    def to_pair(c, j):
        pair, _ = partners(c)
        quarter = pair if j == 0 else lax.rem(x + 2, TPN)
        return remote(
            part.at[quarter, c],
            near.at[c, j],
            near_send.at[c, j],
            near_recv.at[c, j],
            (s, pair),
        )

    def own_back(c):
        return pltpu.make_async_copy(final.at[c, s], back.at[c, s], own_sem.at[c])

    def home(c, k, target):
        return remote(
            final.at[c, target], back.at[c, s], ret_send.at[c, k], ret_recv.at[c, k], (target, x)
        )

    def to_other(c):
        _, other = partners(c)
        return remote(give.at[c], second.at[c], two_send.at[c], two_recv.at[c], (s, other))

    def spread(c, side):
        src = grad.at[x, c]
        return remote(
            src, src, all_send.at[side, 0, c], all_recv.at[side, 0, c], (s, (right, left)[side])
        )

    def spread_on(c, side):
        src = grad.at[(left, right)[side], c, pl.ds(side * 128, 128), :]
        return remote(
            src, src, all_send.at[side, 1, c], all_recv.at[side, 1, c], (s, (right, left)[side])
        )

    def begin(c):
        for j in range(2):
            to_pair(c, j).start()

    def load(q):
        rows = pl.ds(pl.multiple_of(q * QW, QW), QW)
        return (
            pltpu.make_async_copy(gate.at[rows, :], v_gate.at[q], w_sem.at[0, q]),
            pltpu.make_async_copy(up.at[rows, :], v_up.at[q], w_sem.at[1, q]),
        )

    def begin_load(q):
        for copy in load(q):
            copy.start()

    def rows_of(q):
        for copy in load(q):
            copy.wait()
        rows = (
            contract(v_slopes[:, 0:FFQ], v_gate[q], 1, 1)
            + contract(v_slopes[:, FFQ : 2 * FFQ], v_up[q], 1, 1)
        ).astype(BF)
        for c in range(CHUNKS):
            part[q, c] = rows[:, c * CW : (c + 1) * CW]

    take = pltpu.make_async_copy(slopes, v_slopes, slope_sem)
    take.start()
    loop(0, TPN, begin_load)
    start()
    take.wait()
    loop(1, TPN // 2, lambda k: rows_of(lax.rem(x + k, TPN)))
    hello_lines(s, x, met_sem)
    loop(TPN // 2, TPN, lambda k: rows_of(lax.rem(x + k, TPN)))
    hello_cores(s, x, met_sem)
    met(met_sem)
    loop(0, CHUNKS, begin)
    rows_of(x)
    fill()

    def open_chunk(t):
        _, other = partners(t)
        for j in range(2):
            to_pair(t, j).wait_recv()
            mine = part[x if j == 0 else other, t]
            total = (mine.astype(F32) + near[t, j].astype(F32)).astype(BF)
            lanes = slice(j * CW, (j + 1) * CW)
            final[t, :, 0:8, lanes] = total[0:256].reshape(32, 8, CW)
            final[t, :, 8:16, lanes] = total[256:512].reshape(32, 8, CW)
            mixed = total[512:640].reshape(16, 8, CW)
            final[t, 0:16, 16:24, lanes] = mixed
            final[t, 16:32, 16:24, lanes] = mixed
        own_back(t).start()
        for k in range(1, SPN):
            home(t, k, peer(s, k)).start()

    def close_chunk(c):
        own_back(c).wait()
        loop(1, SPN, lambda k: home(c, k, s ^ 1).wait_recv())
        summed = contract(combine[...], back[c].reshape(768, 2 * CW), 1, 0)
        held[c] = summed[:, 0:CW]
        give[c] = summed[:, CW : 2 * CW].astype(BF)
        to_other(c).start()

    def share(c):
        to_other(c).wait_recv()
        grad[x, c] = (held[c] + second[c].astype(F32)).astype(BF)
        for side in range(2):
            spread(c, side).start()

    def share_on(c):
        for side in range(2):
            spread(c, side).wait_recv()
            spread_on(c, side).start()

    lag = 2

    def stage(t):
        open_chunk(t)

        @pl.when(t >= lag)
        def _():
            close_chunk(t - lag)

    loop(0, CHUNKS, stage)
    early = CHUNKS - 3
    loop(0, early, share)
    close_chunk(CHUNKS - 2)
    loop(0, early, share_on)
    share(CHUNKS - 3)
    close_chunk(CHUNKS - 1)
    share(CHUNKS - 2)
    share_on(CHUNKS - 3)
    share(CHUNKS - 1)
    share_on(CHUNKS - 2)
    share_on(CHUNKS - 1)

    def finish(c):
        for j in range(2):
            to_pair(c, j).wait_send()
        to_other(c).wait_send()
        for side in range(2):
            spread(c, side).wait_send()
            spread_on(c, side).wait_send()
            spread_on(c, side).wait_recv()
        loop(1, SPN, lambda k: home(c, k, s ^ 1).wait_send())

    loop(0, CHUNKS, finish)


def expm1_negative(v):
    series = 1.0 + v * (1.0 / 9.0)
    for k in (8, 7, 6, 5, 4, 3, 2):
        series = 1.0 + v * (1.0 / k) * series
    return jnp.where(v > -0.5, v * series, jnp.exp(v) - 1.0)


def scan_rows(coeff, value, reverse):
    rows = lax.broadcasted_iota(I32, coeff.shape, 0)
    for k in (1, 2, 4, 8, 16, 32, 64, 128):
        if reverse:
            inside = rows < TOK - k
            shift = TOK - k
        else:
            inside = rows >= k
            shift = k
        coeff_far = jnp.where(inside, pltpu.roll(coeff, shift, 0), 1.0)
        value_far = jnp.where(inside, pltpu.roll(value, shift, 0), 0.0)
        value = value + coeff * value_far
        coeff = coeff * coeff_far
    return coeff, value


def mixer_steps(
    stream, out_grad, gain, grad, states, branch, out_proj, conv, decay_map, input_map, base, shift,
    branch_grad, conv_grad, proj_grad,
    v_stream, v_out, v_proj, v_states, v_shift, v_branch, v_conv, v_decay, v_input,
    sgb, dot, scale, lru, pulled, linear, coeffs, factors,
    ends, edges, pieces, pair, paired, far_y, far_z, sum_y, sum_z, last_y, last_z,
    big_sem, small_sem, end_send, end_recv, pair_send, pair_recv, one_send, one_recv,
    two_send, two_recv,
):
    s = lax.axis_index("sp")
    x = lax.axis_index("tp")
    z, y, core = s // 8, (s // 2) % 4, s % 2

    def big(which, q):
        cols = pl.ds(pl.multiple_of(q * QW, QW), QW)
        src, dst = (
            (stream.at[:, cols], v_stream.at[q]),
            (out_grad.at[:, cols], v_out.at[q]),
            (out_proj.at[cols, :], v_proj.at[q]),
        )[which]
        return pltpu.make_async_copy(src, dst, big_sem.at[which, q])

    small = [
        pltpu.make_async_copy(src, dst, small_sem.at[k])
        for k, (src, dst) in enumerate(
            (
                (conv, v_conv),
                (decay_map, v_decay),
                (input_map, v_input),
                (shift, v_shift),
                (states, v_states),
                (branch, v_branch),
            )
        )
    ]
    def begin(q):
        for which in range(3):
            big(which, q).start()

    def start():
        for copy in small:
            copy.start()
        loop(0, TPN, begin)

    def gates():
        for copy in small:
            copy.wait()

        c = v_conv[...].astype(F32)
        rows = lax.broadcasted_iota(I32, (TOK, FFQ), 0)
        for d in range(2):
            r = jax.nn.sigmoid(contract(v_conv[...], v_decay[d], 1, 0))
            i = jax.nn.sigmoid(contract(v_conv[...], v_input[d], 1, 0))
            rate = (-rate_scale) * base[d : d + 1, :]
            log_decay = r * rate + v_shift[d]
            decay = jnp.exp(log_decay)
            width = jnp.sqrt(-expm1_negative(2.0 * log_decay))
            drive = width * i * c
            if d == 0:
                coeffs[d] = jnp.where(rows == TOK - 1, 1.0, pltpu.roll(decay, TOK - 1, 0))
                ends[0:1, :] = decay[0:1]
            else:
                coeffs[d] = jnp.where(rows == 0, 1.0, pltpu.roll(decay, 1, 0))
                ends[2:3, :] = decay[TOK - 1 : TOK]
            linear[d, 0] = width * i
            linear[d, 1] = (
                ((v_states[d] - drive) - i * c * decay * decay / width) * rate * r * (1.0 - r)
            )
            linear[d, 2] = width * c * i * (1.0 - i)
        total = v_states[0] + v_states[1]
        b = v_branch[...].astype(F32)
        root = 0.7978845608028654
        tanh = jnp.tanh(root * (b + 0.044715 * b * b * b))
        gelu = 0.5 * b * (1.0 + tanh)
        slope = 0.5 * (1.0 + tanh) + 0.5 * b * (1.0 - tanh * tanh) * root * (
            1.0 + 3.0 * 0.044715 * b * b
        )
        lru[...] = (total * gelu).astype(BF)
        factors[0] = total * slope
        factors[1] = gelu

        def squares(q, carry):
            big(0, q).wait()
            v = v_stream[q].astype(F32)
            return carry + jnp.sum(v * v, axis=1, keepdims=True)

        square = lax.fori_loop(0, TPN, squares, jnp.zeros((TOK, 1), F32))
        scale[...] = jnp.broadcast_to(
            lax.rsqrt(square * (1.0 / (TPN * QW)) + norm_eps), (TOK, 128)
        )

    def rest():
        def grad_of(q):
            return jnp.concatenate([grad[q, c] for c in range(CHUNKS)], axis=1).astype(F32)

        def projected(q, carry):
            g = gain[pl.ds(pl.multiple_of(q * QW, QW), QW)].astype(F32).reshape(1, QW)
            w = v_stream[q].astype(F32) * (g * grad_of(q))
            return carry + jnp.sum(w, axis=1, keepdims=True)

        along = lax.fori_loop(0, TPN, projected, jnp.zeros((TOK, 1), F32))
        dot[...] = jnp.broadcast_to(along * scale[:, 0:1] * (1.0 / (TPN * QW)), (TOK, 128))
        pulled[...] = jnp.zeros_like(pulled)

        def rows_grad(q):
            big(1, q).wait()
            big(2, q).wait()
            r = scale[:, 0:1]
            unit = v_stream[q].astype(F32) * r
            scaled = gain[pl.ds(pl.multiple_of(q * QW, QW), QW)].astype(F32).reshape(1, QW) * grad_of(q)
            v = (v_out[q].astype(F32) + r * (scaled - unit * dot[:, 0:1])).astype(BF)
            sgb[q] = v
            pulled[...] += contract(v, v_proj[q], 1, 0)

        loop(0, TPN, rows_grad)
        lru_grad = pulled[...]
        branch_grad[...] = lru_grad * factors[0]
        state_grad = lru_grad * factors[1]
        def pair_to(q):
            return remote(
                pieces.at[q, :, 1 - core],
                pair.at[q],
                pair_send.at[q],
                pair_recv.at[q],
                (s + 1 - 2 * core, x),
            )

        def proj(q):
            pieces[q] = (
                contract(sgb[q], lru[...], 0, 0).astype(BF).reshape(TPN, 2, 128, FFQ)
            )
            pair_to(q).start()

        loop(0, TPN, proj)
        for d in range(2):
            reach, inner = scan_rows(coeffs[d], state_grad, d == 0)
            edge = slice(0, 1) if d == 0 else slice(TOK - 1, TOK)
            decay = ends[2 * d : 2 * d + 1, :]
            ends[2 * d : 2 * d + 1, :] = decay * reach[edge]
            ends[2 * d + 1 : 2 * d + 2, :] = decay * inner[edge]
            linear[d, 3] = reach
            linear[d, 4] = inner

        def ends_to(k, target):
            return remote(ends, edges.at[s], end_send.at[k], end_recv.at[k], (target, x))

        for k in range(1, SPN):
            ends_to(k, peer(s, k)).start()
        edges[s] = ends[...]


        def meet(q):
            pair_to(q).wait_recv()
            paired[q] = (pieces[q, :, core].astype(F32) + pair[q].astype(F32)).astype(BF)

        loop(0, TPN, meet)
        first, second = pl.ds(0, 64), pl.ds(64, 64)

        def along_y(k):
            return lax.rem(y + k, 4), (z * 8 + lax.rem(y + k, 4) * 2 + core, x)

        def along_z(k):
            return lax.rem(z + k, 4), (lax.rem(z + k, 4) * 8 + y * 2 + core, x)

        def one(side, k):
            place, target = (along_y, along_z)[side](k)
            if side == 0:
                src, dst = paired.at[:, place, first, :], far_y.at[k - 1]
            else:
                src, dst = paired.at[place, :, second, :], far_z.at[k - 1]
            return remote(src, dst, one_send.at[side, k], one_recv.at[side, k], target)

        def two(side, k):
            place, target = (along_z, along_y)[side](k)
            if side == 0:
                src, dst = sum_y.at[place], last_y.at[k - 1]
            else:
                src, dst = sum_z.at[place], last_z.at[k - 1]
            return remote(src, dst, two_send.at[side, k], two_recv.at[side, k], target)

        for k in (1, 3, 2):
            for side in range(2):
                one(side, k).start()

        for k in range(1, SPN):
            ends_to(k, s ^ 1).wait_recv()

        def carry_in(j, carry):
            later = SPN - 1 - j
            e0, e1 = edges[later], edges[j]
            from_right = jnp.where(later > s, e0[1:2] + e0[0:1] * carry[0], carry[0])
            from_left = jnp.where(j < s, e1[3:4] + e1[2:3] * carry[1], carry[1])
            return from_right, from_left

        none = jnp.zeros((1, FFQ), F32)
        incoming = lax.fori_loop(0, SPN, carry_in, (none, none))

        def back_maps(d):
            adjoint = linear[d, 4] + linear[d, 3] * incoming[d]
            highest = lax.Precision.HIGHEST
            return (
                adjoint * linear[d, 0]
                + contract(adjoint * linear[d, 1], v_decay[d].astype(F32), 1, 1, highest)
                + contract(adjoint * linear[d, 2], v_input[d].astype(F32), 1, 1, highest)
            )

        conv_grad[...] = back_maps(0) + back_maps(1)

        for side in range(2):
            for k in (1, 3, 2):
                one(side, k).wait_recv()
            if side == 0:
                acc = paired[:, y, first, :].astype(F32)
            else:
                acc = paired[z, :, second, :].astype(F32)
            came = (far_y, far_z)[side]
            acc = acc + came[0].astype(F32) + came[1].astype(F32) + came[2].astype(F32)
            (sum_y, sum_z)[side][...] = acc.astype(BF)
            for k in (1, 3, 2):
                two(side, k).start()

        for side in range(2):
            for k in (1, 3, 2):
                two(side, k).wait_recv()
            came = (last_y, last_z)[side]
            acc = (sum_y[z] if side == 0 else sum_z[y]).astype(F32)
            acc = acc + came[0].astype(F32) + came[1].astype(F32) + came[2].astype(F32)
            proj_grad[pl.ds(side * 64, 64), :] = acc

        for side in range(2):
            for k in (1, 3, 2):
                one(side, k).wait_send()
                two(side, k).wait_send()
        loop(1, SPN, lambda k: ends_to(k, s ^ 1).wait_send())
        loop(0, TPN, lambda q: pair_to(q).wait_send())

    return start, gates, rest


def tail_kernel(
    slopes, gate, up, combine, stream, out_grad, gain, states, branch, out_proj, conv, decay_map,
    input_map, base, shift, branch_grad, conv_grad, proj_grad, grad, *scratch,
):
    hello(lax.axis_index("sp"), lax.axis_index("tp"))
    start, gates, rest = mixer_steps(
        stream, out_grad, gain, grad, states, branch, out_proj, conv, decay_map, input_map, base,
        shift, branch_grad, conv_grad, proj_grad, *scratch[NBACK:],
    )
    back_steps(start, gates, slopes, gate, up, combine, grad, *scratch[:NBACK])
    rest()


def tail(*operands):
    whole = (TPN, TOK, QW)
    square = (TOK, FFQ)
    dma = pltpu.SemaphoreType.DMA
    return pl.pallas_call(
        tail_kernel,
        in_specs=[ANY, ANY, ANY, VM, ANY, ANY, VM, ANY, ANY, ANY, ANY, ANY, ANY, VM, ANY],
        out_specs=[VM] * 3,
        out_shape=[
            jax.ShapeDtypeStruct(square, F32),
            jax.ShapeDtypeStruct(square, F32),
            jax.ShapeDtypeStruct((128, FFQ), F32),
        ],
        scratch_shapes=[
            pltpu.VMEM((TPN, CHUNKS, TOK, CW), BF),
            pltpu.VMEM((TPN, CHUNKS, 640, CW), BF),
            pltpu.VMEM((TPN, QW, FFQ), BF),
            pltpu.VMEM((TPN, QW, FFQ), BF),
            pltpu.VMEM((640, 2 * FFQ), BF),
            pltpu.VMEM((CHUNKS, 2, 640, CW), BF),
            pltpu.VMEM((CHUNKS, SPN, 24, 2 * CW), BF),
            pltpu.VMEM((CHUNKS, SPN, 24, 2 * CW), BF),
            pltpu.VMEM((CHUNKS, TOK, CW), F32),
            pltpu.VMEM((CHUNKS, TOK, CW), BF),
            pltpu.VMEM((CHUNKS, TOK, CW), BF),
            dma((CHUNKS, 2)),
            dma((CHUNKS, 2)),
            dma((CHUNKS,)),
            dma((CHUNKS, SPN)),
            dma((CHUNKS, SPN)),
            dma((CHUNKS,)),
            dma((CHUNKS,)),
            dma((2, 2, CHUNKS)),
            dma((2, 2, CHUNKS)),
            dma((2, TPN)),
            dma,
            pltpu.SemaphoreType.REGULAR((2,)),
            pltpu.VMEM(whole, BF),
            pltpu.VMEM(whole, BF),
            pltpu.VMEM((TPN, QW, FFQ), BF),
            pltpu.VMEM((2,) + square, F32),
            pltpu.VMEM((2,) + square, F32),
            pltpu.VMEM(square, BF),
            pltpu.VMEM(square, BF),
            pltpu.VMEM((2, FFQ, FFQ), BF),
            pltpu.VMEM((2, FFQ, FFQ), BF),
            pltpu.VMEM(whole, BF),
            pltpu.VMEM((TOK, 128), F32),
            pltpu.VMEM((TOK, 128), F32),
            pltpu.VMEM(square, BF),
            pltpu.VMEM(square, F32),
            pltpu.VMEM((2, 5) + square, F32),
            pltpu.VMEM((2,) + square, F32),
            pltpu.VMEM((2,) + square, F32),
            pltpu.VMEM((4, FFQ), F32),
            pltpu.VMEM((SPN, 4, FFQ), F32),
            pltpu.VMEM((4, 4, 2, 128, FFQ), BF),
            pltpu.VMEM((4, 4, 128, FFQ), BF),
            pltpu.VMEM((4, 4, 128, FFQ), BF),
            pltpu.VMEM((3, 4, 64, FFQ), BF),
            pltpu.VMEM((3, 4, 64, FFQ), BF),
            pltpu.VMEM((4, 64, FFQ), BF),
            pltpu.VMEM((4, 64, FFQ), BF),
            pltpu.VMEM((3, 64, FFQ), BF),
            pltpu.VMEM((3, 64, FFQ), BF),
            dma((3, TPN)),
            dma((6,)),
            dma((SPN,)),
            dma((SPN,)),
            dma((TPN,)),
            dma((TPN,)),
            dma((2, 4)),
            dma((2, 4)),
            dma((2, 4)),
            dma((2, 4)),
        ],
        compiler_params=pltpu.CompilerParams(
            collective_id=1, has_side_effects=True, vmem_limit_bytes=52 * 1024 * 1024
        ),
        name="tail",
    )(*operands)


def body(
    out_grad,
    stream,
    norm_gain,
    routes,
    route_weight,
    gate_weight,
    up_weight,
    down_weight,
    out_proj,
    conv_out,
    gate_branch,
    decay_map,
    input_map,
    decay_param,
    decay_shift,
    states,
):
    gain = norm_gain
    got, combine = dispatch(stream, out_grad, gain, routes.T, route_weight.T)
    slopes, gate_wgrad, up_wgrad, down_wgrad = expert(
        got, gate_weight[0], up_weight[0], down_weight[0]
    )
    base = jax.nn.softplus(-decay_param)
    branch_grad, conv_grad, proj_grad = tail(
        slopes, gate_weight[0], up_weight[0], combine, stream, out_grad, gain, states, gate_branch, out_proj, conv_out,
        decay_map[:, 0], input_map[:, 0], base, decay_shift,
    )
    return (
        conv_grad, branch_grad, proj_grad, gate_wgrad[None], up_wgrad[None], down_wgrad[None]
    )


def solution(mesh):
    in_specs = (
        P(SP, None),
        P(SP, None),
        P(),
        P(SP, None),
        P(SP, None),
        P(SP, None, "tp"),
        P(SP, None, "tp"),
        P(SP, "tp", None),
        P(None, "tp"),
        P(SP, "tp"),
        P(SP, "tp"),
        P(None, "tp", None, None),
        P(None, "tp", None, None),
        P(None, "tp"),
        P(None, SP, "tp"),
        P(None, SP, "tp"),
    )
    out_specs = (
        P(SP, "tp"),
        P(SP, "tp"),
        P(SP, "tp"),
        P(SP, None, "tp"),
        P(SP, None, "tp"),
        P(SP, "tp", None),
    )
    return jax.shard_map(body, mesh=mesh, in_specs=in_specs, out_specs=out_specs, check_vma=False)
```
